32 devices in a mesh: grp: 2 (over y), fs: 4 (over z), tp: 4 (over x, core).
Axes of the slice: x: 2, y: 2, z: 4, core: 2. Of those that a mesh axis runs over, the one named last changes fastest.
Arguments:
- tokens: bfloat16 [2048, 2048], P(('grp', 'fs')), parts along dimension 0, may hold values from -6 to 6
- ffn_pre_gain: bfloat16 [2048], replicated, may hold values from 0.099609375 to 1.8984375
- gate_weight: bfloat16 [2048, 5632], P('fs', 'tp'), may hold values from -0.125 to 0.125
- up_weight: bfloat16 [2048, 5632], P('fs', 'tp'), may hold values from -0.125 to 0.125
- down_weight: bfloat16 [5632, 2048], P('tp', 'fs'), may hold values from -0.078125 to 0.078125
- ffn_post_gain: bfloat16 [2048], replicated, may hold values from 0.099609375 to 1.8984375
- mix_pre_gain: bfloat16 [2048], replicated, may hold values from 0.099609375 to 1.8984375
- mix_u_weight: bfloat16 [2048, 2048], P('fs', 'tp'), may hold values from -0.125 to 0.125
- mix_v_weight: bfloat16 [2048, 2048], P('fs', 'tp'), may hold values from -0.125 to 0.125
- spatial_gain: bfloat16 [2048], P('tp'), may hold values from 0.099609375 to 1.8984375
- spatial_weight: bfloat16 [16, 128, 128], P('tp'), may hold values from -0.5 to 0.5
- spatial_bias: bfloat16 [16, 128], P('tp'), may hold values from 0.099609375 to 1.8984375
- mix_out_weight: bfloat16 [2048, 2048], P('tp', 'fs'), may hold values from -0.125 to 0.125
- mix_post_gain: bfloat16 [2048], replicated, may hold values from 0.099609375 to 1.8984375
- late_pre_gain: bfloat16 [2048], replicated, may hold values from 0.099609375 to 1.8984375
- late_post_gain: bfloat16 [2048], replicated, may hold values from 0.099609375 to 1.8984375
Outputs:
- result: bfloat16 [2048, 2048], P(('grp', 'fs')), parts along dimension 0
The draws below stay inside these ranges and needn't reach their ends.
There are 2 independent parts, one for each index of `grp`. The reference program is written for one: setup_inputs(seed, part) draws one part's arguments, and reference() takes and returns one part's arrays. A program takes and returns all parts, laid end to end along the dimension named above; an argument that names none is the same for every part. Nothing has to cross between parts.
All inputs are finite; a program needn't handle non-finite values.
Results may differ from the reference program's by a relative error of at most 0.019.
Values may be sent and summed in bfloat16 or wider, within the bound.
A program may use at most 128 MiB of HBM per device.

```python
import jax
import jax.numpy as jnp
from jax import lax

D = 2048
FF = 5632
MIX_WIDTH = 2048
GROUP_WIDTH = 128
BLOCK = 128
GROUPS = 16
TOKENS = 1024
N_TP = 4


def block_scale(stream_key, extent, split, smallest, top_value):
    def one(dim, shards_of):
        steps = jax.random.uniform(jax.random.fold_in(jax.random.fold_in(stream_key, 6), dim), (shards_of,), jnp.float32, smallest / len(split), top_value / len(split))
        return jnp.repeat(jnp.exp(steps), extent[dim] // shards_of).reshape((-1,) + (1,) * (len(extent) - dim - 1))

    loudness = one(*split[0])
    for cut in split[1:]:
        loudness = loudness * one(*cut)
    return loudness


def noise(own_key, dims, scale, reach, cuts=(), kind=jnp.bfloat16):
    entries = jax.random.normal(own_key, dims, jnp.float32) * scale
    if len(cuts) > 0:
        entries = block_scale(own_key, dims, cuts, -0.22, 0.18) * entries
    return jnp.clip(entries, min=-reach, max=reach).astype(kind)


def setup_inputs(seed: int = 0, part: int = 0) -> dict:
    seeds = jax.random.split(jax.random.key(seed), 17)
    own_keys = jax.random.split(jax.random.fold_in(seeds[16], part), 17)
    return {
        "tokens": noise(own_keys[0], (TOKENS, D), 1.0, 6.0, ((0, 4),)),
        "ffn_pre_gain": jnp.clip(1.0 + 0.18 * jax.random.normal(seeds[1], (D,), jnp.float32), 0.099609375, 1.8984375).astype(jnp.bfloat16),
        "gate_weight": noise(seeds[2], (D, FF), D ** -0.5, 0.125, ((0, 4), (1, 4))),
        "up_weight": noise(seeds[3], (D, FF), D ** -0.5, 0.125, ((0, 4), (1, 4))),
        "down_weight": noise(seeds[4], (FF, D), FF ** -0.5, 0.078125, ((0, 4), (1, 4))),
        "ffn_post_gain": jnp.clip(1.0 + 0.18 * jax.random.normal(seeds[5], (D,), jnp.float32), 0.099609375, 1.8984375).astype(jnp.bfloat16),
        "mix_pre_gain": jnp.clip(1.0 + 0.18 * jax.random.normal(seeds[6], (D,), jnp.float32), 0.099609375, 1.8984375).astype(jnp.bfloat16),
        "mix_u_weight": noise(seeds[7], (D, MIX_WIDTH), D ** -0.5, 0.125, ((0, 4), (1, 4))),
        "mix_v_weight": noise(seeds[8], (D, MIX_WIDTH), D ** -0.5, 0.125, ((0, 4), (1, 4))),
        "spatial_gain": jnp.clip(1.0 + 0.18 * jax.random.normal(seeds[9], (MIX_WIDTH,), jnp.float32), 0.099609375, 1.8984375).astype(jnp.bfloat16),
        "spatial_weight": noise(seeds[10], (GROUPS, BLOCK, BLOCK), BLOCK ** -0.5, 0.5, ((0, 4),)),
        "spatial_bias": jnp.clip(1.0 + 0.18 * jax.random.normal(seeds[11], (GROUPS, BLOCK), jnp.float32), 0.099609375, 1.8984375).astype(jnp.bfloat16),
        "mix_out_weight": noise(seeds[12], (MIX_WIDTH, D), MIX_WIDTH ** -0.5, 0.125, ((0, 4), (1, 4))),
        "mix_post_gain": jnp.clip(1.0 + 0.18 * jax.random.normal(seeds[13], (D,), jnp.float32), 0.099609375, 1.8984375).astype(jnp.bfloat16),
        "late_pre_gain": jnp.clip(1.0 + 0.18 * jax.random.normal(seeds[14], (D,), jnp.float32), 0.099609375, 1.8984375).astype(jnp.bfloat16),
        "late_post_gain": jnp.clip(1.0 + 0.18 * jax.random.normal(seeds[15], (D,), jnp.float32), 0.099609375, 1.8984375).astype(jnp.bfloat16),
    }


def row_norm(values, gain):
    scale = lax.rsqrt(lax.optimization_barrier(jnp.mean(values * values, axis=-1, keepdims=True)) + 1e-06)
    return values * scale * gain.astype(jnp.float32)

def split_sum(left, right, pieces):
    width = left.shape[1] // pieces
    total = jnp.zeros((left.shape[0], right.shape[1]), jnp.float32)
    for index in range(pieces):
        partial_term = jnp.dot(left[:, index * width:(index + 1) * width], right[index * width:(index + 1) * width], preferred_element_type=jnp.float32)
        rounded = lax.optimization_barrier(partial_term.astype(jnp.bfloat16))
        total = total + rounded.astype(jnp.float32)
    return total

def feed_forward(stream, pre_gain, post_gain, gate_weight, up_weight, down_weight):
    normed = row_norm(stream.astype(jnp.float32), pre_gain).astype(jnp.bfloat16)
    gate = jnp.dot(normed, gate_weight, preferred_element_type=jnp.float32)
    upper = jnp.dot(normed, up_weight, preferred_element_type=jnp.float32)
    hidden = (jax.nn.silu(gate) * upper).astype(jnp.bfloat16)
    branch = split_sum(hidden, down_weight, N_TP)
    return (stream.astype(jnp.float32) + 0.5 * row_norm(branch, post_gain)).astype(jnp.bfloat16)

def reference(tokens, ffn_pre_gain, gate_weight, up_weight, down_weight, ffn_post_gain, mix_pre_gain, mix_u_weight, mix_v_weight, spatial_gain, spatial_weight, spatial_bias, mix_out_weight, mix_post_gain, late_pre_gain, late_post_gain):
    first = feed_forward(tokens, ffn_pre_gain, ffn_post_gain, gate_weight, up_weight, down_weight)
    normed = row_norm(first.astype(jnp.float32), mix_pre_gain).astype(jnp.bfloat16)
    gated_u = jax.nn.gelu(jnp.dot(normed, mix_u_weight, preferred_element_type=jnp.float32), approximate=False)
    gating_v = jax.nn.gelu(jnp.dot(normed, mix_v_weight, preferred_element_type=jnp.float32), approximate=False)
    count = gating_v.shape[0]
    grouped = gating_v.reshape(count, GROUPS, GROUP_WIDTH)
    centred = grouped - lax.optimization_barrier(jnp.mean(grouped, axis=-1, keepdims=True))
    vnorm = centred * lax.rsqrt(lax.optimization_barrier(jnp.mean(centred * centred, axis=-1, keepdims=True)) + 1e-05)
    vnorm = (vnorm * spatial_gain.astype(jnp.float32).reshape(GROUPS, GROUP_WIDTH)).astype(jnp.bfloat16)
    blocks = vnorm.reshape(count // BLOCK, BLOCK, GROUPS, GROUP_WIDTH).astype(jnp.float32)
    lower = jnp.tril(jnp.ones((BLOCK, BLOCK), dtype=bool))
    masked = jnp.where(lower[None], spatial_weight, jnp.zeros_like(spatial_weight)).astype(jnp.float32)
    spatial = jnp.einsum('gts,nsgc->ntgc', masked, blocks)
    spatial = spatial + spatial_bias.astype(jnp.float32).T[None, :, :, None]
    mixed = (gated_u * spatial.reshape(count, MIX_WIDTH)).astype(jnp.bfloat16)
    branch = split_sum(mixed, mix_out_weight, N_TP)
    second = (first.astype(jnp.float32) + row_norm(branch, mix_post_gain)).astype(jnp.bfloat16)
    return feed_forward(second, late_pre_gain, late_post_gain, gate_weight, up_weight, down_weight)
```

```python
import functools
import math

import jax
import jax.numpy as jnp
from jax import lax
from jax.experimental import pallas as pl
from jax.experimental.pallas import tpu as pltpu
from jax.sharding import PartitionSpec as P

GROUP_WIDTH = 128
BLOCK = 128
TILE = 256
F32 = jnp.float32
BF16 = jnp.bfloat16
MESH = pl.DeviceIdType.MESH
SPLITS = (2, 2, 2, 1, 1, 2)
PIECE = 32


def aligned(value, unit):
    return value if isinstance(value, int) else pl.multiple_of(value, unit)


def over_tiles(width, body):
    count = width // TILE

    def step(i, carry):
        body(pl.multiple_of(i * TILE, TILE), TILE)
        return carry

    lax.fori_loop(0, count, step, 0)
    if width % TILE:
        body(count * TILE, width % TILE)


def over_rows(count, size, body):
    def step(i, carry):
        body(pl.multiple_of(i * size, size))
        return carry

    lax.fori_loop(0, count // size, step, 0)


def gelu(a):
    return 0.5 * a * (1.0 + lax.erf(a * (2.0**-0.5)))


def kernel(
    sizes,
    tokens,
    gain0,
    gain1,
    gain2,
    gain3,
    gain4,
    gain5,
    gate_w,
    up_w,
    down_w,
    u_w,
    v_w,
    out_w,
    spatial_gain,
    spatial_weight,
    spatial_bias,
    result,
    gate_full,
    up_full,
    down_full,
    u_full,
    v_full,
    out_full,
    normed,
    hidden,
    mixed,
    parts,
    paired,
    outgoing,
    landed,
    streams,
    own_sem,
    left_send,
    left_recv,
    right_send,
    right_recv,
    side_send,
    side_recv,
    pair_send,
    pair_recv,
    sum_send,
    sum_recv,
    twin_send,
    twin_recv,
    put_send,
    put_recv,
    pass_send,
    pass_recv,
    last_sem,
):
    grp_n, fs_n, tp_n = sizes
    grp, fs, tp = lax.axis_index("grp"), lax.axis_index("fs"), lax.axis_index("tp")
    shards = (gate_w, up_w, down_w, u_w, v_w, out_w)
    fulls = (gate_full, up_full, down_full, u_full, v_full, out_full)
    count, width = tokens.shape
    chunk = count // tp_n
    chips = tp_n // 2
    chip, core = tp // 2, lax.rem(tp, 2)
    twin = tp + 1 - 2 * core
    columns = pair_send.shape[1]
    column = width // columns
    piece_n = put_send.shape[1]
    piece_rows = chunk // piece_n
    all_gains = (gain0, gain1, gain2, gain3, gain4, gain5)

    barrier = pltpu.get_barrier_semaphore()
    for move in (1, fs_n - 1):
        pl.semaphore_signal(
            barrier, inc=1, device_id={"fs": lax.rem(fs + move, fs_n)}, device_id_type=MESH
        )
    for move in range(1, grp_n):
        pl.semaphore_signal(
            barrier, inc=1, device_id={"grp": lax.rem(grp + move, grp_n)}, device_id_type=MESH
        )
    for move in range(1, tp_n):
        pl.semaphore_signal(
            barrier, inc=1, device_id={"tp": lax.rem(tp + move, tp_n)}, device_id_type=MESH
        )
    pl.semaphore_wait(barrier, 2 + grp_n - 1 + tp_n - 1)

    units = []
    for w in range(6):
        piece = shards[w].shape[0] // grp_n // SPLITS[w]
        for s in range(SPLITS[w]):
            units.append((w, s * piece, piece))

    def unit_rows(unit):
        w, low, piece = units[unit]
        return aligned(grp * (shards[w].shape[0] // grp_n) + low, 16), piece

    def place(w, block, low, piece):
        if w in (2, 5):
            return fulls[w].at[block, pl.ds(low, piece), :]
        start = aligned(block * shards[w].shape[0] + low, 16)
        return fulls[w].at[pl.ds(start, piece), :]

    def own_copy(w):
        return pltpu.make_async_copy(
            shards[w], place(w, fs, 0, shards[w].shape[0]), own_sem.at[w]
        )

    def to_right(unit, hop, own=False):
        w = units[unit][0]
        low, piece = unit_rows(unit)
        target = place(w, fs - hop, low, piece)
        source = shards[w].at[pl.ds(low, piece), :] if own else target
        return pltpu.make_async_remote_copy(
            src_ref=source,
            dst_ref=target,
            send_sem=right_send.at[unit, hop],
            recv_sem=right_recv.at[unit, hop],
            device_id={"fs": fs + 1},
            device_id_type=MESH,
        )

    def to_left(unit, hop, own=False):
        w = units[unit][0]
        low, piece = unit_rows(unit)
        target = place(w, fs + hop, low, piece)
        source = shards[w].at[pl.ds(low, piece), :] if own else target
        return pltpu.make_async_remote_copy(
            src_ref=source,
            dst_ref=target,
            send_sem=left_send.at[unit, hop],
            recv_sem=left_recv.at[unit, hop],
            device_id={"fs": fs - 1},
            device_id_type=MESH,
        )

    def to_side(unit, side, hop, move):
        w = units[unit][0]
        low, piece = unit_rows(unit)
        block = fs - hop if side == 0 else fs + hop
        target = place(w, block, low, piece)
        return pltpu.make_async_remote_copy(
            src_ref=target,
            dst_ref=target,
            send_sem=side_send.at[unit, side, move - 1, hop],
            recv_sem=side_recv.at[unit, side, move - 1, hop],
            device_id={"grp": lax.rem(grp + move, grp_n)},
            device_id_type=MESH,
        )

    def send_own(unit):
        if unit >= len(units):
            return

        @pl.when(fs < fs_n - 1)
        def _():
            to_right(unit, 0, own=True).start()

        @pl.when(fs > 0)
        def _():
            to_left(unit, 0, own=True).start()

    def relay(unit):
        def step(hop, carry):
            @pl.when(fs >= hop)
            def _():
                to_right(unit, hop - 1).wait_recv()

                @pl.when(fs < fs_n - 1)
                def _():
                    to_right(unit, hop).start()

                for move in range(1, grp_n):
                    to_side(unit, 0, hop, move).start()

            @pl.when(fs + hop < fs_n)
            def _():
                to_left(unit, hop - 1).wait_recv()

                @pl.when(fs > 0)
                def _():
                    to_left(unit, hop).start()

                for move in range(1, grp_n):
                    to_side(unit, 1, hop, move).start()

            return carry

        lax.fori_loop(1, fs_n, step, 0)

    def wait_weight(w):
        own_copy(w).wait()
        for unit in range(len(units)):
            if units[unit][0] == w:

                def step(hop, carry, unit=unit):
                    for move in range(1, grp_n):

                        @pl.when(fs >= hop)
                        def _():
                            to_side(unit, 0, hop, move).wait_recv()

                        @pl.when(fs + hop < fs_n)
                        def _():
                            to_side(unit, 1, hop, move).wait_recv()

                    return carry

                lax.fori_loop(1, fs_n, step, 0)

    def finish_sends():
        for unit in range(len(units)):

            def step(hop, carry, unit=unit):
                @pl.when((fs >= hop) & (fs < fs_n - 1))
                def _():
                    to_right(unit, hop).wait_send()

                @pl.when((fs + hop < fs_n) & (fs > 0))
                def _():
                    to_left(unit, hop).wait_send()

                @pl.when(hop > 0)
                def _():
                    for move in range(1, grp_n):

                        @pl.when(fs >= hop)
                        def _():
                            to_side(unit, 0, hop, move).wait_send()

                        @pl.when(fs + hop < fs_n)
                        def _():
                            to_side(unit, 1, hop, move).wait_send()

                return carry

            lax.fori_loop(0, fs_n, step, 0)

    def other(move, which):
        return lax.rem(chip + move, chips) * 2 + which

    def origin(move, which):
        return lax.rem(chip + chips - move, chips) * 2 + which

    def chunk_rows(owner):
        return pl.ds(aligned(owner * chunk, 16), chunk)

    def column_span(col):
        return pl.ds(aligned(col * column, 128), column)

    def pair_copy(phase, col, move):
        span = column_span(col)
        return pltpu.make_async_remote_copy(
            src_ref=parts.at[phase, chunk_rows(other(move, 1 - core)), span],
            dst_ref=paired.at[phase, move, :, span],
            send_sem=pair_send.at[phase, col, move],
            recv_sem=pair_recv.at[phase, col, move],
            device_id={"tp": twin},
            device_id_type=MESH,
        )

    def sum_copy(phase, col, move):
        span = column_span(col)
        return pltpu.make_async_remote_copy(
            src_ref=outgoing.at[phase, move, :, span],
            dst_ref=landed.at[phase, move, :, span],
            send_sem=sum_send.at[phase, col, move],
            recv_sem=sum_recv.at[phase, col, move],
            device_id={"tp": other(move, core)},
            device_id_type=MESH,
        )

    def piece_span(owner, piece):
        return pl.ds(aligned(owner * chunk + piece * piece_rows, 16), piece_rows)

    def twin_copy(phase, piece):
        rows = piece_span(tp, piece)
        return pltpu.make_async_remote_copy(
            src_ref=streams.at[phase, rows, :],
            dst_ref=streams.at[phase, rows, :],
            send_sem=twin_send.at[phase, piece],
            recv_sem=twin_recv.at[phase, piece],
            device_id={"tp": twin},
            device_id_type=MESH,
        )

    def put_copy(phase, piece, move):
        rows = piece_span(tp, piece)
        return pltpu.make_async_remote_copy(
            src_ref=streams.at[phase, rows, :],
            dst_ref=streams.at[phase, rows, :],
            send_sem=put_send.at[phase, piece, move],
            recv_sem=put_recv.at[phase, piece, move],
            device_id={"tp": other(move, core)},
            device_id_type=MESH,
        )

    def pass_copy(phase, piece, move):
        rows = piece_span(origin(move, core), piece)
        return pltpu.make_async_remote_copy(
            src_ref=streams.at[phase, rows, :],
            dst_ref=streams.at[phase, rows, :],
            send_sem=pass_send.at[phase, piece, move],
            recv_sem=pass_recv.at[phase, piece, move],
            device_id={"tp": twin},
            device_id_type=MESH,
        )

    def gain(row):
        return all_gains[row][...].astype(F32).reshape(1, width)

    def norm_rows(load, row):
        def body(low):
            values = load(pl.ds(low, 32)).astype(F32)
            scale = lax.rsqrt(jnp.mean(values * values, axis=-1, keepdims=True) + 1e-06)
            normed[pl.ds(low, 32), :] = (values * scale * gain(row)).astype(BF16)

        over_rows(count, 32, body)

    def start_sums(phase, col):
        for move in range(1, chips):
            pair_copy(phase, col, move).wait_recv()
            span = column_span(col)
            mine = parts[phase, chunk_rows(other(move, core)), span].astype(F32)
            both = mine + paired[phase, move, :, span].astype(F32)
            outgoing[phase, move, :, span] = both.astype(BF16)
            sum_copy(phase, col, move).start()

    def add_branch(phase, load, row, factor):
        for col in range(columns):
            pair_copy(phase, col, 0).wait_recv()
            for move in range(1, chips):
                sum_copy(phase, col, move).wait_recv()
        for piece in range(piece_n):

            def body(low, piece=piece):
                here = pl.ds(aligned(piece * piece_rows + low, 16), 16)
                rows = pl.ds(aligned(tp * chunk + piece * piece_rows + low, 16), 16)
                total = parts[phase, rows, :].astype(F32) + paired[phase, 0, here, :].astype(F32)
                for move in range(1, chips):
                    total = total + landed[phase, move, here, :].astype(F32)
                scale = lax.rsqrt(jnp.mean(total * total, axis=-1, keepdims=True) + 1e-06)
                branch = total * scale * gain(row)
                streams[phase, rows, :] = (load(rows).astype(F32) + factor * branch).astype(BF16)

            over_rows(piece_rows, 16, body)
            for move in range(1, chips):
                put_copy(phase, piece, move).start()
            twin_copy(phase, piece).start()

    def wait_put(phase):
        for piece in range(piece_n):
            for move in range(1, chips):
                put_copy(phase, piece, move).wait_recv()
                pass_copy(phase, piece, move).start()
        for piece in range(piece_n):
            twin_copy(phase, piece).wait_recv()
            for move in range(1, chips):
                pass_copy(phase, piece, move).wait_recv()

    def finish_phase(phase):
        for col in range(columns):
            for move in range(chips):
                pair_copy(phase, col, move).wait_send()
            for move in range(1, chips):
                sum_copy(phase, col, move).wait_send()
        for piece in range(piece_n):
            twin_copy(phase, piece).wait_send()
            for move in range(1, chips):
                put_copy(phase, piece, move).wait_send()
                pass_copy(phase, piece, move).wait_send()

    def hidden_units():
        def body(low, size):
            cols = pl.ds(low, size)
            gate = jnp.dot(normed[...], gate_full[:, cols], preferred_element_type=F32)
            upper = jnp.dot(normed[...], up_full[:, cols], preferred_element_type=F32)
            hidden[:, cols] = (gate / (1.0 + jnp.exp(-gate)) * upper).astype(BF16)

        over_tiles(hidden.shape[1], body)

    def project(phase, left, right):
        blocks = fs_n // columns

        def step(col, carry):
            terms = [
                jnp.dot(left[...], right[col * blocks + b], preferred_element_type=F32)
                for b in range(blocks)
            ]
            terms = terms[0] if blocks == 1 else jnp.concatenate(terms, axis=1)
            parts[phase, :, column_span(col)] = terms.astype(BF16)
            for move in range(chips - 1, -1, -1):
                pair_copy(phase, col, move).start()

            @pl.when(col > 0)
            def _():
                start_sums(phase, col - 1)

            return carry

        lax.fori_loop(0, columns, step, 0)
        start_sums(phase, columns - 1)

    def mix():
        rows = lax.broadcasted_iota(jnp.int32, (BLOCK, BLOCK), 0)
        cols = lax.broadcasted_iota(jnp.int32, (BLOCK, BLOCK), 1)
        all_spatial_gain = spatial_gain[...].astype(F32).reshape(1, mixed.shape[1])
        for g in range(mixed.shape[1] // GROUP_WIDTH):
            span = slice(g * GROUP_WIDTH, (g + 1) * GROUP_WIDTH)
            v = gelu(jnp.dot(normed[...], v_full[:, span], preferred_element_type=F32))
            u = gelu(jnp.dot(normed[...], u_full[:, span], preferred_element_type=F32))
            v = v - jnp.mean(v, axis=-1, keepdims=True)
            v = v * lax.rsqrt(jnp.mean(v * v, axis=-1, keepdims=True) + 1e-05)
            v = (v * all_spatial_gain[:, span]).astype(BF16)
            weight = spatial_weight[g].astype(F32)
            weight = jnp.where(rows >= cols, weight, 0.0).astype(BF16)
            bias = spatial_bias[...][g : g + 1, :].astype(F32)
            bias = jnp.sum(jnp.where(rows == cols, bias, 0.0), axis=1, keepdims=True)
            for n in range(count // BLOCK):
                part = slice(n * BLOCK, (n + 1) * BLOCK)
                spatial = jnp.dot(weight, v[part], preferred_element_type=F32)
                spatial = spatial + bias
                mixed[part, span] = (u[part] * spatial).astype(BF16)

    load_tokens = lambda rows: tokens[rows, :]
    load_first = lambda rows: streams[0, rows, :]
    load_second = lambda rows: streams[1, rows, :]

    send_own(0)
    send_own(1)
    for w in range(6):
        own_copy(w).start()
    norm_rows(load_tokens, 0)

    for unit in range(5):
        relay(unit)
        send_own(unit + 2)
    wait_weight(0)
    wait_weight(1)
    hidden_units()
    relay(5)
    send_own(7)
    relay(6)
    send_own(8)
    send_own(9)
    wait_weight(2)
    project(0, hidden, down_full)
    relay(7)
    add_branch(0, load_tokens, 1, 0.5)
    relay(8)
    wait_put(0)
    norm_rows(load_first, 2)
    relay(9)
    wait_weight(3)
    wait_weight(4)
    mix()
    wait_weight(5)
    project(1, mixed, out_full)
    add_branch(1, load_first, 3, 1.0)
    wait_put(1)
    norm_rows(load_second, 4)
    hidden_units()
    project(2, hidden, down_full)
    add_branch(2, load_second, 5, 0.5)
    finish_sends()
    wait_put(2)
    last = pltpu.make_async_copy(streams.at[2], result, last_sem)
    last.start()
    for phase in range(3):
        finish_phase(phase)
    last.wait()


def shards(
    sizes,
    tokens,
    ffn_pre_gain,
    gate_weight,
    up_weight,
    down_weight,
    ffn_post_gain,
    mix_pre_gain,
    mix_u_weight,
    mix_v_weight,
    spatial_gain,
    spatial_weight,
    spatial_bias,
    mix_out_weight,
    mix_post_gain,
    late_pre_gain,
    late_post_gain,
):
    grp_n, fs_n, tp_n = sizes
    count, width = tokens.shape
    hidden_width = gate_weight.shape[1]
    channels = mix_u_weight.shape[1]
    columns = math.gcd(fs_n, 4)
    chips = tp_n // 2
    chunk = count // tp_n
    pieces = max(1, chunk // PIECE)
    vmem = pl.BlockSpec(memory_space=pltpu.VMEM)
    hbm = pl.BlockSpec(memory_space=pl.ANY)
    units = sum(SPLITS)
    dma = pltpu.SemaphoreType.DMA
    return pl.pallas_call(
        functools.partial(kernel, sizes),
        out_shape=jax.ShapeDtypeStruct((count, width), BF16),
        in_specs=[vmem] * 7 + [hbm, hbm, hbm, hbm, hbm, hbm, vmem, vmem, vmem],
        out_specs=hbm,
        scratch_shapes=[
            pltpu.VMEM((width, hidden_width), BF16),
            pltpu.VMEM((width, hidden_width), BF16),
            pltpu.VMEM((fs_n,) + down_weight.shape, BF16),
            pltpu.VMEM((width, channels), BF16),
            pltpu.VMEM((width, channels), BF16),
            pltpu.VMEM((fs_n,) + mix_out_weight.shape, BF16),
            pltpu.VMEM((count, width), BF16),
            pltpu.VMEM((count, hidden_width), BF16),
            pltpu.VMEM((count, channels), BF16),
            pltpu.VMEM((3, count, width), BF16),
            pltpu.VMEM((3, chips, chunk, width), BF16),
            pltpu.VMEM((3, chips, chunk, width), BF16),
            pltpu.VMEM((3, chips, chunk, width), BF16),
            pltpu.VMEM((3, count, width), BF16),
            dma((6,)),
            dma((units, fs_n)),
            dma((units, fs_n)),
            dma((units, fs_n)),
            dma((units, fs_n)),
            dma((units, 2, grp_n - 1, fs_n)),
            dma((units, 2, grp_n - 1, fs_n)),
            dma((3, columns, chips)),
            dma((3, columns, chips)),
            dma((3, columns, chips)),
            dma((3, columns, chips)),
            dma((3, pieces)),
            dma((3, pieces)),
            dma((3, pieces, chips)),
            dma((3, pieces, chips)),
            dma((3, pieces, chips)),
            dma((3, pieces, chips)),
            dma(()),
        ],
        compiler_params=pltpu.CompilerParams(
            collective_id=0, has_side_effects=True, vmem_limit_bytes=60 * 2**20
        ),
    )(
        tokens,
        ffn_pre_gain,
        ffn_post_gain,
        mix_pre_gain,
        mix_post_gain,
        late_pre_gain,
        late_post_gain,
        gate_weight,
        up_weight,
        down_weight,
        mix_u_weight,
        mix_v_weight,
        mix_out_weight,
        spatial_gain,
        spatial_weight,
        spatial_bias,
    )


FFN_PAIR = "far"
MIX_PAIR = "near"
PIECES = (2, 2, 2, 1, 1, 1)
AHEAD = 2
ROW_SPLIT = (2, 5)


def halves(size):
    small = size // 256 * 128
    return small, size - 2 * small


def weight_units(shapes, grp_n):
    units = []
    for group in ((0, 1), (2,), (3,), (4,), (5,)):
        made = []
        for w in group:
            rows, cols = shapes[w]
            split = w in ROW_SPLIT
            small, extra = halves(rows if split else cols)
            span = small if split else rows
            share = span // grp_n
            piece = share // PIECES[w]
            mine = []
            for n in range(PIECES[w]):
                width = cols if split else small
                mine.append((w, n * piece, share, piece, 0, width, False))
            if extra and split:
                mine.append((w, small, extra // grp_n, extra // grp_n, 0, cols, True))
            elif extra:
                mine.append((w, 0, rows // grp_n, rows // grp_n, small, extra, True))
            made.append(mine)
        for n in range(max(len(mine) for mine in made)):
            units += [mine[n] for mine in made if n < len(mine)]
    return units


def shared_kernel(
    sizes,
    units,
    tokens,
    gain0,
    gain1,
    gain2,
    gain3,
    gain4,
    gain5,
    gate_w,
    up_w,
    down_w,
    u_w,
    v_w,
    out_w,
    spatial_gain,
    spatial_weight,
    spatial_bias,
    result,
    gate_full,
    up_full,
    down_full,
    u_full,
    v_full,
    out_full,
    normed,
    hidden,
    mixed,
    streams,
    parts,
    paired,
    outgoing,
    landed,
    crossing,
    crossed,
    own_sem,
    fresh_send,
    relay_send,
    relay_recv,
    side_send,
    side_recv,
    pair_send,
    pair_recv,
    sum_send,
    sum_recv,
    cross_send,
    cross_recv,
    put_send,
    put_recv,
    last_sem,
):
    grp_n, fs_n, tp_n = sizes
    grp, fs, tp = lax.axis_index("grp"), lax.axis_index("fs"), lax.axis_index("tp")
    shards = (gate_w, up_w, down_w, u_w, v_w, out_w)
    fulls = (gate_full, up_full, down_full, u_full, v_full, out_full)
    count, width = tokens.shape
    chunk = count // tp_n
    chips = tp_n // 2
    chip, core = tp // 2, lax.rem(tp, 2)
    twin = tp + 1 - 2 * core
    across = (1 - chip) * 2 + core
    spot = core * chips + chip
    far_spot = core * chips + 1 - chip
    columns = pair_send.shape[2]
    column = width // columns
    piece_n = put_send.shape[2]
    piece_rows = chunk // piece_n
    all_gains = (gain0, gain1, gain2, gain3, gain4, gain5)
    middle = fs_n // 2

    class Near:
        half = lax.rem(fs, 2)
        partner = fs + 1 - 2 * lax.rem(fs, 2)
        reach = 2
        left_ok, right_ok = fs >= 2, fs + 2 < fs_n
        other_left, other_right = (fs >= 1, fs - 1), (fs + 1 < fs_n, fs + 1)

    class Far:
        half = fs // middle
        partner = lax.rem(fs + middle, fs_n)
        reach = 1
        left_ok, right_ok = lax.rem(fs, middle) > 0, lax.rem(fs, middle) < middle - 1
        other_left, other_right = (fs >= middle, middle - 1), (fs < middle, middle)

    named = {"near": Near, "far": Far}
    ffn, mixer = named[FFN_PAIR], named[MIX_PAIR]
    pairs = (ffn, ffn, ffn, mixer, mixer, mixer)
    phases = (ffn, mixer, ffn)

    barrier = pltpu.get_barrier_semaphore()
    for move in range(1, fs_n):
        pl.semaphore_signal(
            barrier, inc=1, device_id={"fs": lax.rem(fs + move, fs_n)}, device_id_type=MESH
        )
    for move in range(1, grp_n):
        pl.semaphore_signal(
            barrier, inc=1, device_id={"grp": lax.rem(grp + move, grp_n)}, device_id_type=MESH
        )
    for move in range(1, tp_n):
        pl.semaphore_signal(
            barrier, inc=1, device_id={"tp": lax.rem(tp + move, tp_n)}, device_id_type=MESH
        )
    pl.semaphore_wait(barrier, fs_n - 1 + grp_n - 1 + tp_n - 1)

    def large(half):
        return (half + core) % 2 == 0

    def half_start(w, half):
        small, extra = halves(shards[w].shape[0 if w in ROW_SPLIT else 1])
        return half * (small + extra * (1 - core))

    def view(unit, block):
        w, low, share, rows, col, cols, _ = units[unit]
        start = low + grp * share
        if w in ROW_SPLIT:
            return fulls[w].at[block, pl.ds(aligned(start, 16), rows), :]
        start = aligned(block * shards[w].shape[0] + start, 16)
        return fulls[w].at[pl.ds(start, rows), pl.ds(col, cols)]

    def shard_view(unit, half):
        w, low, share, rows, col, cols, _ = units[unit]
        start = low + grp * share
        base = half_start(w, half)
        if w in ROW_SPLIT:
            return shards[w].at[pl.ds(aligned(base + start, 16), rows), :]
        return shards[w].at[pl.ds(aligned(start, 16), rows), pl.ds(aligned(base + col, 128), cols)]

    def has(unit, half):
        return large(half) if units[unit][6] else True

    def own_copies(w):
        half = pairs[w].half
        base = half_start(w, half)
        small, extra = halves(shards[w].shape[0 if w in ROW_SPLIT else 1])

        def part(low, size, sem):
            if w in ROW_SPLIT:
                source = shards[w].at[pl.ds(aligned(base + low, 128), size), :]
                target = fulls[w].at[fs, pl.ds(low, size), :]
            else:
                rows = shards[w].shape[0]
                source = shards[w].at[:, pl.ds(aligned(base + low, 128), size)]
                target = fulls[w].at[pl.ds(aligned(fs * rows, 16), rows), pl.ds(low, size)]
            return pltpu.make_async_copy(source, target, own_sem.at[w, sem])

        made = [(True, part(0, small, 0))]
        if extra:
            made.append((large(half), part(small, extra, 1)))
        return made

    def guarded(ok, act):
        if ok is True:
            act()
        else:
            pl.when(ok)(act)

    def both(a, b):
        if a is True:
            return b
        if b is True:
            return a
        return a & b

    def fresh_copies(unit):
        pair = pairs[units[unit][0]]
        block = view(unit, fs)

        def made(slot, half, target):
            return pltpu.make_async_remote_copy(
                src_ref=shard_view(unit, half),
                dst_ref=block,
                send_sem=fresh_send.at[unit, slot],
                recv_sem=relay_recv.at[unit, fs],
                device_id={"fs": target},
                device_id_type=MESH,
            )

        own, other = pair.half, 1 - pair.half
        near, away = has(unit, own), has(unit, other)
        return (
            (both(pair.left_ok, near), lambda: made(0, own, fs - pair.reach)),
            (both(pair.right_ok, near), lambda: made(1, own, fs + pair.reach)),
            (both(pair.other_left[0], away), lambda: made(2, other, pair.other_left[1])),
            (both(pair.other_right[0], away), lambda: made(3, other, pair.other_right[1])),
        )

    def send_own(unit):
        if unit < len(units):
            for ok, copy in fresh_copies(unit):
                guarded(ok, lambda copy=copy: copy().start())

    def relay_copy(unit, block, leftward):
        pair = pairs[units[unit][0]]
        target = view(unit, block)
        return pltpu.make_async_remote_copy(
            src_ref=target,
            dst_ref=target,
            send_sem=relay_send.at[unit, block],
            recv_sem=relay_recv.at[unit, block],
            device_id={"fs": fs - pair.reach if leftward else fs + pair.reach},
            device_id_type=MESH,
        )

    def side_copy(unit, block, move):
        target = view(unit, block)
        return pltpu.make_async_remote_copy(
            src_ref=target,
            dst_ref=target,
            send_sem=side_send.at[unit, move - 1, block],
            recv_sem=side_recv.at[unit, move - 1, block],
            device_id={"grp": lax.rem(grp + move, grp_n)},
            device_id_type=MESH,
        )

    def over_blocks(unit, act):
        def whole():
            def step(d, carry):
                @pl.when(fs + d < fs_n)
                def _():
                    act(fs + d, True)

                @pl.when(fs >= d)
                def _():
                    act(fs - d, False)

                return carry

            lax.fori_loop(1, fs_n, step, 0)

        pair = pairs[units[unit][0]]
        guarded(has(unit, pair.half), whole)

    def relay(unit):
        pair = pairs[units[unit][0]]

        def act(block, leftward):
            relay_copy(unit, block, leftward).wait_recv()

            @pl.when(pair.left_ok if leftward else pair.right_ok)
            def _():
                relay_copy(unit, block, leftward).start()

            for move in range(1, grp_n):
                side_copy(unit, block, move).start()

        over_blocks(unit, act)
        send_own(unit + AHEAD)

    def wait_weight(w):
        for ok, copy in own_copies(w):
            guarded(ok, copy.wait)
        for unit in range(len(units)):
            if units[unit][0] == w:

                def act(block, leftward, unit=unit):
                    for move in range(1, grp_n):
                        side_copy(unit, block, move).wait_recv()

                over_blocks(unit, act)

    def finish_sends():
        for unit in range(len(units)):
            pair = pairs[units[unit][0]]
            for ok, copy in fresh_copies(unit):
                guarded(ok, lambda copy=copy: copy().wait_send())

            def act(block, leftward, unit=unit, pair=pair):
                @pl.when(pair.left_ok if leftward else pair.right_ok)
                def _():
                    relay_copy(unit, block, leftward).wait_send()

                for move in range(1, grp_n):
                    side_copy(unit, block, move).wait_send()

            over_blocks(unit, act)

    def column_span(col):
        return pl.ds(aligned(col * column, 128), column)

    def side_of(phase, turn):
        half = phases[phase].half
        return half + (1 - 2 * half) * (1 - turn)

    def pair_copy(phase, turn, col):
        span = column_span(col)
        low = side_of(phase, turn) * count + (1 - core) * (count // 2)
        return pltpu.make_async_remote_copy(
            src_ref=parts.at[phase, pl.ds(aligned(low, 16), count // 2), span],
            dst_ref=paired.at[phase, turn, :, span],
            send_sem=pair_send.at[phase, turn, col],
            recv_sem=pair_recv.at[phase, turn, col],
            device_id={"tp": twin},
            device_id_type=MESH,
        )

    def sum_copy(phase, turn, col):
        span = column_span(col)
        return pltpu.make_async_remote_copy(
            src_ref=outgoing.at[phase, turn, :, span],
            dst_ref=landed.at[phase, turn, :, span],
            send_sem=sum_send.at[phase, turn, col],
            recv_sem=sum_recv.at[phase, turn, col],
            device_id={"tp": across},
            device_id_type=MESH,
        )

    def cross_copy(phase, col):
        span = column_span(col)
        return pltpu.make_async_remote_copy(
            src_ref=crossing.at[phase, :, span],
            dst_ref=crossed.at[phase, :, span],
            send_sem=cross_send.at[phase, col],
            recv_sem=cross_recv.at[phase, col],
            device_id={"fs": phases[phase].partner},
            device_id_type=MESH,
        )

    def put_copy(phase, which, piece):
        half = phases[phase].half if phase < 3 else 0
        side = 1 - half if which in (3, 4, 6) else half
        place = far_spot if which in (5, 6) else spot
        start = side * count + place * chunk + piece * piece_rows
        rows = normed.at[phase, pl.ds(aligned(start, 16), piece_rows), :]
        if which in (0, 3):
            target = {"tp": across}
        elif which == 1:
            target = {"fs": phases[phase].partner}
        else:
            target = {"tp": twin}
        return pltpu.make_async_remote_copy(
            src_ref=rows,
            dst_ref=rows,
            send_sem=put_send.at[phase, which, piece],
            recv_sem=put_recv.at[phase, which, piece],
            device_id=target,
            device_id_type=MESH,
        )

    own_puts = ((1,), (0, 1, 2), (0, 1, 2), (0, 2))
    all_puts = ((1, 3, 4, 6), (0, 1, 2, 3, 4, 5, 6), (0, 1, 2, 3, 4, 5, 6), (0, 2, 5))

    def start_puts(phase, piece):
        for which in (1, 0, 2):
            if which in own_puts[phase]:
                put_copy(phase, which, piece).start()

    def pass_puts(phase):
        for piece in range(piece_n):
            if 1 in all_puts[phase]:
                put_copy(phase, 1, piece).wait_recv()
                put_copy(phase, 3, piece).start()
                put_copy(phase, 4, piece).start()
            if 0 in all_puts[phase]:
                put_copy(phase, 0, piece).wait_recv()
                put_copy(phase, 5, piece).start()
        for piece in range(piece_n):
            if 3 in all_puts[phase]:
                put_copy(phase, 3, piece).wait_recv()
                put_copy(phase, 6, piece).start()

    def wait_puts(phase):
        for which in (2, 4, 5, 6):
            if which in all_puts[phase]:
                for piece in range(piece_n):
                    put_copy(phase, which, piece).wait_recv()

    def finish_phase(phase):
        def step(col, carry):
            for turn in range(2):
                pair_copy(phase, turn, col).wait_send()
                sum_copy(phase, turn, col).wait_send()
            cross_copy(phase, col).wait_send()
            return carry

        lax.fori_loop(0, columns, step, 0)

    def finish_puts(phase):
        for which in all_puts[phase]:
            for piece in range(piece_n):
                put_copy(phase, which, piece).wait_send()

    def gain(row):
        return all_gains[row][...].astype(F32).reshape(1, width)

    def scaled(values, row):
        scale = lax.rsqrt(jnp.mean(values * values, axis=-1, keepdims=True) + 1e-06)
        return values * scale * gain(row)

    def norm_tokens(start, size):
        base = ffn.half * count

        def body(low):
            here = aligned(start + low, 16)
            values = tokens[pl.ds(here, 16), :].astype(F32)
            target = pl.ds(aligned(base + start + low, 16), 16)
            normed[0, target, :] = scaled(values, 0).astype(BF16)

        over_rows(size, 16, body)

    def pass_sum(phase, turn, col):
        span = column_span(col)
        pair_copy(phase, turn, col).wait_recv()
        low = side_of(phase, turn) * count + far_spot * chunk
        mine = parts[phase, pl.ds(aligned(low, 16), chunk), span].astype(F32)
        here = pl.ds(aligned((1 - chip) * chunk, 16), chunk)
        total = mine + paired[phase, turn, here, span].astype(F32)
        outgoing[phase, turn, :, span] = total.astype(BF16)
        sum_copy(phase, turn, col).start()

    def cross_sums(phase):
        def step(col, carry):
            span = column_span(col)
            sum_copy(phase, 0, col).wait_recv()
            low = side_of(phase, 0) * count + spot * chunk
            mine = parts[phase, pl.ds(aligned(low, 16), chunk), span].astype(F32)
            here = pl.ds(aligned(chip * chunk, 16), chunk)
            total = mine + paired[phase, 0, here, span].astype(F32)
            total = total + landed[phase, 0, :, span].astype(F32)
            crossing[phase, :, span] = total.astype(BF16)
            cross_copy(phase, col).start()
            return carry

        lax.fori_loop(0, columns, step, 0)

    def add_branch(phase, load, row, factor):
        def wait(col, carry):
            sum_copy(phase, 1, col).wait_recv()
            cross_copy(phase, col).wait_recv()
            return carry

        lax.fori_loop(0, columns, wait, 0)
        half = phases[phase].half
        after = phases[phase + 1].half if phase < 2 else 0
        for piece in range(piece_n):

            def body(low, piece=piece):
                inside = aligned(piece * piece_rows + low, 16)
                rows = pl.ds(inside, 16)
                low = half * count + spot * chunk + inside
                total = parts[phase, pl.ds(aligned(low, 16), 16), :].astype(F32)
                here = pl.ds(aligned(chip * chunk + inside, 16), 16)
                total = total + paired[phase, 1, here, :].astype(F32)
                total = total + landed[phase, 1, rows, :].astype(F32)
                total = total + crossed[phase, rows, :].astype(F32)
                value = load(inside).astype(F32) + factor * scaled(total, row)
                value = value.astype(BF16)
                target = pl.ds(aligned(after * count + spot * chunk + inside, 16), 16)
                if phase < 2:
                    streams[phase, rows, :] = value
                    value = scaled(value.astype(F32), row + 1).astype(BF16)
                normed[phase + 1, target, :] = value

            over_rows(piece_rows, 16, body)
            start_puts(phase + 1, piece)

    def hidden_tile(phase, rows, cols):
        left = normed[phase, rows, :]
        gate = jnp.dot(left, gate_full[:, cols], preferred_element_type=F32)
        upper = jnp.dot(left, up_full[:, cols], preferred_element_type=F32)
        hidden[rows, cols] = (gate / (1.0 + jnp.exp(-gate)) * upper).astype(BF16)

    def hidden_half(phase, side):
        rows = pl.ds(aligned(side * count, 16), count)
        over_tiles(hidden.shape[1], lambda low, size: hidden_tile(phase, rows, pl.ds(low, size)))

    def project(phase, left, right):
        def step(i, carry):
            turn, col = i // columns, lax.rem(i, columns)
            rows = pl.ds(aligned(side_of(phase, turn) * count, 16), count)
            per = fs_n // columns
            terms = [
                jnp.dot(left[rows, :], right[col * per + b], preferred_element_type=F32)
                for b in range(per)
            ]
            terms = terms[0] if per == 1 else jnp.concatenate(terms, axis=1)
            parts[phase, rows, column_span(col)] = terms.astype(BF16)
            pair_copy(phase, turn, col).start()

            @pl.when(i > 0)
            def _():
                pass_sum(phase, (i - 1) // columns, lax.rem(i - 1, columns))

            return carry

        lax.fori_loop(0, 2 * columns, step, 0)
        pass_sum(phase, 1, columns - 1)

    def mix(side):
        at = lax.broadcasted_iota(jnp.int32, (BLOCK, BLOCK), 0)
        to = lax.broadcasted_iota(jnp.int32, (BLOCK, BLOCK), 1)
        half = mixer.half
        here = mixed.shape[1]
        groups = here // GROUP_WIDTH
        all_gain = spatial_gain[...].astype(F32).reshape(1, 2 * here)
        all_gain = jnp.where(half == 0, all_gain[:, :here], all_gain[:, here:])
        all_bias = spatial_bias[...].astype(F32)
        all_bias = jnp.where(half == 0, all_bias[:groups], all_bias[groups:])

        def block(n, carry):
            rows = pl.ds(aligned(side * count + n * BLOCK, 16), BLOCK)
            left = normed[1, rows, :]
            every_v = gelu(jnp.dot(left, v_full[...], preferred_element_type=F32))
            every_u = gelu(jnp.dot(left, u_full[...], preferred_element_type=F32))
            for g in range(groups):
                span = slice(g * GROUP_WIDTH, (g + 1) * GROUP_WIDTH)
                v = every_v[:, span]
                v = v - jnp.mean(v, axis=-1, keepdims=True)
                v = v * lax.rsqrt(jnp.mean(v * v, axis=-1, keepdims=True) + 1e-05)
                v = (v * all_gain[:, span]).astype(BF16)
                weight = spatial_weight[half * groups + g].astype(F32)
                weight = jnp.where(at >= to, weight, 0.0).astype(BF16)
                bias = jnp.where(at == to, all_bias[g : g + 1, :], 0.0)
                bias = jnp.sum(bias, axis=1, keepdims=True)
                spatial = jnp.dot(weight, v, preferred_element_type=F32) + bias
                mixed[rows, span] = (every_u[:, span] * spatial).astype(BF16)
            return carry

        lax.fori_loop(0, count // BLOCK, block, 0)

    def load_tokens(low):
        return tokens[pl.ds(aligned(spot * chunk + low, 16), 16), :]

    def load_stream(phase):
        return lambda low: streams[phase, pl.ds(low, 16), :]

    last = [unit for unit in range(len(units)) if units[unit][0] < 2][-1]
    downs = [unit for unit in range(len(units)) if units[unit][0] == 2]
    first = [unit for unit in range(len(units)) if units[unit][0] == 3]
    second = [unit for unit in range(len(units)) if units[unit][0] == 4]
    third = [unit for unit in range(len(units)) if units[unit][0] == 5]

    def relays(some):
        for unit in some:
            relay(unit)

    for unit in range(AHEAD):
        send_own(unit)
    for w in range(6):
        for ok, copy in own_copies(w):
            guarded(ok, copy.start)
    norm_tokens(spot * chunk, chunk)
    for piece in range(piece_n):
        start_puts(0, piece)

    small, extra = halves(gate_w.shape[1])
    if extra:

        @pl.when(jnp.logical_not(large(ffn.half)))
        def _():
            for full in (gate_full, up_full):
                full[:, pl.ds(small, extra)] = jnp.zeros((full.shape[0], extra), BF16)
            pad = jnp.zeros((fs_n, extra, down_full.shape[2]), BF16)
            down_full[:, pl.ds(small, extra), :] = pad

    for move in range(1, tp_n):
        norm_tokens(lax.rem(spot + move, tp_n) * chunk, chunk)

    relay(0)
    pass_puts(0)
    relays(range(1, last + 1))
    wait_puts(0)
    wait_weight(0)
    wait_weight(1)
    relay(downs[0])
    hidden_half(0, ffn.half)
    relays(downs[1:2])
    hidden_half(0, 1 - ffn.half)
    relays(downs[2:])
    wait_weight(2)
    project(0, hidden, down_full)
    relays(first)
    cross_sums(0)
    relays(second)
    add_branch(0, load_tokens, 1, 0.5)
    relays(third)
    pass_puts(1)
    wait_weight(3)
    wait_weight(4)
    wait_puts(1)
    mix(mixer.half)
    mix(1 - mixer.half)
    wait_weight(5)
    project(1, mixed, out_full)
    cross_sums(1)
    add_branch(1, load_stream(0), 3, 1.0)
    pass_puts(2)
    wait_puts(2)
    hidden_half(2, ffn.half)
    hidden_half(2, 1 - ffn.half)
    project(2, hidden, down_full)
    cross_sums(2)
    add_branch(2, load_stream(1), 5, 0.5)
    pass_puts(3)
    finish_sends()
    for phase in range(3):
        finish_phase(phase)
        finish_puts(phase)
    wait_puts(3)
    copy = pltpu.make_async_copy(normed.at[3, pl.ds(0, count), :], result, last_sem)
    copy.start()
    finish_puts(3)
    copy.wait()


def shared(
    sizes,
    tokens,
    ffn_pre_gain,
    gate_weight,
    up_weight,
    down_weight,
    ffn_post_gain,
    mix_pre_gain,
    mix_u_weight,
    mix_v_weight,
    spatial_gain,
    spatial_weight,
    spatial_bias,
    mix_out_weight,
    mix_post_gain,
    late_pre_gain,
    late_post_gain,
):
    grp_n, fs_n, tp_n = sizes
    count, width = tokens.shape
    small, extra = halves(gate_weight.shape[1])
    hidden_width = small + extra
    channels = mix_u_weight.shape[1] // 2
    columns = math.gcd(fs_n, 4)
    chunk = count // tp_n
    pieces = max(1, chunk // PIECE)
    vmem = pl.BlockSpec(memory_space=pltpu.VMEM)
    hbm = pl.BlockSpec(memory_space=pl.ANY)
    weights = (gate_weight, up_weight, down_weight, mix_u_weight, mix_v_weight, mix_out_weight)
    units = weight_units([w.shape for w in weights], grp_n)
    unit_n = len(units)
    dma = pltpu.SemaphoreType.DMA
    return pl.pallas_call(
        functools.partial(shared_kernel, sizes, units),
        out_shape=jax.ShapeDtypeStruct((count, width), BF16),
        in_specs=[vmem] * 7 + [hbm, hbm, hbm, hbm, hbm, hbm, vmem, vmem, vmem],
        out_specs=hbm,
        scratch_shapes=[
            pltpu.VMEM((width, hidden_width), BF16),
            pltpu.VMEM((width, hidden_width), BF16),
            pltpu.VMEM((fs_n, hidden_width, down_weight.shape[1]), BF16),
            pltpu.VMEM((width, channels), BF16),
            pltpu.VMEM((width, channels), BF16),
            pltpu.VMEM((fs_n, channels, mix_out_weight.shape[1]), BF16),
            pltpu.VMEM((4, 2 * count, width), BF16),
            pltpu.VMEM((2 * count, hidden_width), BF16),
            pltpu.VMEM((2 * count, channels), BF16),
            pltpu.VMEM((2, chunk, width), BF16),
            pltpu.VMEM((3, 2 * count, width), BF16),
            pltpu.VMEM((3, 2, count // 2, width), BF16),
            pltpu.VMEM((3, 2, chunk, width), BF16),
            pltpu.VMEM((3, 2, chunk, width), BF16),
            pltpu.VMEM((3, chunk, width), BF16),
            pltpu.VMEM((3, chunk, width), BF16),
            dma((6, 2)),
            dma((unit_n, 4)),
            dma((unit_n, fs_n)),
            dma((unit_n, fs_n)),
            dma((unit_n, max(1, grp_n - 1), fs_n)),
            dma((unit_n, max(1, grp_n - 1), fs_n)),
            dma((3, 2, columns)),
            dma((3, 2, columns)),
            dma((3, 2, columns)),
            dma((3, 2, columns)),
            dma((3, columns)),
            dma((3, columns)),
            dma((4, 7, pieces)),
            dma((4, 7, pieces)),
            dma(()),
        ],
        compiler_params=pltpu.CompilerParams(
            collective_id=0, has_side_effects=True, vmem_limit_bytes=60 * 2**20
        ),
    )(
        tokens,
        ffn_pre_gain,
        ffn_post_gain,
        mix_pre_gain,
        mix_post_gain,
        late_pre_gain,
        late_post_gain,
        gate_weight,
        up_weight,
        down_weight,
        mix_u_weight,
        mix_v_weight,
        mix_out_weight,
        spatial_gain,
        spatial_weight,
        spatial_bias,
    )


def can_share(sizes, tokens, gate_weight, mix_u_weight):
    grp_n, fs_n, tp_n = sizes
    count = tokens.shape[0] // (grp_n * fs_n)
    rows = gate_weight.shape[0] // fs_n
    hidden_width = gate_weight.shape[1] // tp_n
    channels = mix_u_weight.shape[1] // tp_n
    return (
        tp_n == 4
        and fs_n == 4
        and count % (4 * PIECE) == 0
        and rows % (32 * grp_n) == 0
        and hidden_width % 128 == 0
        and halves(hidden_width)[0] % (32 * grp_n) == 0
        and channels % (2 * GROUP_WIDTH) == 0
    )


def solution(mesh):
    in_specs = (
        P(("grp", "fs"), None),
        P(),
        P("fs", "tp"),
        P("fs", "tp"),
        P("tp", "fs"),
        P(),
        P(),
        P("fs", "tp"),
        P("fs", "tp"),
        P("tp"),
        P("tp", None, None),
        P("tp", None),
        P("tp", "fs"),
        P(),
        P(),
        P(),
    )
    out_specs = P(("grp", "fs"), None)
    sizes = (mesh.shape["grp"], mesh.shape["fs"], mesh.shape["tp"])

    def step(*arrays):
        plan = shared if can_share(sizes, arrays[0], arrays[2], arrays[7]) else shards
        body = functools.partial(plan, sizes)
        return jax.shard_map(
            body, mesh=mesh, in_specs=in_specs, out_specs=out_specs, check_vma=False
        )(*arrays)

    return step
```

```python
import functools
import math

import jax
import jax.numpy as jnp
from jax import lax
from jax.experimental import pallas as pl
from jax.experimental.pallas import tpu as pltpu
from jax.sharding import PartitionSpec as P

GROUP_WIDTH = 128
BLOCK = 128
TILE = 256
F32 = jnp.float32
BF16 = jnp.bfloat16
MESH = pl.DeviceIdType.MESH
SPLITS = (2, 2, 2, 1, 1, 2)
PIECE = 32


def aligned(value, unit):
    return value if isinstance(value, int) else pl.multiple_of(value, unit)


def over_tiles(width, body):
    count = width // TILE

    def step(i, carry):
        body(pl.multiple_of(i * TILE, TILE), TILE)
        return carry

    lax.fori_loop(0, count, step, 0)
    if width % TILE:
        body(count * TILE, width % TILE)


def over_rows(count, size, body):
    def step(i, carry):
        body(pl.multiple_of(i * size, size))
        return carry

    lax.fori_loop(0, count // size, step, 0)


def gelu(a):
    return 0.5 * a * (1.0 + lax.erf(a * (2.0**-0.5)))


def kernel(
    sizes,
    tokens,
    gain0,
    gain1,
    gain2,
    gain3,
    gain4,
    gain5,
    gate_w,
    up_w,
    down_w,
    u_w,
    v_w,
    out_w,
    spatial_gain,
    spatial_weight,
    spatial_bias,
    result,
    gate_full,
    up_full,
    down_full,
    u_full,
    v_full,
    out_full,
    normed,
    hidden,
    mixed,
    parts,
    paired,
    outgoing,
    landed,
    streams,
    own_sem,
    left_send,
    left_recv,
    right_send,
    right_recv,
    side_send,
    side_recv,
    pair_send,
    pair_recv,
    sum_send,
    sum_recv,
    twin_send,
    twin_recv,
    put_send,
    put_recv,
    pass_send,
    pass_recv,
    last_sem,
):
    grp_n, fs_n, tp_n = sizes
    grp, fs, tp = lax.axis_index("grp"), lax.axis_index("fs"), lax.axis_index("tp")
    shards = (gate_w, up_w, down_w, u_w, v_w, out_w)
    fulls = (gate_full, up_full, down_full, u_full, v_full, out_full)
    count, width = tokens.shape
    chunk = count // tp_n
    chips = tp_n // 2
    chip, core = tp // 2, lax.rem(tp, 2)
    twin = tp + 1 - 2 * core
    columns = pair_send.shape[1]
    column = width // columns
    piece_n = put_send.shape[1]
    piece_rows = chunk // piece_n
    all_gains = (gain0, gain1, gain2, gain3, gain4, gain5)

    barrier = pltpu.get_barrier_semaphore()
    for move in (1, fs_n - 1):
        pl.semaphore_signal(
            barrier, inc=1, device_id={"fs": lax.rem(fs + move, fs_n)}, device_id_type=MESH
        )
    for move in range(1, grp_n):
        pl.semaphore_signal(
            barrier, inc=1, device_id={"grp": lax.rem(grp + move, grp_n)}, device_id_type=MESH
        )
    for move in range(1, tp_n):
        pl.semaphore_signal(
            barrier, inc=1, device_id={"tp": lax.rem(tp + move, tp_n)}, device_id_type=MESH
        )
    pl.semaphore_wait(barrier, 2 + grp_n - 1 + tp_n - 1)

    units = []
    for w in range(6):
        piece = shards[w].shape[0] // grp_n // SPLITS[w]
        for s in range(SPLITS[w]):
            units.append((w, s * piece, piece))

    def unit_rows(unit):
        w, low, piece = units[unit]
        return aligned(grp * (shards[w].shape[0] // grp_n) + low, 16), piece

    def place(w, block, low, piece):
        if w in (2, 5):
            return fulls[w].at[block, pl.ds(low, piece), :]
        start = aligned(block * shards[w].shape[0] + low, 16)
        return fulls[w].at[pl.ds(start, piece), :]

    def own_copy(w):
        return pltpu.make_async_copy(
            shards[w], place(w, fs, 0, shards[w].shape[0]), own_sem.at[w]
        )

    def to_right(unit, hop, own=False):
        w = units[unit][0]
        low, piece = unit_rows(unit)
        target = place(w, fs - hop, low, piece)
        source = shards[w].at[pl.ds(low, piece), :] if own else target
        return pltpu.make_async_remote_copy(
            src_ref=source,
            dst_ref=target,
            send_sem=right_send.at[unit, hop],
            recv_sem=right_recv.at[unit, hop],
            device_id={"fs": fs + 1},
            device_id_type=MESH,
        )

    def to_left(unit, hop, own=False):
        w = units[unit][0]
        low, piece = unit_rows(unit)
        target = place(w, fs + hop, low, piece)
        source = shards[w].at[pl.ds(low, piece), :] if own else target
        return pltpu.make_async_remote_copy(
            src_ref=source,
            dst_ref=target,
            send_sem=left_send.at[unit, hop],
            recv_sem=left_recv.at[unit, hop],
            device_id={"fs": fs - 1},
            device_id_type=MESH,
        )

    def to_side(unit, side, hop, move):
        w = units[unit][0]
        low, piece = unit_rows(unit)
        block = fs - hop if side == 0 else fs + hop
        target = place(w, block, low, piece)
        return pltpu.make_async_remote_copy(
            src_ref=target,
            dst_ref=target,
            send_sem=side_send.at[unit, side, move - 1, hop],
            recv_sem=side_recv.at[unit, side, move - 1, hop],
            device_id={"grp": lax.rem(grp + move, grp_n)},
            device_id_type=MESH,
        )

    def send_own(unit):
        if unit >= len(units):
            return

        @pl.when(fs < fs_n - 1)
        def _():
            to_right(unit, 0, own=True).start()

        @pl.when(fs > 0)
        def _():
            to_left(unit, 0, own=True).start()

    def relay(unit):
        def step(hop, carry):
            @pl.when(fs >= hop)
            def _():
                to_right(unit, hop - 1).wait_recv()

                @pl.when(fs < fs_n - 1)
                def _():
                    to_right(unit, hop).start()

                for move in range(1, grp_n):
                    to_side(unit, 0, hop, move).start()

            @pl.when(fs + hop < fs_n)
            def _():
                to_left(unit, hop - 1).wait_recv()

                @pl.when(fs > 0)
                def _():
                    to_left(unit, hop).start()

                for move in range(1, grp_n):
                    to_side(unit, 1, hop, move).start()

            return carry

        lax.fori_loop(1, fs_n, step, 0)

    def wait_weight(w):
        own_copy(w).wait()
        for unit in range(len(units)):
            if units[unit][0] == w:

                def step(hop, carry, unit=unit):
                    for move in range(1, grp_n):

                        @pl.when(fs >= hop)
                        def _():
                            to_side(unit, 0, hop, move).wait_recv()

                        @pl.when(fs + hop < fs_n)
                        def _():
                            to_side(unit, 1, hop, move).wait_recv()

                    return carry

                lax.fori_loop(1, fs_n, step, 0)

    def finish_sends():
        for unit in range(len(units)):

            def step(hop, carry, unit=unit):
                @pl.when((fs >= hop) & (fs < fs_n - 1))
                def _():
                    to_right(unit, hop).wait_send()

                @pl.when((fs + hop < fs_n) & (fs > 0))
                def _():
                    to_left(unit, hop).wait_send()

                @pl.when(hop > 0)
                def _():
                    for move in range(1, grp_n):

                        @pl.when(fs >= hop)
                        def _():
                            to_side(unit, 0, hop, move).wait_send()

                        @pl.when(fs + hop < fs_n)
                        def _():
                            to_side(unit, 1, hop, move).wait_send()

                return carry

            lax.fori_loop(0, fs_n, step, 0)

    def other(move, which):
        return lax.rem(chip + move, chips) * 2 + which

    def origin(move, which):
        return lax.rem(chip + chips - move, chips) * 2 + which

    def chunk_rows(owner):
        return pl.ds(aligned(owner * chunk, 16), chunk)

    def column_span(col):
        return pl.ds(aligned(col * column, 128), column)

    def pair_copy(phase, col, move):
        span = column_span(col)
        return pltpu.make_async_remote_copy(
            src_ref=parts.at[phase, chunk_rows(other(move, 1 - core)), span],
            dst_ref=paired.at[phase, move, :, span],
            send_sem=pair_send.at[phase, col, move],
            recv_sem=pair_recv.at[phase, col, move],
            device_id={"tp": twin},
            device_id_type=MESH,
        )

    def sum_copy(phase, col, move):
        span = column_span(col)
        return pltpu.make_async_remote_copy(
            src_ref=outgoing.at[phase, move, :, span],
            dst_ref=landed.at[phase, move, :, span],
            send_sem=sum_send.at[phase, col, move],
            recv_sem=sum_recv.at[phase, col, move],
            device_id={"tp": other(move, core)},
            device_id_type=MESH,
        )

    def piece_span(owner, piece):
        return pl.ds(aligned(owner * chunk + piece * piece_rows, 16), piece_rows)

    def twin_copy(phase, piece):
        rows = piece_span(tp, piece)
        return pltpu.make_async_remote_copy(
            src_ref=streams.at[phase, rows, :],
            dst_ref=streams.at[phase, rows, :],
            send_sem=twin_send.at[phase, piece],
            recv_sem=twin_recv.at[phase, piece],
            device_id={"tp": twin},
            device_id_type=MESH,
        )

    def put_copy(phase, piece, move):
        rows = piece_span(tp, piece)
        return pltpu.make_async_remote_copy(
            src_ref=streams.at[phase, rows, :],
            dst_ref=streams.at[phase, rows, :],
            send_sem=put_send.at[phase, piece, move],
            recv_sem=put_recv.at[phase, piece, move],
            device_id={"tp": other(move, core)},
            device_id_type=MESH,
        )

    def pass_copy(phase, piece, move):
        rows = piece_span(origin(move, core), piece)
        return pltpu.make_async_remote_copy(
            src_ref=streams.at[phase, rows, :],
            dst_ref=streams.at[phase, rows, :],
            send_sem=pass_send.at[phase, piece, move],
            recv_sem=pass_recv.at[phase, piece, move],
            device_id={"tp": twin},
            device_id_type=MESH,
        )

    def gain(row):
        return all_gains[row][...].astype(F32).reshape(1, width)

    def norm_rows(load, row):
        def body(low):
            values = load(pl.ds(low, 32)).astype(F32)
            scale = lax.rsqrt(jnp.mean(values * values, axis=-1, keepdims=True) + 1e-06)
            normed[pl.ds(low, 32), :] = (values * scale * gain(row)).astype(BF16)

        over_rows(count, 32, body)

    def start_sums(phase, col):
        for move in range(1, chips):
            pair_copy(phase, col, move).wait_recv()
            span = column_span(col)
            mine = parts[phase, chunk_rows(other(move, core)), span].astype(F32)
            both = mine + paired[phase, move, :, span].astype(F32)
            outgoing[phase, move, :, span] = both.astype(BF16)
            sum_copy(phase, col, move).start()

    def add_branch(phase, load, row, factor):
        for col in range(columns):
            pair_copy(phase, col, 0).wait_recv()
            for move in range(1, chips):
                sum_copy(phase, col, move).wait_recv()
        for piece in range(piece_n):

            def body(low, piece=piece):
                here = pl.ds(aligned(piece * piece_rows + low, 16), 16)
                rows = pl.ds(aligned(tp * chunk + piece * piece_rows + low, 16), 16)
                total = parts[phase, rows, :].astype(F32) + paired[phase, 0, here, :].astype(F32)
                for move in range(1, chips):
                    total = total + landed[phase, move, here, :].astype(F32)
                scale = lax.rsqrt(jnp.mean(total * total, axis=-1, keepdims=True) + 1e-06)
                branch = total * scale * gain(row)
                streams[phase, rows, :] = (load(rows).astype(F32) + factor * branch).astype(BF16)

            over_rows(piece_rows, 16, body)
            for move in range(1, chips):
                put_copy(phase, piece, move).start()
            twin_copy(phase, piece).start()

    def wait_put(phase):
        for piece in range(piece_n):
            for move in range(1, chips):
                put_copy(phase, piece, move).wait_recv()
                pass_copy(phase, piece, move).start()
        for piece in range(piece_n):
            twin_copy(phase, piece).wait_recv()
            for move in range(1, chips):
                pass_copy(phase, piece, move).wait_recv()

    def finish_phase(phase):
        for col in range(columns):
            for move in range(chips):
                pair_copy(phase, col, move).wait_send()
            for move in range(1, chips):
                sum_copy(phase, col, move).wait_send()
        for piece in range(piece_n):
            twin_copy(phase, piece).wait_send()
            for move in range(1, chips):
                put_copy(phase, piece, move).wait_send()
                pass_copy(phase, piece, move).wait_send()

    def hidden_units():
        def body(low, size):
            cols = pl.ds(low, size)
            gate = jnp.dot(normed[...], gate_full[:, cols], preferred_element_type=F32)
            upper = jnp.dot(normed[...], up_full[:, cols], preferred_element_type=F32)
            hidden[:, cols] = (gate / (1.0 + jnp.exp(-gate)) * upper).astype(BF16)

        over_tiles(hidden.shape[1], body)

    def project(phase, left, right):
        blocks = fs_n // columns

        def step(col, carry):
            terms = [
                jnp.dot(left[...], right[col * blocks + b], preferred_element_type=F32)
                for b in range(blocks)
            ]
            terms = terms[0] if blocks == 1 else jnp.concatenate(terms, axis=1)
            parts[phase, :, column_span(col)] = terms.astype(BF16)
            for move in range(chips - 1, -1, -1):
                pair_copy(phase, col, move).start()

            @pl.when(col > 0)
            def _():
                start_sums(phase, col - 1)

            return carry

        lax.fori_loop(0, columns, step, 0)
        start_sums(phase, columns - 1)

    def mix():
        rows = lax.broadcasted_iota(jnp.int32, (BLOCK, BLOCK), 0)
        cols = lax.broadcasted_iota(jnp.int32, (BLOCK, BLOCK), 1)
        all_spatial_gain = spatial_gain[...].astype(F32).reshape(1, mixed.shape[1])
        for g in range(mixed.shape[1] // GROUP_WIDTH):
            span = slice(g * GROUP_WIDTH, (g + 1) * GROUP_WIDTH)
            v = gelu(jnp.dot(normed[...], v_full[:, span], preferred_element_type=F32))
            u = gelu(jnp.dot(normed[...], u_full[:, span], preferred_element_type=F32))
            v = v - jnp.mean(v, axis=-1, keepdims=True)
            v = v * lax.rsqrt(jnp.mean(v * v, axis=-1, keepdims=True) + 1e-05)
            v = (v * all_spatial_gain[:, span]).astype(BF16)
            weight = spatial_weight[g].astype(F32)
            weight = jnp.where(rows >= cols, weight, 0.0).astype(BF16)
            bias = spatial_bias[...][g : g + 1, :].astype(F32)
            bias = jnp.sum(jnp.where(rows == cols, bias, 0.0), axis=1, keepdims=True)
            for n in range(count // BLOCK):
                part = slice(n * BLOCK, (n + 1) * BLOCK)
                spatial = jnp.dot(weight, v[part], preferred_element_type=F32)
                spatial = spatial + bias
                mixed[part, span] = (u[part] * spatial).astype(BF16)

    load_tokens = lambda rows: tokens[rows, :]
    load_first = lambda rows: streams[0, rows, :]
    load_second = lambda rows: streams[1, rows, :]

    send_own(0)
    send_own(1)
    for w in range(6):
        own_copy(w).start()
    norm_rows(load_tokens, 0)

    for unit in range(5):
        relay(unit)
        send_own(unit + 2)
    wait_weight(0)
    wait_weight(1)
    hidden_units()
    relay(5)
    send_own(7)
    relay(6)
    send_own(8)
    send_own(9)
    wait_weight(2)
    project(0, hidden, down_full)
    relay(7)
    add_branch(0, load_tokens, 1, 0.5)
    relay(8)
    wait_put(0)
    norm_rows(load_first, 2)
    relay(9)
    wait_weight(3)
    wait_weight(4)
    mix()
    wait_weight(5)
    project(1, mixed, out_full)
    add_branch(1, load_first, 3, 1.0)
    wait_put(1)
    norm_rows(load_second, 4)
    hidden_units()
    project(2, hidden, down_full)
    add_branch(2, load_second, 5, 0.5)
    finish_sends()
    wait_put(2)
    last = pltpu.make_async_copy(streams.at[2], result, last_sem)
    last.start()
    for phase in range(3):
        finish_phase(phase)
    last.wait()


def shards(
    sizes,
    tokens,
    ffn_pre_gain,
    gate_weight,
    up_weight,
    down_weight,
    ffn_post_gain,
    mix_pre_gain,
    mix_u_weight,
    mix_v_weight,
    spatial_gain,
    spatial_weight,
    spatial_bias,
    mix_out_weight,
    mix_post_gain,
    late_pre_gain,
    late_post_gain,
):
    grp_n, fs_n, tp_n = sizes
    count, width = tokens.shape
    hidden_width = gate_weight.shape[1]
    channels = mix_u_weight.shape[1]
    columns = math.gcd(fs_n, 4)
    chips = tp_n // 2
    chunk = count // tp_n
    pieces = max(1, chunk // PIECE)
    vmem = pl.BlockSpec(memory_space=pltpu.VMEM)
    hbm = pl.BlockSpec(memory_space=pl.ANY)
    units = sum(SPLITS)
    dma = pltpu.SemaphoreType.DMA
    return pl.pallas_call(
        functools.partial(kernel, sizes),
        out_shape=jax.ShapeDtypeStruct((count, width), BF16),
        in_specs=[vmem] * 7 + [hbm, hbm, hbm, hbm, hbm, hbm, vmem, vmem, vmem],
        out_specs=hbm,
        scratch_shapes=[
            pltpu.VMEM((width, hidden_width), BF16),
            pltpu.VMEM((width, hidden_width), BF16),
            pltpu.VMEM((fs_n,) + down_weight.shape, BF16),
            pltpu.VMEM((width, channels), BF16),
            pltpu.VMEM((width, channels), BF16),
            pltpu.VMEM((fs_n,) + mix_out_weight.shape, BF16),
            pltpu.VMEM((count, width), BF16),
            pltpu.VMEM((count, hidden_width), BF16),
            pltpu.VMEM((count, channels), BF16),
            pltpu.VMEM((3, count, width), BF16),
            pltpu.VMEM((3, chips, chunk, width), BF16),
            pltpu.VMEM((3, chips, chunk, width), BF16),
            pltpu.VMEM((3, chips, chunk, width), BF16),
            pltpu.VMEM((3, count, width), BF16),
            dma((6,)),
            dma((units, fs_n)),
            dma((units, fs_n)),
            dma((units, fs_n)),
            dma((units, fs_n)),
            dma((units, 2, grp_n - 1, fs_n)),
            dma((units, 2, grp_n - 1, fs_n)),
            dma((3, columns, chips)),
            dma((3, columns, chips)),
            dma((3, columns, chips)),
            dma((3, columns, chips)),
            dma((3, pieces)),
            dma((3, pieces)),
            dma((3, pieces, chips)),
            dma((3, pieces, chips)),
            dma((3, pieces, chips)),
            dma((3, pieces, chips)),
            dma(()),
        ],
        compiler_params=pltpu.CompilerParams(
            collective_id=0, has_side_effects=True, vmem_limit_bytes=60 * 2**20
        ),
    )(
        tokens,
        ffn_pre_gain,
        ffn_post_gain,
        mix_pre_gain,
        mix_post_gain,
        late_pre_gain,
        late_post_gain,
        gate_weight,
        up_weight,
        down_weight,
        mix_u_weight,
        mix_v_weight,
        mix_out_weight,
        spatial_gain,
        spatial_weight,
        spatial_bias,
    )


FFN_PAIR = "far"
MIX_PAIR = "near"
PIECES = (2, 2, 2, 1, 1, 1)
AHEAD = 3
LAG = 2
ROW_SPLIT = (2, 5)


def halves(size):
    small = size // 256 * 128
    return small, size - 2 * small


def weight_units(shapes, grp_n):
    units = []
    for group in ((0, 1), (2,), (3,), (4,), (5,)):
        made = []
        for w in group:
            rows, cols = shapes[w]
            split = w in ROW_SPLIT
            small, extra = halves(rows if split else cols)
            span = small if split else rows
            share = span // grp_n
            piece = share // PIECES[w]
            mine = []
            for n in range(PIECES[w]):
                width = cols if split else small
                mine.append((w, n * piece, share, piece, 0, width, False))
            if extra and split:
                mine.append((w, small, extra // grp_n, extra // grp_n, 0, cols, True))
            elif extra:
                mine.append((w, 0, rows // grp_n, rows // grp_n, small, extra, True))
            made.append(mine)
        for n in range(max(len(mine) for mine in made)):
            units += [mine[n] for mine in made if n < len(mine)]
    return units


def shared_kernel(
    sizes,
    units,
    tokens,
    gain0,
    gain1,
    gain2,
    gain3,
    gain4,
    gain5,
    gate_w,
    up_w,
    down_w,
    u_w,
    v_w,
    out_w,
    spatial_gain,
    spatial_weight,
    spatial_bias,
    result,
    gate_full,
    up_full,
    down_full,
    u_full,
    v_full,
    out_full,
    normed,
    hidden,
    mixed,
    streams,
    parts,
    paired,
    outgoing,
    landed,
    crossing,
    crossed,
    own_sem,
    fresh_send,
    relay_send,
    relay_recv,
    side_send,
    side_recv,
    pair_send,
    pair_recv,
    sum_send,
    sum_recv,
    cross_send,
    cross_recv,
    put_send,
    put_recv,
    last_sem,
):
    grp_n, fs_n, tp_n = sizes
    grp, fs, tp = lax.axis_index("grp"), lax.axis_index("fs"), lax.axis_index("tp")
    shards = (gate_w, up_w, down_w, u_w, v_w, out_w)
    fulls = (gate_full, up_full, down_full, u_full, v_full, out_full)
    count, width = tokens.shape
    chips = tp_n // 2
    chip, core = tp // 2, lax.rem(tp, 2)
    twin = tp + 1 - 2 * core
    across = (1 - chip) * 2 + core
    spot = core * chips + chip
    far_spot = core * chips + 1 - chip
    columns = pair_recv.shape[2]
    column = width // columns
    piece_n = put_send.shape[2]
    piece_rows = count // piece_n
    chunk = piece_rows // tp_n
    all_gains = (gain0, gain1, gain2, gain3, gain4, gain5)
    middle = fs_n // 2

    last = [unit for unit in range(len(units)) if units[unit][0] < 2][-1]
    downs = [unit for unit in range(len(units)) if units[unit][0] == 2]
    first = [unit for unit in range(len(units)) if units[unit][0] == 3]
    second = [unit for unit in range(len(units)) if units[unit][0] == 4]
    third = [unit for unit in range(len(units)) if units[unit][0] == 5]

    class Near:
        half = lax.rem(fs, 2)
        partner = fs + 1 - 2 * lax.rem(fs, 2)
        reach = 2
        left_ok, right_ok = fs >= 2, fs + 2 < fs_n
        other_left, other_right = (fs >= 1, fs - 1), (fs + 1 < fs_n, fs + 1)

    class Far:
        half = fs // middle
        partner = lax.rem(fs + middle, fs_n)
        reach = 1
        left_ok, right_ok = lax.rem(fs, middle) > 0, lax.rem(fs, middle) < middle - 1
        other_left, other_right = (fs >= middle, middle - 1), (fs < middle, middle)

    named = {"near": Near, "far": Far}
    ffn, mixer = named[FFN_PAIR], named[MIX_PAIR]
    pairs = (ffn, ffn, ffn, mixer, mixer, mixer)
    phases = (ffn, mixer, ffn)

    barrier = pltpu.get_barrier_semaphore()
    for move in range(1, fs_n):
        pl.semaphore_signal(
            barrier, inc=1, device_id={"fs": lax.rem(fs + move, fs_n)}, device_id_type=MESH
        )
    for move in range(1, grp_n):
        pl.semaphore_signal(
            barrier, inc=1, device_id={"grp": lax.rem(grp + move, grp_n)}, device_id_type=MESH
        )
    for move in range(1, tp_n):
        pl.semaphore_signal(
            barrier, inc=1, device_id={"tp": lax.rem(tp + move, tp_n)}, device_id_type=MESH
        )
    pl.semaphore_wait(barrier, fs_n - 1 + grp_n - 1 + tp_n - 1)

    def large(half):
        return (half + core) % 2 == 0

    def half_start(w, half):
        small, extra = halves(shards[w].shape[0 if w in ROW_SPLIT else 1])
        return half * (small + extra * (1 - core))

    def view(unit, block):
        w, low, share, rows, col, cols, _ = units[unit]
        start = low + grp * share
        if w in ROW_SPLIT:
            return fulls[w].at[block, pl.ds(aligned(start, 16), rows), :]
        start = aligned(block * shards[w].shape[0] + start, 16)
        return fulls[w].at[pl.ds(start, rows), pl.ds(col, cols)]

    def shard_view(unit, half):
        w, low, share, rows, col, cols, _ = units[unit]
        start = low + grp * share
        base = half_start(w, half)
        if w in ROW_SPLIT:
            return shards[w].at[pl.ds(aligned(base + start, 16), rows), :]
        return shards[w].at[pl.ds(aligned(start, 16), rows), pl.ds(aligned(base + col, 128), cols)]

    def has(unit, half):
        return large(half) if units[unit][6] else True

    def own_copies(w):
        half = pairs[w].half
        base = half_start(w, half)
        small, extra = halves(shards[w].shape[0 if w in ROW_SPLIT else 1])

        def part(low, size, sem):
            if w in ROW_SPLIT:
                source = shards[w].at[pl.ds(aligned(base + low, 128), size), :]
                target = fulls[w].at[fs, pl.ds(low, size), :]
            else:
                rows = shards[w].shape[0]
                source = shards[w].at[:, pl.ds(aligned(base + low, 128), size)]
                target = fulls[w].at[pl.ds(aligned(fs * rows, 16), rows), pl.ds(low, size)]
            return pltpu.make_async_copy(source, target, own_sem.at[w, sem])

        made = [(True, part(0, small, 0))]
        if extra:
            made.append((large(half), part(small, extra, 1)))
        return made

    def guarded(ok, act):
        if ok is True:
            act()
        else:
            pl.when(ok)(act)

    def both(a, b):
        if a is True:
            return b
        if b is True:
            return a
        return a & b

    def fresh_copies(unit):
        pair = pairs[units[unit][0]]
        block = view(unit, fs)

        def made(slot, half, target):
            return pltpu.make_async_remote_copy(
                src_ref=shard_view(unit, half),
                dst_ref=block,
                send_sem=fresh_send.at[unit, slot],
                recv_sem=relay_recv.at[unit, fs],
                device_id={"fs": target},
                device_id_type=MESH,
            )

        own, other = pair.half, 1 - pair.half
        near, away = has(unit, own), has(unit, other)
        left, right = fs - pair.reach, fs + pair.reach
        other_left, other_right = pair.other_left[1], pair.other_right[1]
        return (
            (both(pair.left_ok, near), left, lambda: made(0, own, left)),
            (both(pair.right_ok, near), right, lambda: made(1, own, right)),
            (both(pair.other_left[0], away), other_left, lambda: made(2, other, other_left)),
            (both(pair.other_right[0], away), other_right, lambda: made(3, other, other_right)),
        )

    def send_own(unit):
        if unit < first[0]:
            for ok, _, copy in fresh_copies(unit):
                guarded(ok, lambda copy=copy: copy().start())

    def send_some(some, ends):
        for unit in some:
            for ok, target, copy in fresh_copies(unit):
                inner = jnp.logical_and(target > 0, target < fs_n - 1)
                chosen = jnp.logical_not(inner) if ends else inner
                guarded(jnp.logical_and(ok, chosen), lambda copy=copy: copy().start())

    def relay_copy(unit, block, leftward):
        pair = pairs[units[unit][0]]
        target = view(unit, block)
        return pltpu.make_async_remote_copy(
            src_ref=target,
            dst_ref=target,
            send_sem=relay_send.at[unit, block],
            recv_sem=relay_recv.at[unit, block],
            device_id={"fs": fs - pair.reach if leftward else fs + pair.reach},
            device_id_type=MESH,
        )

    def side_copy(unit, block, move):
        target = view(unit, block)
        return pltpu.make_async_remote_copy(
            src_ref=target,
            dst_ref=target,
            send_sem=side_send.at[unit, move - 1, block],
            recv_sem=side_recv.at[unit, move - 1, block],
            device_id={"grp": lax.rem(grp + move, grp_n)},
            device_id_type=MESH,
        )

    def over_blocks(unit, act):
        def whole():
            def step(d, carry):
                @pl.when(fs + d < fs_n)
                def _():
                    act(fs + d, True)

                @pl.when(fs >= d)
                def _():
                    act(fs - d, False)

                return carry

            lax.fori_loop(1, fs_n, step, 0)

        pair = pairs[units[unit][0]]
        guarded(has(unit, pair.half), whole)

    def relay(unit):
        pair = pairs[units[unit][0]]

        def act(block, leftward):
            relay_copy(unit, block, leftward).wait_recv()

            @pl.when(pair.left_ok if leftward else pair.right_ok)
            def _():
                relay_copy(unit, block, leftward).start()

            for move in range(1, grp_n):
                side_copy(unit, block, move).start()

        over_blocks(unit, act)
        send_own(unit + AHEAD)

    def wait_weight(w):
        for ok, copy in own_copies(w):
            guarded(ok, copy.wait)
        for unit in range(len(units)):
            if units[unit][0] == w:

                def act(block, leftward, unit=unit):
                    for move in range(1, grp_n):
                        side_copy(unit, block, move).wait_recv()

                over_blocks(unit, act)

    def finish_sends(some):
        for unit in some:
            pair = pairs[units[unit][0]]
            for ok, _, copy in fresh_copies(unit):
                guarded(ok, lambda copy=copy: copy().wait_send())

            def act(block, leftward, unit=unit, pair=pair):
                @pl.when(pair.left_ok if leftward else pair.right_ok)
                def _():
                    relay_copy(unit, block, leftward).wait_send()

                for move in range(1, grp_n):
                    side_copy(unit, block, move).wait_send()

            over_blocks(unit, act)

    def column_span(col):
        return pl.ds(aligned(col * column, 128), column)

    def pair_step(phase, piece, col):
        span = column_span(col)
        return pltpu.make_async_remote_copy(
            src_ref=parts.at[phase, piece, :, 1 - core, :, span],
            dst_ref=paired.at[phase, piece, :, :, span],
            send_sem=pair_send.at[phase, piece],
            recv_sem=pair_recv.at[phase, piece, col],
            device_id={"tp": twin},
            device_id_type=MESH,
        )

    def side_of(phase, turn):
        half = phases[phase].half
        return 1 - half if turn == 0 else half

    def sum_step(phase, piece, turn, col):
        span = column_span(col)
        return pltpu.make_async_remote_copy(
            src_ref=outgoing.at[phase, piece, turn, :, span],
            dst_ref=landed.at[phase, piece, turn, :, span],
            send_sem=sum_send.at[phase, piece],
            recv_sem=sum_recv.at[phase, piece, turn, col],
            device_id={"tp": across},
            device_id_type=MESH,
        )

    def cross_step(phase, piece, col):
        span = column_span(col)
        return pltpu.make_async_remote_copy(
            src_ref=crossing.at[phase, piece, :, span],
            dst_ref=crossed.at[phase, piece, :, span],
            send_sem=cross_send.at[phase, piece],
            recv_sem=cross_recv.at[phase, piece, col],
            device_id={"fs": phases[phase].partner},
            device_id_type=MESH,
        )

    def all_sent(source, target, sem, device):
        pltpu.make_async_remote_copy(
            src_ref=source,
            dst_ref=target,
            send_sem=sem,
            recv_sem=pair_recv.at[0, 0, 0],
            device_id=device,
            device_id_type=MESH,
        ).wait_send()

    def group_rows(phase, side, piece, inside, size):
        start = piece * 2 * piece_rows + side * piece_rows + inside
        if phase == 3:
            start = piece * piece_rows + inside
        return pl.ds(aligned(start, 16), size)

    def put_copy(phase, which, piece):
        half = phases[phase].half if phase < 3 else 0
        side = 1 - half if which in (3, 4, 6) else half
        place = far_spot if which in (5, 6, 7) else spot
        rows = normed.at[phase, group_rows(phase, side, piece, place * chunk, chunk), :]
        if which in (0, 3):
            target = {"tp": across}
        elif which in (1, 7):
            target = {"fs": phases[phase].partner}
        else:
            target = {"tp": twin}
        return pltpu.make_async_remote_copy(
            src_ref=rows,
            dst_ref=rows,
            send_sem=put_send.at[phase, which, piece],
            recv_sem=put_recv.at[phase, which, piece],
            device_id=target,
            device_id_type=MESH,
        )

    own_puts = ((1,), (0, 1, 2), (0, 1, 2), (0, 2))
    every_put = (0, 1, 2, 3, 4, 5, 6, 7)
    all_puts = ((1, 3, 4, 6), every_put, every_put, (0, 2, 5))

    def start_puts(phase, piece):
        for which in (1, 0, 2):
            if which in own_puts[phase]:
                put_copy(phase, which, piece).start()

    def routed(phase, which):
        split = phase > 0 and phase < 3 and phases[phase] is Near
        cut = piece_n // 2 if split else piece_n
        return range(cut) if which == 3 else range(cut, piece_n)

    def pieces_of(phase, which):
        if which in (3, 7):
            return routed(phase, which)
        return range(piece_n)

    def pass_near(phase, piece):
        put_copy(phase, 1, piece).wait_recv()
        if piece in routed(phase, 3):
            put_copy(phase, 3, piece).start()
        put_copy(phase, 4, piece).start()

    def pass_side(phase, piece):
        put_copy(phase, 0, piece).wait_recv()
        if phase < 3 and piece in routed(phase, 7):
            put_copy(phase, 7, piece).start()
        put_copy(phase, 5, piece).start()

    def pass_last(phase, piece):
        put_copy(phase, 3 if piece in routed(phase, 3) else 7, piece).wait_recv()
        put_copy(phase, 6, piece).start()

    def wait_puts(phase, piece, some):
        for which in some:
            put_copy(phase, which, piece).wait_recv()

    def finish_phase(phase):
        for piece in range(piece_n):
            target = paired.at[phase, piece]
            source = parts.at[phase, piece, :, 1 - core]
            all_sent(source, target, pair_send.at[phase, piece], {"tp": twin})
            source, target = outgoing.at[phase, piece], landed.at[phase, piece]
            all_sent(source, target, sum_send.at[phase, piece], {"tp": across})
            source, target = crossing.at[phase, piece], crossed.at[phase, piece]
            device = {"fs": phases[phase].partner}
            all_sent(source, target, cross_send.at[phase, piece], device)

    def finish_puts(phase):
        for which in all_puts[phase]:
            for piece in pieces_of(phase, which):
                put_copy(phase, which, piece).wait_send()

    def gain(row):
        return all_gains[row][...].astype(F32).reshape(1, width)

    def scaled(values, row):
        scale = lax.rsqrt(jnp.mean(values * values, axis=-1, keepdims=True) + 1e-06)
        return values * scale * gain(row)

    def norm_tokens(piece, start, size):
        def body(low):
            here = aligned(piece * piece_rows + start + low, 16)
            values = tokens[pl.ds(here, 16), :].astype(F32)
            target = group_rows(0, ffn.half, piece, start + low, 16)
            normed[0, target, :] = scaled(values, 0).astype(BF16)

        over_rows(size, 16, body)

    def pass_sum(phase, piece, turn, col):
        span = column_span(col)
        if turn == 0:
            pair_step(phase, piece, col).wait_recv()
        here = pl.ds(aligned((1 - chip) * chunk, 16), chunk)
        side = side_of(phase, turn)
        total = parts[phase, piece, side, core, here, span].astype(F32)
        total = total + paired[phase, piece, side, here, span].astype(F32)
        outgoing[phase, piece, turn, :, span] = total.astype(BF16)
        sum_step(phase, piece, turn, col).start()

    def cross_sums(phase, piece):
        side = 1 - phases[phase].half
        here = pl.ds(aligned(chip * chunk, 16), chunk)

        def step(col, carry):
            span = column_span(col)
            sum_step(phase, piece, 0, col).wait_recv()
            total = parts[phase, piece, side, core, here, span].astype(F32)
            total = total + paired[phase, piece, side, here, span].astype(F32)
            total = total + landed[phase, piece, 0, :, span].astype(F32)
            crossing[phase, piece, :, span] = total.astype(BF16)
            cross_step(phase, piece, col).start()
            return carry

        lax.fori_loop(0, columns, step, 0)

    def add_branch(phase, piece, load, row, factor):
        def wait(col, carry):
            sum_step(phase, piece, 1, col).wait_recv()
            cross_step(phase, piece, col).wait_recv()
            return carry

        lax.fori_loop(0, columns, wait, 0)
        side = phases[phase].half
        after = phases[phase + 1].half if phase < 2 else 0

        def body(low):
            rows = pl.ds(low, 16)
            here = pl.ds(aligned(chip * chunk + low, 16), 16)
            total = parts[phase, piece, side, core, here, :].astype(F32)
            total = total + paired[phase, piece, side, here, :].astype(F32)
            total = total + landed[phase, piece, 1, rows, :].astype(F32)
            total = total + crossed[phase, piece, rows, :].astype(F32)
            value = load(piece, low).astype(F32) + factor * scaled(total, row)
            value = value.astype(BF16)
            if phase < 2:
                streams[phase, pl.ds(aligned(piece * chunk + low, 16), 16), :] = value
                value = scaled(value.astype(F32), row + 1).astype(BF16)
            target = group_rows(phase + 1, after, piece, spot * chunk + low, 16)
            normed[phase + 1, target, :] = value

        over_rows(chunk, 16, body)
        start_puts(phase + 1, piece)

    def hidden_tile(phase, rows, cols):
        left = normed[phase, rows, :]
        gate = jnp.dot(left, gate_full[:, cols], preferred_element_type=F32)
        upper = jnp.dot(left, up_full[:, cols], preferred_element_type=F32)
        hidden[rows, cols] = (gate / (1.0 + jnp.exp(-gate)) * upper).astype(BF16)

    def piece_span(piece):
        return pl.ds(piece * 2 * piece_rows, 2 * piece_rows)

    def hidden_piece(phase, piece):
        rows = piece_span(piece)
        over_tiles(hidden.shape[1], lambda low, size: hidden_tile(phase, rows, pl.ds(low, size)))

    def project(phase, piece, left, right):
        rows = piece_span(piece)

        def step(col, carry):
            per = fs_n // columns
            terms = [
                jnp.dot(left[rows, :], right[col * per + b], preferred_element_type=F32)
                for b in range(per)
            ]
            terms = terms[0] if per == 1 else jnp.concatenate(terms, axis=1)
            terms = terms.astype(BF16).reshape(2, 2, chips * chunk, column)
            parts[phase, piece, :, :, :, column_span(col)] = terms
            pair_step(phase, piece, col).start()

            @pl.when(col >= LAG)
            def _():
                pass_sum(phase, piece, 0, col - LAG)

            return carry

        def late(turn):
            def step(col, carry):
                pass_sum(phase, piece, turn, col)
                return carry

            return step

        lax.fori_loop(0, columns, step, 0)
        lax.fori_loop(columns - LAG, columns, late(0), 0)
        lax.fori_loop(0, columns, late(1), 0)

    def mix(piece):
        at = lax.broadcasted_iota(jnp.int32, (BLOCK, BLOCK), 0)
        to = lax.broadcasted_iota(jnp.int32, (BLOCK, BLOCK), 1)
        half = mixer.half
        here = mixed.shape[1]
        groups = here // GROUP_WIDTH
        all_gain = spatial_gain[...].astype(F32).reshape(1, 2 * here)
        all_gain = jnp.where(half == 0, all_gain[:, :here], all_gain[:, here:])
        all_bias = spatial_bias[...].astype(F32)
        all_bias = jnp.where(half == 0, all_bias[:groups], all_bias[groups:])

        def block(n, carry):
            rows = pl.ds(aligned(piece * 2 * piece_rows + n * BLOCK, 16), BLOCK)
            left = normed[1, rows, :]
            every_v = gelu(jnp.dot(left, v_full[...], preferred_element_type=F32))
            every_u = gelu(jnp.dot(left, u_full[...], preferred_element_type=F32))
            for g in range(groups):
                span = slice(g * GROUP_WIDTH, (g + 1) * GROUP_WIDTH)
                v = every_v[:, span]
                v = v - jnp.mean(v, axis=-1, keepdims=True)
                v = v * lax.rsqrt(jnp.mean(v * v, axis=-1, keepdims=True) + 1e-05)
                v = (v * all_gain[:, span]).astype(BF16)
                weight = spatial_weight[half * groups + g].astype(F32)
                weight = jnp.where(at >= to, weight, 0.0).astype(BF16)
                bias = jnp.where(at == to, all_bias[g : g + 1, :], 0.0)
                bias = jnp.sum(bias, axis=1, keepdims=True)
                spatial = jnp.dot(weight, v, preferred_element_type=F32) + bias
                mixed[rows, span] = (every_u[:, span] * spatial).astype(BF16)
            return carry

        lax.fori_loop(0, 2 * piece_rows // BLOCK, block, 0)

    def load_tokens(piece, low):
        start = piece * piece_rows + spot * chunk + low
        return tokens[pl.ds(aligned(start, 16), 16), :]

    def load_stream(phase):
        return lambda piece, low: streams[phase, pl.ds(aligned(piece * chunk + low, 16), 16), :]

    def relays(some):
        for unit in some:
            relay(unit)

    for unit in range(AHEAD):
        send_own(unit)
    for w in range(6):
        for ok, copy in own_copies(w):
            guarded(ok, copy.start)
    for piece in range(piece_n):
        norm_tokens(piece, spot * chunk, chunk)
        start_puts(0, piece)

    small, extra = halves(gate_w.shape[1])
    if extra:

        @pl.when(jnp.logical_not(large(ffn.half)))
        def _():
            for full in (gate_full, up_full):
                full[:, pl.ds(small, extra)] = jnp.zeros((full.shape[0], extra), BF16)
            pad = jnp.zeros((fs_n, extra, down_full.shape[2]), BF16)
            down_full[:, pl.ds(small, extra), :] = pad

    for piece in range(piece_n):
        for move in range(1, tp_n):
            norm_tokens(piece, lax.rem(spot + move, tp_n) * chunk, chunk)

    inner = jnp.logical_and(fs > 0, fs < fs_n - 1)

    def relay_mixer(some):
        send_some(some, True)
        relays(some)

    outer = jnp.logical_not(inner)

    relays(range(0, 2))
    for piece in range(piece_n):
        pass_near(0, piece)
    relays(range(2, 4))
    send_some(first, False)
    for piece in range(piece_n):
        pass_last(0, piece)
    relays(range(4, last + 1))
    send_some(second, False)
    relay(downs[0])
    wait_weight(0)
    wait_weight(1)
    for piece in range(piece_n):
        wait_puts(0, piece, (4, 6))
        hidden_piece(0, piece)
        if piece == 0:
            relays(downs[1:2])
            send_some(third, False)
    relays(downs[2:])
    wait_weight(2)
    project(0, 0, hidden, down_full)
    project(0, 1, hidden, down_full)
    finish_sends(range(first[0]))
    pl.when(inner)(lambda: relay_mixer(first))
    cross_sums(0, 0)
    cross_sums(0, 1)
    pl.when(inner)(lambda: relay_mixer(second))
    pl.when(outer)(lambda: relays(first))
    add_branch(0, 0, load_tokens, 1, 0.5)
    pl.when(inner)(lambda: relay_mixer(third))
    add_branch(0, 1, load_tokens, 1, 0.5)
    pl.when(outer)(lambda: relays(second))
    pass_near(1, 0)
    pass_side(1, 0)
    wait_weight(3)
    wait_weight(4)
    pass_last(1, 0)
    pl.when(outer)(lambda: relays(third))
    pass_near(1, 1)
    pass_side(1, 1)
    wait_puts(1, 0, (2, 4, 5, 6))
    mix(0)
    wait_weight(5)
    project(1, 0, mixed, out_full)
    pass_last(1, 1)
    wait_puts(1, 1, (2, 4, 5, 6))
    cross_sums(1, 0)
    mix(1)
    project(1, 1, mixed, out_full)
    add_branch(1, 0, load_stream(0), 3, 1.0)
    cross_sums(1, 1)
    add_branch(1, 1, load_stream(0), 3, 1.0)
    pass_side(2, 0)
    pass_near(2, 0)
    pass_last(2, 0)
    pass_side(2, 1)
    wait_puts(2, 0, (2, 4, 5, 6))
    hidden_piece(2, 0)
    pass_near(2, 1)
    project(2, 0, hidden, down_full)
    cross_sums(2, 0)
    pass_last(2, 1)
    wait_puts(2, 1, (2, 4, 5, 6))
    hidden_piece(2, 1)
    project(2, 1, hidden, down_full)
    add_branch(2, 0, load_stream(1), 5, 0.5)
    cross_sums(2, 1)
    pass_side(3, 0)
    add_branch(2, 1, load_stream(1), 5, 0.5)
    pass_side(3, 1)
    finish_sends(range(first[0], len(units)))
    for phase in range(3):
        finish_phase(phase)
        finish_puts(phase)
    for piece in range(piece_n):
        wait_puts(3, piece, (2, 5))
    copy = pltpu.make_async_copy(normed.at[3, pl.ds(0, count), :], result, last_sem)
    copy.start()
    finish_puts(3)
    copy.wait()


def shared(
    sizes,
    tokens,
    ffn_pre_gain,
    gate_weight,
    up_weight,
    down_weight,
    ffn_post_gain,
    mix_pre_gain,
    mix_u_weight,
    mix_v_weight,
    spatial_gain,
    spatial_weight,
    spatial_bias,
    mix_out_weight,
    mix_post_gain,
    late_pre_gain,
    late_post_gain,
):
    grp_n, fs_n, tp_n = sizes
    count, width = tokens.shape
    small, extra = halves(gate_weight.shape[1])
    hidden_width = small + extra
    channels = mix_u_weight.shape[1] // 2
    columns = math.gcd(fs_n, 4)
    pieces = count // BLOCK
    chunk = BLOCK // tp_n
    vmem = pl.BlockSpec(memory_space=pltpu.VMEM)
    hbm = pl.BlockSpec(memory_space=pl.ANY)
    weights = (gate_weight, up_weight, down_weight, mix_u_weight, mix_v_weight, mix_out_weight)
    units = weight_units([w.shape for w in weights], grp_n)
    unit_n = len(units)
    dma = pltpu.SemaphoreType.DMA
    return pl.pallas_call(
        functools.partial(shared_kernel, sizes, units),
        out_shape=jax.ShapeDtypeStruct((count, width), BF16),
        in_specs=[vmem] * 7 + [hbm, hbm, hbm, hbm, hbm, hbm, vmem, vmem, vmem],
        out_specs=hbm,
        scratch_shapes=[
            pltpu.VMEM((width, hidden_width), BF16),
            pltpu.VMEM((width, hidden_width), BF16),
            pltpu.VMEM((fs_n, hidden_width, down_weight.shape[1]), BF16),
            pltpu.VMEM((width, channels), BF16),
            pltpu.VMEM((width, channels), BF16),
            pltpu.VMEM((fs_n, channels, mix_out_weight.shape[1]), BF16),
            pltpu.VMEM((4, 2 * count, width), BF16),
            pltpu.VMEM((2 * count, hidden_width), BF16),
            pltpu.VMEM((2 * count, channels), BF16),
            pltpu.VMEM((2, count // tp_n, width), BF16),
            pltpu.VMEM((3, pieces, 2, 2, BLOCK // 2, width), BF16),
            pltpu.VMEM((3, pieces, 2, BLOCK // 2, width), BF16),
            pltpu.VMEM((3, pieces, 2, chunk, width), BF16),
            pltpu.VMEM((3, pieces, 2, chunk, width), BF16),
            pltpu.VMEM((3, pieces, chunk, width), BF16),
            pltpu.VMEM((3, pieces, chunk, width), BF16),
            dma((6, 2)),
            dma((unit_n, 4)),
            dma((unit_n, fs_n)),
            dma((unit_n, fs_n)),
            dma((unit_n, max(1, grp_n - 1), fs_n)),
            dma((unit_n, max(1, grp_n - 1), fs_n)),
            dma((3, pieces)),
            dma((3, pieces, columns)),
            dma((3, pieces)),
            dma((3, pieces, 2, columns)),
            dma((3, pieces)),
            dma((3, pieces, columns)),
            dma((4, 8, pieces)),
            dma((4, 8, pieces)),
            dma(()),
        ],
        compiler_params=pltpu.CompilerParams(
            collective_id=0, has_side_effects=True, vmem_limit_bytes=60 * 2**20
        ),
    )(
        tokens,
        ffn_pre_gain,
        ffn_post_gain,
        mix_pre_gain,
        mix_post_gain,
        late_pre_gain,
        late_post_gain,
        gate_weight,
        up_weight,
        down_weight,
        mix_u_weight,
        mix_v_weight,
        mix_out_weight,
        spatial_gain,
        spatial_weight,
        spatial_bias,
    )


def can_share(sizes, tokens, gate_weight, mix_u_weight):
    grp_n, fs_n, tp_n = sizes
    count = tokens.shape[0] // (grp_n * fs_n)
    rows = gate_weight.shape[0] // fs_n
    hidden_width = gate_weight.shape[1] // tp_n
    channels = mix_u_weight.shape[1] // tp_n
    return (
        tp_n == 4
        and fs_n == 4
        and count == 2 * BLOCK
        and rows % (32 * grp_n) == 0
        and hidden_width % 128 == 0
        and halves(hidden_width)[0] % (32 * grp_n) == 0
        and channels % (2 * GROUP_WIDTH) == 0
    )


def solution(mesh):
    in_specs = (
        P(("grp", "fs"), None),
        P(),
        P("fs", "tp"),
        P("fs", "tp"),
        P("tp", "fs"),
        P(),
        P(),
        P("fs", "tp"),
        P("fs", "tp"),
        P("tp"),
        P("tp", None, None),
        P("tp", None),
        P("tp", "fs"),
        P(),
        P(),
        P(),
    )
    out_specs = P(("grp", "fs"), None)
    sizes = (mesh.shape["grp"], mesh.shape["fs"], mesh.shape["tp"])

    def step(*arrays):
        plan = shared if can_share(sizes, arrays[0], arrays[2], arrays[7]) else shards
        body = functools.partial(plan, sizes)
        return jax.shard_map(
            body, mesh=mesh, in_specs=in_specs, out_specs=out_specs, check_vma=False
        )(*arrays)

    return step
```

```python
import functools
import math

import jax
import jax.numpy as jnp
from jax import lax
from jax.experimental import pallas as pl
from jax.experimental.pallas import tpu as pltpu
from jax.sharding import PartitionSpec as P

GROUP_WIDTH = 128
BLOCK = 128
TILE = 256
F32 = jnp.float32
BF16 = jnp.bfloat16
MESH = pl.DeviceIdType.MESH
SPLITS = (2, 2, 2, 1, 1, 2)
PIECE = 32


def aligned(value, unit):
    return value if isinstance(value, int) else pl.multiple_of(value, unit)


def over_tiles(width, body):
    count = width // TILE

    def step(i, carry):
        body(pl.multiple_of(i * TILE, TILE), TILE)
        return carry

    lax.fori_loop(0, count, step, 0)
    if width % TILE:
        body(count * TILE, width % TILE)


def over_rows(count, size, body):
    def step(i, carry):
        body(pl.multiple_of(i * size, size))
        return carry

    lax.fori_loop(0, count // size, step, 0)


def gelu(a):
    return 0.5 * a * (1.0 + lax.erf(a * (2.0**-0.5)))


def kernel(
    sizes,
    tokens,
    gain0,
    gain1,
    gain2,
    gain3,
    gain4,
    gain5,
    gate_w,
    up_w,
    down_w,
    u_w,
    v_w,
    out_w,
    spatial_gain,
    spatial_weight,
    spatial_bias,
    result,
    gate_full,
    up_full,
    down_full,
    u_full,
    v_full,
    out_full,
    normed,
    hidden,
    mixed,
    parts,
    paired,
    outgoing,
    landed,
    streams,
    own_sem,
    left_send,
    left_recv,
    right_send,
    right_recv,
    side_send,
    side_recv,
    pair_send,
    pair_recv,
    sum_send,
    sum_recv,
    twin_send,
    twin_recv,
    put_send,
    put_recv,
    pass_send,
    pass_recv,
    last_sem,
):
    grp_n, fs_n, tp_n = sizes
    grp, fs, tp = lax.axis_index("grp"), lax.axis_index("fs"), lax.axis_index("tp")
    shards = (gate_w, up_w, down_w, u_w, v_w, out_w)
    fulls = (gate_full, up_full, down_full, u_full, v_full, out_full)
    count, width = tokens.shape
    chunk = count // tp_n
    chips = tp_n // 2
    chip, core = tp // 2, lax.rem(tp, 2)
    twin = tp + 1 - 2 * core
    columns = pair_send.shape[1]
    column = width // columns
    piece_n = put_send.shape[1]
    piece_rows = chunk // piece_n
    all_gains = (gain0, gain1, gain2, gain3, gain4, gain5)

    barrier = pltpu.get_barrier_semaphore()
    for move in (1, fs_n - 1):
        pl.semaphore_signal(
            barrier, inc=1, device_id={"fs": lax.rem(fs + move, fs_n)}, device_id_type=MESH
        )
    for move in range(1, grp_n):
        pl.semaphore_signal(
            barrier, inc=1, device_id={"grp": lax.rem(grp + move, grp_n)}, device_id_type=MESH
        )
    for move in range(1, tp_n):
        pl.semaphore_signal(
            barrier, inc=1, device_id={"tp": lax.rem(tp + move, tp_n)}, device_id_type=MESH
        )
    pl.semaphore_wait(barrier, 2 + grp_n - 1 + tp_n - 1)

    units = []
    for w in range(6):
        piece = shards[w].shape[0] // grp_n // SPLITS[w]
        for s in range(SPLITS[w]):
            units.append((w, s * piece, piece))

    def unit_rows(unit):
        w, low, piece = units[unit]
        return aligned(grp * (shards[w].shape[0] // grp_n) + low, 16), piece

    def place(w, block, low, piece):
        if w in (2, 5):
            return fulls[w].at[block, pl.ds(low, piece), :]
        start = aligned(block * shards[w].shape[0] + low, 16)
        return fulls[w].at[pl.ds(start, piece), :]

    def own_copy(w):
        return pltpu.make_async_copy(
            shards[w], place(w, fs, 0, shards[w].shape[0]), own_sem.at[w]
        )

    def to_right(unit, hop, own=False):
        w = units[unit][0]
        low, piece = unit_rows(unit)
        target = place(w, fs - hop, low, piece)
        source = shards[w].at[pl.ds(low, piece), :] if own else target
        return pltpu.make_async_remote_copy(
            src_ref=source,
            dst_ref=target,
            send_sem=right_send.at[unit, hop],
            recv_sem=right_recv.at[unit, hop],
            device_id={"fs": fs + 1},
            device_id_type=MESH,
        )

    def to_left(unit, hop, own=False):
        w = units[unit][0]
        low, piece = unit_rows(unit)
        target = place(w, fs + hop, low, piece)
        source = shards[w].at[pl.ds(low, piece), :] if own else target
        return pltpu.make_async_remote_copy(
            src_ref=source,
            dst_ref=target,
            send_sem=left_send.at[unit, hop],
            recv_sem=left_recv.at[unit, hop],
            device_id={"fs": fs - 1},
            device_id_type=MESH,
        )

    def to_side(unit, side, hop, move):
        w = units[unit][0]
        low, piece = unit_rows(unit)
        block = fs - hop if side == 0 else fs + hop
        target = place(w, block, low, piece)
        return pltpu.make_async_remote_copy(
            src_ref=target,
            dst_ref=target,
            send_sem=side_send.at[unit, side, move - 1, hop],
            recv_sem=side_recv.at[unit, side, move - 1, hop],
            device_id={"grp": lax.rem(grp + move, grp_n)},
            device_id_type=MESH,
        )

    def send_own(unit):
        if unit >= len(units):
            return

        @pl.when(fs < fs_n - 1)
        def _():
            to_right(unit, 0, own=True).start()

        @pl.when(fs > 0)
        def _():
            to_left(unit, 0, own=True).start()

    def relay(unit):
        def step(hop, carry):
            @pl.when(fs >= hop)
            def _():
                to_right(unit, hop - 1).wait_recv()

                @pl.when(fs < fs_n - 1)
                def _():
                    to_right(unit, hop).start()

                for move in range(1, grp_n):
                    to_side(unit, 0, hop, move).start()

            @pl.when(fs + hop < fs_n)
            def _():
                to_left(unit, hop - 1).wait_recv()

                @pl.when(fs > 0)
                def _():
                    to_left(unit, hop).start()

                for move in range(1, grp_n):
                    to_side(unit, 1, hop, move).start()

            return carry

        lax.fori_loop(1, fs_n, step, 0)

    def wait_weight(w):
        own_copy(w).wait()
        for unit in range(len(units)):
            if units[unit][0] == w:

                def step(hop, carry, unit=unit):
                    for move in range(1, grp_n):

                        @pl.when(fs >= hop)
                        def _():
                            to_side(unit, 0, hop, move).wait_recv()

                        @pl.when(fs + hop < fs_n)
                        def _():
                            to_side(unit, 1, hop, move).wait_recv()

                    return carry

                lax.fori_loop(1, fs_n, step, 0)

    def finish_sends():
        for unit in range(len(units)):

            def step(hop, carry, unit=unit):
                @pl.when((fs >= hop) & (fs < fs_n - 1))
                def _():
                    to_right(unit, hop).wait_send()

                @pl.when((fs + hop < fs_n) & (fs > 0))
                def _():
                    to_left(unit, hop).wait_send()

                @pl.when(hop > 0)
                def _():
                    for move in range(1, grp_n):

                        @pl.when(fs >= hop)
                        def _():
                            to_side(unit, 0, hop, move).wait_send()

                        @pl.when(fs + hop < fs_n)
                        def _():
                            to_side(unit, 1, hop, move).wait_send()

                return carry

            lax.fori_loop(0, fs_n, step, 0)

    def other(move, which):
        return lax.rem(chip + move, chips) * 2 + which

    def origin(move, which):
        return lax.rem(chip + chips - move, chips) * 2 + which

    def chunk_rows(owner):
        return pl.ds(aligned(owner * chunk, 16), chunk)

    def column_span(col):
        return pl.ds(aligned(col * column, 128), column)

    def pair_copy(phase, col, move):
        span = column_span(col)
        return pltpu.make_async_remote_copy(
            src_ref=parts.at[phase, chunk_rows(other(move, 1 - core)), span],
            dst_ref=paired.at[phase, move, :, span],
            send_sem=pair_send.at[phase, col, move],
            recv_sem=pair_recv.at[phase, col, move],
            device_id={"tp": twin},
            device_id_type=MESH,
        )

    def sum_copy(phase, col, move):
        span = column_span(col)
        return pltpu.make_async_remote_copy(
            src_ref=outgoing.at[phase, move, :, span],
            dst_ref=landed.at[phase, move, :, span],
            send_sem=sum_send.at[phase, col, move],
            recv_sem=sum_recv.at[phase, col, move],
            device_id={"tp": other(move, core)},
            device_id_type=MESH,
        )

    def piece_span(owner, piece):
        return pl.ds(aligned(owner * chunk + piece * piece_rows, 16), piece_rows)

    def twin_copy(phase, piece):
        rows = piece_span(tp, piece)
        return pltpu.make_async_remote_copy(
            src_ref=streams.at[phase, rows, :],
            dst_ref=streams.at[phase, rows, :],
            send_sem=twin_send.at[phase, piece],
            recv_sem=twin_recv.at[phase, piece],
            device_id={"tp": twin},
            device_id_type=MESH,
        )

    def put_copy(phase, piece, move):
        rows = piece_span(tp, piece)
        return pltpu.make_async_remote_copy(
            src_ref=streams.at[phase, rows, :],
            dst_ref=streams.at[phase, rows, :],
            send_sem=put_send.at[phase, piece, move],
            recv_sem=put_recv.at[phase, piece, move],
            device_id={"tp": other(move, core)},
            device_id_type=MESH,
        )

    def pass_copy(phase, piece, move):
        rows = piece_span(origin(move, core), piece)
        return pltpu.make_async_remote_copy(
            src_ref=streams.at[phase, rows, :],
            dst_ref=streams.at[phase, rows, :],
            send_sem=pass_send.at[phase, piece, move],
            recv_sem=pass_recv.at[phase, piece, move],
            device_id={"tp": twin},
            device_id_type=MESH,
        )

    def gain(row):
        return all_gains[row][...].astype(F32).reshape(1, width)

    def norm_rows(load, row):
        def body(low):
            values = load(pl.ds(low, 32)).astype(F32)
            scale = lax.rsqrt(jnp.mean(values * values, axis=-1, keepdims=True) + 1e-06)
            normed[pl.ds(low, 32), :] = (values * scale * gain(row)).astype(BF16)

        over_rows(count, 32, body)

    def start_sums(phase, col):
        for move in range(1, chips):
            pair_copy(phase, col, move).wait_recv()
            span = column_span(col)
            mine = parts[phase, chunk_rows(other(move, core)), span].astype(F32)
            both = mine + paired[phase, move, :, span].astype(F32)
            outgoing[phase, move, :, span] = both.astype(BF16)
            sum_copy(phase, col, move).start()

    def add_branch(phase, load, row, factor):
        for col in range(columns):
            pair_copy(phase, col, 0).wait_recv()
            for move in range(1, chips):
                sum_copy(phase, col, move).wait_recv()
        for piece in range(piece_n):

            def body(low, piece=piece):
                here = pl.ds(aligned(piece * piece_rows + low, 16), 16)
                rows = pl.ds(aligned(tp * chunk + piece * piece_rows + low, 16), 16)
                total = parts[phase, rows, :].astype(F32) + paired[phase, 0, here, :].astype(F32)
                for move in range(1, chips):
                    total = total + landed[phase, move, here, :].astype(F32)
                scale = lax.rsqrt(jnp.mean(total * total, axis=-1, keepdims=True) + 1e-06)
                branch = total * scale * gain(row)
                streams[phase, rows, :] = (load(rows).astype(F32) + factor * branch).astype(BF16)

            over_rows(piece_rows, 16, body)
            for move in range(1, chips):
                put_copy(phase, piece, move).start()
            twin_copy(phase, piece).start()

    def wait_put(phase):
        for piece in range(piece_n):
            for move in range(1, chips):
                put_copy(phase, piece, move).wait_recv()
                pass_copy(phase, piece, move).start()
        for piece in range(piece_n):
            twin_copy(phase, piece).wait_recv()
            for move in range(1, chips):
                pass_copy(phase, piece, move).wait_recv()

    def finish_phase(phase):
        for col in range(columns):
            for move in range(chips):
                pair_copy(phase, col, move).wait_send()
            for move in range(1, chips):
                sum_copy(phase, col, move).wait_send()
        for piece in range(piece_n):
            twin_copy(phase, piece).wait_send()
            for move in range(1, chips):
                put_copy(phase, piece, move).wait_send()
                pass_copy(phase, piece, move).wait_send()

    def hidden_units():
        def body(low, size):
            cols = pl.ds(low, size)
            gate = jnp.dot(normed[...], gate_full[:, cols], preferred_element_type=F32)
            upper = jnp.dot(normed[...], up_full[:, cols], preferred_element_type=F32)
            hidden[:, cols] = (gate / (1.0 + jnp.exp(-gate)) * upper).astype(BF16)

        over_tiles(hidden.shape[1], body)

    def project(phase, left, right):
        blocks = fs_n // columns

        def step(col, carry):
            terms = [
                jnp.dot(left[...], right[col * blocks + b], preferred_element_type=F32)
                for b in range(blocks)
            ]
            terms = terms[0] if blocks == 1 else jnp.concatenate(terms, axis=1)
            parts[phase, :, column_span(col)] = terms.astype(BF16)
            for move in range(chips - 1, -1, -1):
                pair_copy(phase, col, move).start()

            @pl.when(col > 0)
            def _():
                start_sums(phase, col - 1)

            return carry

        lax.fori_loop(0, columns, step, 0)
        start_sums(phase, columns - 1)

    def mix():
        rows = lax.broadcasted_iota(jnp.int32, (BLOCK, BLOCK), 0)
        cols = lax.broadcasted_iota(jnp.int32, (BLOCK, BLOCK), 1)
        all_spatial_gain = spatial_gain[...].astype(F32).reshape(1, mixed.shape[1])
        for g in range(mixed.shape[1] // GROUP_WIDTH):
            span = slice(g * GROUP_WIDTH, (g + 1) * GROUP_WIDTH)
            v = gelu(jnp.dot(normed[...], v_full[:, span], preferred_element_type=F32))
            u = gelu(jnp.dot(normed[...], u_full[:, span], preferred_element_type=F32))
            v = v - jnp.mean(v, axis=-1, keepdims=True)
            v = v * lax.rsqrt(jnp.mean(v * v, axis=-1, keepdims=True) + 1e-05)
            v = (v * all_spatial_gain[:, span]).astype(BF16)
            weight = spatial_weight[g].astype(F32)
            weight = jnp.where(rows >= cols, weight, 0.0).astype(BF16)
            bias = spatial_bias[...][g : g + 1, :].astype(F32)
            bias = jnp.sum(jnp.where(rows == cols, bias, 0.0), axis=1, keepdims=True)
            for n in range(count // BLOCK):
                part = slice(n * BLOCK, (n + 1) * BLOCK)
                spatial = jnp.dot(weight, v[part], preferred_element_type=F32)
                spatial = spatial + bias
                mixed[part, span] = (u[part] * spatial).astype(BF16)

    load_tokens = lambda rows: tokens[rows, :]
    load_first = lambda rows: streams[0, rows, :]
    load_second = lambda rows: streams[1, rows, :]

    send_own(0)
    send_own(1)
    for w in range(6):
        own_copy(w).start()
    norm_rows(load_tokens, 0)

    for unit in range(5):
        relay(unit)
        send_own(unit + 2)
    wait_weight(0)
    wait_weight(1)
    hidden_units()
    relay(5)
    send_own(7)
    relay(6)
    send_own(8)
    send_own(9)
    wait_weight(2)
    project(0, hidden, down_full)
    relay(7)
    add_branch(0, load_tokens, 1, 0.5)
    relay(8)
    wait_put(0)
    norm_rows(load_first, 2)
    relay(9)
    wait_weight(3)
    wait_weight(4)
    mix()
    wait_weight(5)
    project(1, mixed, out_full)
    add_branch(1, load_first, 3, 1.0)
    wait_put(1)
    norm_rows(load_second, 4)
    hidden_units()
    project(2, hidden, down_full)
    add_branch(2, load_second, 5, 0.5)
    finish_sends()
    wait_put(2)
    last = pltpu.make_async_copy(streams.at[2], result, last_sem)
    last.start()
    for phase in range(3):
        finish_phase(phase)
    last.wait()


def shards(
    sizes,
    tokens,
    ffn_pre_gain,
    gate_weight,
    up_weight,
    down_weight,
    ffn_post_gain,
    mix_pre_gain,
    mix_u_weight,
    mix_v_weight,
    spatial_gain,
    spatial_weight,
    spatial_bias,
    mix_out_weight,
    mix_post_gain,
    late_pre_gain,
    late_post_gain,
):
    grp_n, fs_n, tp_n = sizes
    count, width = tokens.shape
    hidden_width = gate_weight.shape[1]
    channels = mix_u_weight.shape[1]
    columns = math.gcd(fs_n, 4)
    chips = tp_n // 2
    chunk = count // tp_n
    pieces = max(1, chunk // PIECE)
    vmem = pl.BlockSpec(memory_space=pltpu.VMEM)
    hbm = pl.BlockSpec(memory_space=pl.ANY)
    units = sum(SPLITS)
    dma = pltpu.SemaphoreType.DMA
    return pl.pallas_call(
        functools.partial(kernel, sizes),
        out_shape=jax.ShapeDtypeStruct((count, width), BF16),
        in_specs=[vmem] * 7 + [hbm, hbm, hbm, hbm, hbm, hbm, vmem, vmem, vmem],
        out_specs=hbm,
        scratch_shapes=[
            pltpu.VMEM((width, hidden_width), BF16),
            pltpu.VMEM((width, hidden_width), BF16),
            pltpu.VMEM((fs_n,) + down_weight.shape, BF16),
            pltpu.VMEM((width, channels), BF16),
            pltpu.VMEM((width, channels), BF16),
            pltpu.VMEM((fs_n,) + mix_out_weight.shape, BF16),
            pltpu.VMEM((count, width), BF16),
            pltpu.VMEM((count, hidden_width), BF16),
            pltpu.VMEM((count, channels), BF16),
            pltpu.VMEM((3, count, width), BF16),
            pltpu.VMEM((3, chips, chunk, width), BF16),
            pltpu.VMEM((3, chips, chunk, width), BF16),
            pltpu.VMEM((3, chips, chunk, width), BF16),
            pltpu.VMEM((3, count, width), BF16),
            dma((6,)),
            dma((units, fs_n)),
            dma((units, fs_n)),
            dma((units, fs_n)),
            dma((units, fs_n)),
            dma((units, 2, grp_n - 1, fs_n)),
            dma((units, 2, grp_n - 1, fs_n)),
            dma((3, columns, chips)),
            dma((3, columns, chips)),
            dma((3, columns, chips)),
            dma((3, columns, chips)),
            dma((3, pieces)),
            dma((3, pieces)),
            dma((3, pieces, chips)),
            dma((3, pieces, chips)),
            dma((3, pieces, chips)),
            dma((3, pieces, chips)),
            dma(()),
        ],
        compiler_params=pltpu.CompilerParams(
            collective_id=0, has_side_effects=True, vmem_limit_bytes=60 * 2**20
        ),
    )(
        tokens,
        ffn_pre_gain,
        ffn_post_gain,
        mix_pre_gain,
        mix_post_gain,
        late_pre_gain,
        late_post_gain,
        gate_weight,
        up_weight,
        down_weight,
        mix_u_weight,
        mix_v_weight,
        mix_out_weight,
        spatial_gain,
        spatial_weight,
        spatial_bias,
    )


PIECES = (2, 2, 2, 1, 1, 1)
AHEAD = 3
LAG = 2
ROW_SPLIT = (2, 5)
END_GROUPS = 1


def halves(size):
    small = size // 256 * 128
    return small, size - 2 * small


def end_share(size):
    return size // (4 * GROUP_WIDTH) * END_GROUPS * GROUP_WIDTH


def weight_units(shapes, grp_n):
    units = []
    for group in ((0, 1), (2,), (3,), (4,), (5,)):
        made = []
        for w in group:
            rows, cols = shapes[w]
            split = w in ROW_SPLIT
            size = rows if split else cols
            small, extra = halves(size)
            ends = end_share(size)
            if w < 3:
                cuts = [("side", (0, small + extra), 0, small, PIECES[w])]
                if extra:
                    cuts.append(("middle", (small, small), small, extra, 1))
            else:
                cuts = [
                    ("middle", (ends, ends), 0, size - ends, PIECES[w]),
                    ("ends", (0, 0), 0, ends, PIECES[w]),
                ]
            mine = []
            for route, source, target, span, pieces in cuts:
                share = (span if split else rows) // grp_n
                piece = share // pieces
                for n in range(pieces):
                    mine.append((w, route, source, target, span, share, n * piece, piece))
            made.append(mine)
        for n in range(max(len(mine) for mine in made)):
            units += [mine[n] for mine in made if n < len(mine)]
    return units


def shared_kernel(
    sizes,
    units,
    tokens,
    gain0,
    gain1,
    gain2,
    gain3,
    gain4,
    gain5,
    gate_w,
    up_w,
    down_w,
    u_w,
    v_w,
    out_w,
    spatial_gain,
    spatial_weight,
    spatial_bias,
    result,
    gate_full,
    up_full,
    down_full,
    u_full,
    v_full,
    out_full,
    normed,
    hidden,
    mixed,
    streams,
    parts,
    paired,
    outgoing,
    landed,
    crossing,
    crossed,
    own_sem,
    fresh_send,
    relay_send,
    relay_recv,
    side_send,
    side_recv,
    pair_send,
    pair_recv,
    sum_send,
    sum_recv,
    cross_send,
    cross_recv,
    put_send,
    put_recv,
    last_sem,
):
    grp_n, fs_n, tp_n = sizes
    grp, fs, tp = lax.axis_index("grp"), lax.axis_index("fs"), lax.axis_index("tp")
    shards = (gate_w, up_w, down_w, u_w, v_w, out_w)
    fulls = (gate_full, up_full, down_full, u_full, v_full, out_full)
    count, width = tokens.shape
    chips = tp_n // 2
    chip, core = tp // 2, lax.rem(tp, 2)
    twin = tp + 1 - 2 * core
    across = (1 - chip) * 2 + core
    spot = core * chips + chip
    far_spot = core * chips + 1 - chip
    columns = pair_recv.shape[2]
    column = width // columns
    piece_n = put_send.shape[1]
    piece_rows = count // piece_n
    chunk = piece_rows // tp_n
    all_gains = (gain0, gain1, gain2, gain3, gain4, gain5)
    middle = fs_n // 2

    last = [unit for unit in range(len(units)) if units[unit][0] < 2][-1]
    downs = [unit for unit in range(len(units)) if units[unit][0] == 2]
    first = [unit for unit in range(len(units)) if units[unit][0] == 3]
    second = [unit for unit in range(len(units)) if units[unit][0] == 4]
    third = [unit for unit in range(len(units)) if units[unit][0] == 5]

    inner = jnp.logical_and(fs > 0, fs < fs_n - 1)
    outer = jnp.logical_not(inner)

    class Near:
        half = jnp.where(inner, 1, 0)
        partner = fs + 1 - 2 * lax.rem(fs, 2)

    class Far:
        half = fs // middle
        partner = lax.rem(fs + middle, fs_n)

    ffn, mixer = Far, Near
    phases = (ffn, mixer, ffn)

    barrier = pltpu.get_barrier_semaphore()
    for move in range(1, fs_n):
        pl.semaphore_signal(
            barrier, inc=1, device_id={"fs": lax.rem(fs + move, fs_n)}, device_id_type=MESH
        )
    for move in range(1, grp_n):
        pl.semaphore_signal(
            barrier, inc=1, device_id={"grp": lax.rem(grp + move, grp_n)}, device_id_type=MESH
        )
    for move in range(1, tp_n):
        pl.semaphore_signal(
            barrier, inc=1, device_id={"tp": lax.rem(tp + move, tp_n)}, device_id_type=MESH
        )
    pl.semaphore_wait(barrier, fs_n - 1 + grp_n - 1 + tp_n - 1)

    def view(unit, block):
        w, _, _, target, span, share, low, rows = units[unit]
        start = grp * share + low
        if w in ROW_SPLIT:
            return fulls[w].at[block, pl.ds(aligned(target + start, 16), rows), :]
        start = aligned(block * shards[w].shape[0] + start, 16)
        return fulls[w].at[pl.ds(start, rows), pl.ds(target, span)]

    def shard_view(unit, half):
        w, _, source, _, span, share, low, rows = units[unit]
        start = grp * share + low
        base = source[0] + half * (source[1] - source[0])
        if w in ROW_SPLIT:
            return shards[w].at[pl.ds(aligned(base + start, 16), rows), :]
        return shards[w].at[pl.ds(aligned(start, 16), rows), pl.ds(aligned(base, 128), span)]

    def has(unit):
        return {"side": True, "middle": inner, "ends": outer}[units[unit][1]]

    def own_copies(w):
        size = shards[w].shape[0 if w in ROW_SPLIT else 1]
        small, extra = halves(size)
        ends = end_share(size)

        def part(base, low, span, sem):
            if w in ROW_SPLIT:
                source = shards[w].at[pl.ds(aligned(base, 128), span), :]
                target = fulls[w].at[fs, pl.ds(low, span), :]
            else:
                rows = shards[w].shape[0]
                source = shards[w].at[:, pl.ds(aligned(base, 128), span)]
                target = fulls[w].at[pl.ds(aligned(fs * rows, 16), rows), pl.ds(low, span)]
            return pltpu.make_async_copy(source, target, own_sem.at[w, sem])

        if w >= 3:
            return [(inner, part(ends, 0, size - ends, 0)), (outer, part(0, 0, ends, 1))]
        made = [(True, part(ffn.half * (small + extra), 0, small, 0))]
        if extra:
            made.append((inner, part(small, small, extra, 1)))
        return made

    def guarded(ok, act):
        if ok is True:
            act()
        else:
            pl.when(ok)(act)

    def fresh_copies(unit):
        route = units[unit][1]
        half = ffn.half
        block = view(unit, fs)

        def made(slot, half, target):
            return pltpu.make_async_remote_copy(
                src_ref=shard_view(unit, half),
                dst_ref=block,
                send_sem=fresh_send.at[unit, slot],
                recv_sem=relay_recv.at[unit, fs],
                device_id={"fs": target},
                device_id_type=MESH,
            )

        if route == "middle":
            return (
                (fs != middle - 1, lambda: made(0, 0, middle - 1)),
                (fs != middle, lambda: made(1, 0, middle)),
            )
        if route == "ends":
            return (
                (fs > 0, lambda: made(0, 0, 0)),
                (fs < fs_n - 1, lambda: made(1, 0, fs_n - 1)),
            )
        near = fs + 1 - 2 * lax.rem(fs, 2)
        return (
            (True, lambda: made(0, half, near)),
            (True, lambda: made(1, 1 - half, jnp.where(fs < middle, middle, middle - 1))),
        )

    def send_own(unit):
        if unit < first[0]:
            for ok, copy in fresh_copies(unit):
                guarded(ok, lambda copy=copy: copy().start())

    def send_some(some, route):
        for unit in some:
            if units[unit][1] == route:
                for ok, copy in fresh_copies(unit):
                    guarded(ok, lambda copy=copy: copy().start())

    def relay_copy(unit, block, leftward):
        target = view(unit, block)
        return pltpu.make_async_remote_copy(
            src_ref=target,
            dst_ref=target,
            send_sem=relay_send.at[unit, block],
            recv_sem=relay_recv.at[unit, block],
            device_id={"fs": fs - 1 if leftward else fs + 1},
            device_id_type=MESH,
        )

    def goes_on(unit, leftward, act):
        if units[unit][1] == "side":
            pl.when(lax.rem(fs, middle) == (1 if leftward else 0))(act)

    def side_copy(unit, block, move):
        target = view(unit, block)
        return pltpu.make_async_remote_copy(
            src_ref=target,
            dst_ref=target,
            send_sem=side_send.at[unit, move - 1],
            recv_sem=side_recv.at[unit, move - 1],
            device_id={"grp": lax.rem(grp + move, grp_n)},
            device_id_type=MESH,
        )

    def side_total(unit, move):
        w, _, _, target, span, share, low, rows = units[unit]
        others = fs_n - 1
        if w in ROW_SPLIT:
            total = fulls[w].at[pl.ds(0, others), pl.ds(0, rows), :]
        else:
            total = fulls[w].at[pl.ds(0, others * rows), pl.ds(target, span)]
        return pltpu.make_async_remote_copy(
            src_ref=total,
            dst_ref=total,
            send_sem=side_send.at[unit, move - 1],
            recv_sem=side_recv.at[unit, move - 1],
            device_id={"grp": lax.rem(grp + move, grp_n)},
            device_id_type=MESH,
        )

    def over_blocks(unit, act):
        def whole():
            def step(d, carry):
                @pl.when(fs + d < fs_n)
                def _():
                    act(fs + d, True)

                @pl.when(fs >= d)
                def _():
                    act(fs - d, False)

                return carry

            lax.fori_loop(1, fs_n, step, 0)

        guarded(has(unit), whole)

    def relay(unit):
        def act(block, leftward):
            relay_copy(unit, block, leftward).wait_recv()

            goes_on(unit, leftward, lambda: relay_copy(unit, block, leftward).start())

            for move in range(1, grp_n):
                side_copy(unit, block, move).start()

        over_blocks(unit, act)
        send_own(unit + AHEAD)

    def wait_weight(w):
        for ok, copy in own_copies(w):
            guarded(ok, copy.wait)
        for unit in range(len(units)):
            if units[unit][0] == w:

                def act(unit=unit):
                    for move in range(1, grp_n):
                        side_total(unit, move).wait_recv()

                guarded(has(unit), act)

    def finish_sends(some):
        for unit in some:
            for ok, copy in fresh_copies(unit):
                guarded(ok, lambda copy=copy: copy().wait_send())

            def act(block, leftward, unit=unit):
                goes_on(unit, leftward, lambda: relay_copy(unit, block, leftward).wait_send())

            def sides(unit=unit):
                for move in range(1, grp_n):
                    side_total(unit, move).wait_send()

            over_blocks(unit, act)
            guarded(has(unit), sides)

    def column_span(col):
        return pl.ds(aligned(col * column, 128), column)

    def pair_step(phase, piece, col):
        span = column_span(col)
        return pltpu.make_async_remote_copy(
            src_ref=parts.at[phase, piece, :, 1 - core, :, span],
            dst_ref=paired.at[phase, piece, :, :, span],
            send_sem=pair_send.at[phase, piece],
            recv_sem=pair_recv.at[phase, piece, col],
            device_id={"tp": twin},
            device_id_type=MESH,
        )

    def side_of(phase, turn):
        half = phases[phase].half
        return 1 - half if turn == 0 else half

    def sum_step(phase, piece, turn, col):
        span = column_span(col)
        return pltpu.make_async_remote_copy(
            src_ref=outgoing.at[phase, piece, turn, :, span],
            dst_ref=landed.at[phase, piece, turn, :, span],
            send_sem=sum_send.at[phase, piece],
            recv_sem=sum_recv.at[phase, piece, turn, col],
            device_id={"tp": across},
            device_id_type=MESH,
        )

    def cross_step(phase, piece, col):
        span = column_span(col)
        return pltpu.make_async_remote_copy(
            src_ref=crossing.at[phase, piece, :, span],
            dst_ref=crossed.at[phase, piece, :, span],
            send_sem=cross_send.at[phase, piece],
            recv_sem=cross_recv.at[phase, piece, col],
            device_id={"fs": phases[phase].partner},
            device_id_type=MESH,
        )

    def all_sent(source, target, sem, device):
        pltpu.make_async_remote_copy(
            src_ref=source,
            dst_ref=target,
            send_sem=sem,
            recv_sem=pair_recv.at[0, 0, 0],
            device_id=device,
            device_id_type=MESH,
        ).wait_send()

    def group_rows(phase, side, piece, inside, size):
        start = piece * 2 * piece_rows + side * piece_rows + inside
        if phase == 3:
            start = piece * piece_rows + inside
        return pl.ds(aligned(start, 16), size)

    def put_slot(phase, which):
        before = (0, 4, 11, 18)[phase]
        kinds = ((1, 3, 4, 6), (0, 1, 2, 3, 4, 5, 6), (0, 1, 2, 3, 4, 5, 6), (0, 2, 5))[phase]
        return before + kinds.index(3 if which == 7 else which)

    def put_copy(phase, which, piece):
        half = phases[phase].half if phase < 3 else 0
        side = 1 - half if which in (3, 4, 6) else half
        place = far_spot if which in (5, 6, 7) else spot
        rows = normed.at[phase, group_rows(phase, side, piece, place * chunk, chunk), :]
        if which in (0, 3):
            target = {"tp": across}
        elif which in (1, 7):
            target = {"fs": phases[phase].partner}
        else:
            target = {"tp": twin}
        return pltpu.make_async_remote_copy(
            src_ref=rows,
            dst_ref=rows,
            send_sem=put_send.at[put_slot(phase, which), piece],
            recv_sem=put_recv.at[put_slot(phase, which), piece],
            device_id=target,
            device_id_type=MESH,
        )

    own_puts = ((1,), (0, 1, 2), (0, 1, 2), (0, 2))
    every_put = (0, 1, 2, 3, 4, 5, 6, 7)
    all_puts = ((1, 3, 4, 6), every_put, every_put, (0, 2, 5))

    def start_puts(phase, piece):
        for which in (1, 0, 2):
            if which in own_puts[phase]:
                put_copy(phase, which, piece).start()

    def routed(phase, which):
        split = phase > 0 and phase < 3 and phases[phase] is Near
        cut = piece_n // 2 if split else piece_n
        return range(cut) if which == 3 else range(cut, piece_n)

    def pieces_of(phase, which):
        if which in (3, 7):
            return routed(phase, which)
        return range(piece_n)

    def pass_near(phase, piece):
        put_copy(phase, 1, piece).wait_recv()
        if piece in routed(phase, 3):
            put_copy(phase, 3, piece).start()
        put_copy(phase, 4, piece).start()

    def pass_side(phase, piece):
        put_copy(phase, 0, piece).wait_recv()
        if phase < 3 and piece in routed(phase, 7):
            put_copy(phase, 7, piece).start()
        put_copy(phase, 5, piece).start()

    def pass_last(phase, piece):
        put_copy(phase, 3 if piece in routed(phase, 3) else 7, piece).wait_recv()
        put_copy(phase, 6, piece).start()

    def wait_puts(phase, piece, some):
        for which in some:
            put_copy(phase, which, piece).wait_recv()

    def finish_phase(phase):
        for piece in range(piece_n):
            target = paired.at[phase, piece]
            source = parts.at[phase, piece, :, 1 - core]
            all_sent(source, target, pair_send.at[phase, piece], {"tp": twin})
            source, target = outgoing.at[phase, piece], landed.at[phase, piece]
            all_sent(source, target, sum_send.at[phase, piece], {"tp": across})
            source, target = crossing.at[phase, piece], crossed.at[phase, piece]
            device = {"fs": phases[phase].partner}
            all_sent(source, target, cross_send.at[phase, piece], device)

    def finish_puts(phase):
        for which in all_puts[phase]:
            for piece in pieces_of(phase, which):
                put_copy(phase, which, piece).wait_send()

    def gain(row):
        return all_gains[row][...].astype(F32).reshape(1, width)

    def scaled(values, row):
        scale = lax.rsqrt(jnp.mean(values * values, axis=-1, keepdims=True) + 1e-06)
        return values * scale * gain(row)

    def norm_tokens(piece, start, size):
        def body(low):
            here = aligned(piece * piece_rows + start + low, 16)
            values = tokens[pl.ds(here, 16), :].astype(F32)
            target = group_rows(0, ffn.half, piece, start + low, 16)
            normed[0, target, :] = scaled(values, 0).astype(BF16)

        over_rows(size, 16, body)

    def pass_sum(phase, piece, turn, col):
        span = column_span(col)
        if turn == 0:
            pair_step(phase, piece, col).wait_recv()
        here = pl.ds(aligned((1 - chip) * chunk, 16), chunk)
        side = side_of(phase, turn)
        total = parts[phase, piece, side, core, here, span].astype(F32)
        total = total + paired[phase, piece, side, here, span].astype(F32)
        outgoing[phase, piece, turn, :, span] = total.astype(BF16)
        sum_step(phase, piece, turn, col).start()

    def cross_sums(phase, piece):
        side = 1 - phases[phase].half
        here = pl.ds(aligned(chip * chunk, 16), chunk)

        def step(col, carry):
            span = column_span(col)
            sum_step(phase, piece, 0, col).wait_recv()
            total = parts[phase, piece, side, core, here, span].astype(F32)
            total = total + paired[phase, piece, side, here, span].astype(F32)
            total = total + landed[phase, piece, 0, :, span].astype(F32)
            crossing[phase, piece, :, span] = total.astype(BF16)
            cross_step(phase, piece, col).start()
            return carry

        lax.fori_loop(0, columns, step, 0)

    def add_branch(phase, piece, load, row, factor):
        def wait(col, carry):
            sum_step(phase, piece, 1, col).wait_recv()
            cross_step(phase, piece, col).wait_recv()
            return carry

        lax.fori_loop(0, columns, wait, 0)
        side = phases[phase].half
        after = phases[phase + 1].half if phase < 2 else 0

        def body(low):
            rows = pl.ds(low, 16)
            here = pl.ds(aligned(chip * chunk + low, 16), 16)
            total = parts[phase, piece, side, core, here, :].astype(F32)
            total = total + paired[phase, piece, side, here, :].astype(F32)
            total = total + landed[phase, piece, 1, rows, :].astype(F32)
            total = total + crossed[phase, piece, rows, :].astype(F32)
            value = load(piece, low).astype(F32) + factor * scaled(total, row)
            value = value.astype(BF16)
            if phase < 2:
                streams[phase, pl.ds(aligned(piece * chunk + low, 16), 16), :] = value
                value = scaled(value.astype(F32), row + 1).astype(BF16)
            target = group_rows(phase + 1, after, piece, spot * chunk + low, 16)
            normed[phase + 1, target, :] = value

        over_rows(chunk, 16, body)
        start_puts(phase + 1, piece)

    def hidden_tile(phase, rows, cols):
        left = normed[phase, rows, :]
        gate = jnp.dot(left, gate_full[:, cols], preferred_element_type=F32)
        upper = jnp.dot(left, up_full[:, cols], preferred_element_type=F32)
        hidden[rows, cols] = (gate / (1.0 + jnp.exp(-gate)) * upper).astype(BF16)

    def piece_span(piece):
        return pl.ds(piece * 2 * piece_rows, 2 * piece_rows)

    def hidden_piece(phase, piece):
        rows = piece_span(piece)
        over_tiles(hidden.shape[1], lambda low, size: hidden_tile(phase, rows, pl.ds(low, size)))

    def project(phase, piece, left, right):
        rows = piece_span(piece)

        def step(col, carry):
            per = fs_n // columns
            terms = [
                jnp.dot(left[rows, :], right[col * per + b], preferred_element_type=F32)
                for b in range(per)
            ]
            terms = terms[0] if per == 1 else jnp.concatenate(terms, axis=1)
            terms = terms.astype(BF16).reshape(2, 2, chips * chunk, column)
            parts[phase, piece, :, :, :, column_span(col)] = terms
            pair_step(phase, piece, col).start()

            @pl.when(col >= LAG)
            def _():
                pass_sum(phase, piece, 0, col - LAG)

            return carry

        def late(turn):
            def step(col, carry):
                pass_sum(phase, piece, turn, col)
                return carry

            return step

        lax.fori_loop(0, columns, step, 0)
        lax.fori_loop(columns - LAG, columns, late(0), 0)
        lax.fori_loop(0, columns, late(1), 0)

    def mix(piece):
        at = lax.broadcasted_iota(jnp.int32, (BLOCK, BLOCK), 0)
        to = lax.broadcasted_iota(jnp.int32, (BLOCK, BLOCK), 1)
        here = mixed.shape[1]
        groups = here // GROUP_WIDTH
        shift = spatial_weight.shape[0] - groups
        all_gain = spatial_gain[...].astype(F32).reshape(1, spatial_gain.shape[0])
        all_gain = jnp.where(inner, all_gain[:, all_gain.shape[1] - here :], all_gain[:, :here])
        all_bias = spatial_bias[...].astype(F32)
        all_bias = jnp.where(inner, all_bias[shift:], all_bias[:groups])

        def block(n, carry):
            rows = pl.ds(aligned(piece * 2 * piece_rows + n * BLOCK, 16), BLOCK)
            left = normed[1, rows, :]
            every_v = gelu(jnp.dot(left, v_full[...], preferred_element_type=F32))
            every_u = gelu(jnp.dot(left, u_full[...], preferred_element_type=F32))
            for g in range(groups):
                span = slice(g * GROUP_WIDTH, (g + 1) * GROUP_WIDTH)
                v = every_v[:, span]
                v = v - jnp.mean(v, axis=-1, keepdims=True)
                v = v * lax.rsqrt(jnp.mean(v * v, axis=-1, keepdims=True) + 1e-05)
                v = (v * all_gain[:, span]).astype(BF16)
                weight = spatial_weight[g + shift * mixer.half].astype(F32)
                weight = jnp.where(at >= to, weight, 0.0).astype(BF16)
                bias = jnp.where(at == to, all_bias[g : g + 1, :], 0.0)
                bias = jnp.sum(bias, axis=1, keepdims=True)
                spatial = jnp.dot(weight, v, preferred_element_type=F32) + bias
                mixed[rows, span] = (every_u[:, span] * spatial).astype(BF16)
            return carry

        lax.fori_loop(0, 2 * piece_rows // BLOCK, block, 0)

    def load_tokens(piece, low):
        start = piece * piece_rows + spot * chunk + low
        return tokens[pl.ds(aligned(start, 16), 16), :]

    def load_stream(phase):
        return lambda piece, low: streams[phase, pl.ds(aligned(piece * chunk + low, 16), 16), :]

    def relays(some):
        for unit in some:
            relay(unit)

    for unit in range(AHEAD):
        send_own(unit)
    for w in range(6):
        for ok, copy in own_copies(w):
            guarded(ok, copy.start)
    for piece in range(piece_n):
        norm_tokens(piece, spot * chunk, chunk)
        start_puts(0, piece)

    def clear(pads, low):
        for full in pads:
            size = full.shape[-1] if len(full.shape) == 2 else full.shape[1]
            if low == size:
                continue
            if len(full.shape) == 2:
                full[:, pl.ds(low, size - low)] = jnp.zeros((full.shape[0], size - low), BF16)
            else:
                blank = jnp.zeros((fs_n, size - low, full.shape[2]), BF16)
                full[:, pl.ds(low, size - low), :] = blank

    @pl.when(outer)
    def _():
        small, extra = halves(gate_w.shape[1])
        if extra:
            clear((gate_full, up_full, down_full), small)
        clear((u_full, v_full, out_full), end_share(u_w.shape[1]))

    for piece in range(piece_n):
        for move in range(1, tp_n):
            norm_tokens(piece, lax.rem(spot + move, tp_n) * chunk, chunk)

    relays(range(0, 2))
    for piece in range(piece_n):
        pass_near(0, piece)
    relays(range(2, 4))
    send_some(first, "middle")
    for piece in range(piece_n):
        pass_last(0, piece)
    relays(range(4, last + 1))
    send_some(second, "middle")
    relay(downs[0])
    wait_weight(0)
    wait_weight(1)
    for piece in range(piece_n):
        wait_puts(0, piece, (4, 6))
        hidden_piece(0, piece)
        if piece == 0:
            relays(downs[1:2])
            send_some(third, "middle")
    relays(downs[2:])
    pl.when(inner)(lambda: relays(first))
    wait_weight(2)
    project(0, 0, hidden, down_full)
    project(0, 1, hidden, down_full)
    finish_sends(range(first[0]))
    send_some(first, "ends")
    pl.when(outer)(lambda: send_some(second + third, "ends"))
    pl.when(inner)(lambda: relays(second))
    cross_sums(0, 0)
    cross_sums(0, 1)
    pl.when(inner)(lambda: send_some(second, "ends"))
    pl.when(inner)(lambda: relays(third))
    pl.when(outer)(lambda: relays(first))
    add_branch(0, 0, load_tokens, 1, 0.5)
    pl.when(inner)(lambda: send_some(third, "ends"))
    add_branch(0, 1, load_tokens, 1, 0.5)
    pl.when(outer)(lambda: relays(second))
    pass_near(1, 0)
    pass_side(1, 0)
    wait_weight(3)
    wait_weight(4)
    pass_last(1, 0)
    pl.when(outer)(lambda: relays(third))
    pass_near(1, 1)
    pass_side(1, 1)
    wait_puts(1, 0, (2, 4, 5, 6))
    mix(0)
    wait_weight(5)
    project(1, 0, mixed, out_full)
    pass_last(1, 1)
    wait_puts(1, 1, (2, 4, 5, 6))
    cross_sums(1, 0)
    mix(1)
    project(1, 1, mixed, out_full)
    add_branch(1, 0, load_stream(0), 3, 1.0)
    cross_sums(1, 1)
    add_branch(1, 1, load_stream(0), 3, 1.0)
    pass_side(2, 0)
    pass_near(2, 0)
    pass_last(2, 0)
    pass_side(2, 1)
    wait_puts(2, 0, (2, 4, 5, 6))
    hidden_piece(2, 0)
    pass_near(2, 1)
    project(2, 0, hidden, down_full)
    cross_sums(2, 0)
    pass_last(2, 1)
    wait_puts(2, 1, (2, 4, 5, 6))
    hidden_piece(2, 1)
    project(2, 1, hidden, down_full)
    add_branch(2, 0, load_stream(1), 5, 0.5)
    cross_sums(2, 1)
    pass_side(3, 0)
    add_branch(2, 1, load_stream(1), 5, 0.5)
    pass_side(3, 1)
    finish_sends(range(first[0], len(units)))
    for phase in range(3):
        finish_phase(phase)
        finish_puts(phase)
    for piece in range(piece_n):
        wait_puts(3, piece, (2, 5))
    copy = pltpu.make_async_copy(normed.at[3, pl.ds(0, count), :], result, last_sem)
    copy.start()
    finish_puts(3)
    copy.wait()


def shared(
    sizes,
    tokens,
    ffn_pre_gain,
    gate_weight,
    up_weight,
    down_weight,
    ffn_post_gain,
    mix_pre_gain,
    mix_u_weight,
    mix_v_weight,
    spatial_gain,
    spatial_weight,
    spatial_bias,
    mix_out_weight,
    mix_post_gain,
    late_pre_gain,
    late_post_gain,
):
    grp_n, fs_n, tp_n = sizes
    count, width = tokens.shape
    small, extra = halves(gate_weight.shape[1])
    hidden_width = small + extra
    channels = mix_u_weight.shape[1] - end_share(mix_u_weight.shape[1])
    columns = math.gcd(fs_n, 4)
    pieces = count // BLOCK
    chunk = BLOCK // tp_n
    vmem = pl.BlockSpec(memory_space=pltpu.VMEM)
    hbm = pl.BlockSpec(memory_space=pl.ANY)
    weights = (gate_weight, up_weight, down_weight, mix_u_weight, mix_v_weight, mix_out_weight)
    units = weight_units([w.shape for w in weights], grp_n)
    unit_n = len(units)
    dma = pltpu.SemaphoreType.DMA
    return pl.pallas_call(
        functools.partial(shared_kernel, sizes, units),
        out_shape=jax.ShapeDtypeStruct((count, width), BF16),
        in_specs=[vmem] * 7 + [hbm, hbm, hbm, hbm, hbm, hbm, vmem, vmem, vmem],
        out_specs=hbm,
        scratch_shapes=[
            pltpu.VMEM((width, hidden_width), BF16),
            pltpu.VMEM((width, hidden_width), BF16),
            pltpu.VMEM((fs_n, hidden_width, down_weight.shape[1]), BF16),
            pltpu.VMEM((width, channels), BF16),
            pltpu.VMEM((width, channels), BF16),
            pltpu.VMEM((fs_n, channels, mix_out_weight.shape[1]), BF16),
            pltpu.VMEM((4, 2 * count, width), BF16),
            pltpu.VMEM((2 * count, hidden_width), BF16),
            pltpu.VMEM((2 * count, channels), BF16),
            pltpu.VMEM((2, count // tp_n, width), BF16),
            pltpu.VMEM((3, pieces, 2, 2, BLOCK // 2, width), BF16),
            pltpu.VMEM((3, pieces, 2, BLOCK // 2, width), BF16),
            pltpu.VMEM((3, pieces, 2, chunk, width), BF16),
            pltpu.VMEM((3, pieces, 2, chunk, width), BF16),
            pltpu.VMEM((3, pieces, chunk, width), BF16),
            pltpu.VMEM((3, pieces, chunk, width), BF16),
            dma((6, 2)),
            dma((unit_n, 2)),
            dma((unit_n, fs_n)),
            dma((unit_n, fs_n)),
            dma((unit_n, max(1, grp_n - 1))),
            dma((unit_n, max(1, grp_n - 1))),
            dma((3, pieces)),
            dma((3, pieces, columns)),
            dma((3, pieces)),
            dma((3, pieces, 2, columns)),
            dma((3, pieces)),
            dma((3, pieces, columns)),
            dma((21, pieces)),
            dma((21, pieces)),
            dma(()),
        ],
        compiler_params=pltpu.CompilerParams(
            collective_id=0, has_side_effects=True, vmem_limit_bytes=60 * 2**20
        ),
    )(
        tokens,
        ffn_pre_gain,
        ffn_post_gain,
        mix_pre_gain,
        mix_post_gain,
        late_pre_gain,
        late_post_gain,
        gate_weight,
        up_weight,
        down_weight,
        mix_u_weight,
        mix_v_weight,
        mix_out_weight,
        spatial_gain,
        spatial_weight,
        spatial_bias,
    )


def can_share(sizes, tokens, gate_weight, mix_u_weight):
    grp_n, fs_n, tp_n = sizes
    count = tokens.shape[0] // (grp_n * fs_n)
    rows = gate_weight.shape[0] // fs_n
    hidden_width = gate_weight.shape[1] // tp_n
    channels = mix_u_weight.shape[1] // tp_n
    return (
        tp_n == 4
        and fs_n == 4
        and count == 2 * BLOCK
        and rows % (32 * grp_n) == 0
        and hidden_width % 128 == 0
        and halves(hidden_width)[0] % (32 * grp_n) == 0
        and channels % (4 * GROUP_WIDTH) == 0
    )


def solution(mesh):
    in_specs = (
        P(("grp", "fs"), None),
        P(),
        P("fs", "tp"),
        P("fs", "tp"),
        P("tp", "fs"),
        P(),
        P(),
        P("fs", "tp"),
        P("fs", "tp"),
        P("tp"),
        P("tp", None, None),
        P("tp", None),
        P("tp", "fs"),
        P(),
        P(),
        P(),
    )
    out_specs = P(("grp", "fs"), None)
    sizes = (mesh.shape["grp"], mesh.shape["fs"], mesh.shape["tp"])

    def step(*arrays):
        plan = shared if can_share(sizes, arrays[0], arrays[2], arrays[7]) else shards
        body = functools.partial(plan, sizes)
        return jax.shard_map(
            body, mesh=mesh, in_specs=in_specs, out_specs=out_specs, check_vma=False
        )(*arrays)

    return step
```

```python
import functools
import math

import jax
import jax.numpy as jnp
from jax import lax
from jax.experimental import pallas as pl
from jax.experimental.pallas import tpu as pltpu
from jax.sharding import PartitionSpec as P

GROUP_WIDTH = 128
BLOCK = 128
TILE = 256
F32 = jnp.float32
BF16 = jnp.bfloat16
MESH = pl.DeviceIdType.MESH
SPLITS = (2, 2, 2, 1, 1, 2)
PIECE = 32


def aligned(value, unit):
    return value if isinstance(value, int) else pl.multiple_of(value, unit)


def over_tiles(width, body):
    count = width // TILE

    def step(i, carry):
        body(pl.multiple_of(i * TILE, TILE), TILE)
        return carry

    lax.fori_loop(0, count, step, 0)
    if width % TILE:
        body(count * TILE, width % TILE)


def over_rows(count, size, body):
    def step(i, carry):
        body(pl.multiple_of(i * size, size))
        return carry

    lax.fori_loop(0, count // size, step, 0)


def gelu(a):
    return 0.5 * a * (1.0 + lax.erf(a * (2.0**-0.5)))


def kernel(
    sizes,
    tokens,
    gain0,
    gain1,
    gain2,
    gain3,
    gain4,
    gain5,
    gate_w,
    up_w,
    down_w,
    u_w,
    v_w,
    out_w,
    spatial_gain,
    spatial_weight,
    spatial_bias,
    result,
    gate_full,
    up_full,
    down_full,
    u_full,
    v_full,
    out_full,
    normed,
    hidden,
    mixed,
    parts,
    paired,
    outgoing,
    landed,
    streams,
    own_sem,
    left_send,
    left_recv,
    right_send,
    right_recv,
    side_send,
    side_recv,
    pair_send,
    pair_recv,
    sum_send,
    sum_recv,
    twin_send,
    twin_recv,
    put_send,
    put_recv,
    pass_send,
    pass_recv,
    last_sem,
):
    grp_n, fs_n, tp_n = sizes
    grp, fs, tp = lax.axis_index("grp"), lax.axis_index("fs"), lax.axis_index("tp")
    shards = (gate_w, up_w, down_w, u_w, v_w, out_w)
    fulls = (gate_full, up_full, down_full, u_full, v_full, out_full)
    count, width = tokens.shape
    chunk = count // tp_n
    chips = tp_n // 2
    chip, core = tp // 2, lax.rem(tp, 2)
    twin = tp + 1 - 2 * core
    columns = pair_send.shape[1]
    column = width // columns
    piece_n = put_send.shape[1]
    piece_rows = chunk // piece_n
    all_gains = (gain0, gain1, gain2, gain3, gain4, gain5)

    barrier = pltpu.get_barrier_semaphore()
    for move in (1, fs_n - 1):
        pl.semaphore_signal(
            barrier, inc=1, device_id={"fs": lax.rem(fs + move, fs_n)}, device_id_type=MESH
        )
    for move in range(1, grp_n):
        pl.semaphore_signal(
            barrier, inc=1, device_id={"grp": lax.rem(grp + move, grp_n)}, device_id_type=MESH
        )
    for move in range(1, tp_n):
        pl.semaphore_signal(
            barrier, inc=1, device_id={"tp": lax.rem(tp + move, tp_n)}, device_id_type=MESH
        )
    pl.semaphore_wait(barrier, 2 + grp_n - 1 + tp_n - 1)

    units = []
    for w in range(6):
        piece = shards[w].shape[0] // grp_n // SPLITS[w]
        for s in range(SPLITS[w]):
            units.append((w, s * piece, piece))

    def unit_rows(unit):
        w, low, piece = units[unit]
        return aligned(grp * (shards[w].shape[0] // grp_n) + low, 16), piece

    def place(w, block, low, piece):
        if w in (2, 5):
            return fulls[w].at[block, pl.ds(low, piece), :]
        start = aligned(block * shards[w].shape[0] + low, 16)
        return fulls[w].at[pl.ds(start, piece), :]

    def own_copy(w):
        return pltpu.make_async_copy(
            shards[w], place(w, fs, 0, shards[w].shape[0]), own_sem.at[w]
        )

    def to_right(unit, hop, own=False):
        w = units[unit][0]
        low, piece = unit_rows(unit)
        target = place(w, fs - hop, low, piece)
        source = shards[w].at[pl.ds(low, piece), :] if own else target
        return pltpu.make_async_remote_copy(
            src_ref=source,
            dst_ref=target,
            send_sem=right_send.at[unit, hop],
            recv_sem=right_recv.at[unit, hop],
            device_id={"fs": fs + 1},
            device_id_type=MESH,
        )

    def to_left(unit, hop, own=False):
        w = units[unit][0]
        low, piece = unit_rows(unit)
        target = place(w, fs + hop, low, piece)
        source = shards[w].at[pl.ds(low, piece), :] if own else target
        return pltpu.make_async_remote_copy(
            src_ref=source,
            dst_ref=target,
            send_sem=left_send.at[unit, hop],
            recv_sem=left_recv.at[unit, hop],
            device_id={"fs": fs - 1},
            device_id_type=MESH,
        )

    def to_side(unit, side, hop, move):
        w = units[unit][0]
        low, piece = unit_rows(unit)
        block = fs - hop if side == 0 else fs + hop
        target = place(w, block, low, piece)
        return pltpu.make_async_remote_copy(
            src_ref=target,
            dst_ref=target,
            send_sem=side_send.at[unit, side, move - 1, hop],
            recv_sem=side_recv.at[unit, side, move - 1, hop],
            device_id={"grp": lax.rem(grp + move, grp_n)},
            device_id_type=MESH,
        )

    def send_own(unit):
        if unit >= len(units):
            return

        @pl.when(fs < fs_n - 1)
        def _():
            to_right(unit, 0, own=True).start()

        @pl.when(fs > 0)
        def _():
            to_left(unit, 0, own=True).start()

    def relay(unit):
        def step(hop, carry):
            @pl.when(fs >= hop)
            def _():
                to_right(unit, hop - 1).wait_recv()

                @pl.when(fs < fs_n - 1)
                def _():
                    to_right(unit, hop).start()

                for move in range(1, grp_n):
                    to_side(unit, 0, hop, move).start()

            @pl.when(fs + hop < fs_n)
            def _():
                to_left(unit, hop - 1).wait_recv()

                @pl.when(fs > 0)
                def _():
                    to_left(unit, hop).start()

                for move in range(1, grp_n):
                    to_side(unit, 1, hop, move).start()

            return carry

        lax.fori_loop(1, fs_n, step, 0)

    def wait_weight(w):
        own_copy(w).wait()
        for unit in range(len(units)):
            if units[unit][0] == w:

                def step(hop, carry, unit=unit):
                    for move in range(1, grp_n):

                        @pl.when(fs >= hop)
                        def _():
                            to_side(unit, 0, hop, move).wait_recv()

                        @pl.when(fs + hop < fs_n)
                        def _():
                            to_side(unit, 1, hop, move).wait_recv()

                    return carry

                lax.fori_loop(1, fs_n, step, 0)

    def finish_sends():
        for unit in range(len(units)):

            def step(hop, carry, unit=unit):
                @pl.when((fs >= hop) & (fs < fs_n - 1))
                def _():
                    to_right(unit, hop).wait_send()

                @pl.when((fs + hop < fs_n) & (fs > 0))
                def _():
                    to_left(unit, hop).wait_send()

                @pl.when(hop > 0)
                def _():
                    for move in range(1, grp_n):

                        @pl.when(fs >= hop)
                        def _():
                            to_side(unit, 0, hop, move).wait_send()

                        @pl.when(fs + hop < fs_n)
                        def _():
                            to_side(unit, 1, hop, move).wait_send()

                return carry

            lax.fori_loop(0, fs_n, step, 0)

    def other(move, which):
        return lax.rem(chip + move, chips) * 2 + which

    def origin(move, which):
        return lax.rem(chip + chips - move, chips) * 2 + which

    def chunk_rows(owner):
        return pl.ds(aligned(owner * chunk, 16), chunk)

    def column_span(col):
        return pl.ds(aligned(col * column, 128), column)

    def pair_copy(phase, col, move):
        span = column_span(col)
        return pltpu.make_async_remote_copy(
            src_ref=parts.at[phase, chunk_rows(other(move, 1 - core)), span],
            dst_ref=paired.at[phase, move, :, span],
            send_sem=pair_send.at[phase, col, move],
            recv_sem=pair_recv.at[phase, col, move],
            device_id={"tp": twin},
            device_id_type=MESH,
        )

    def sum_copy(phase, col, move):
        span = column_span(col)
        return pltpu.make_async_remote_copy(
            src_ref=outgoing.at[phase, move, :, span],
            dst_ref=landed.at[phase, move, :, span],
            send_sem=sum_send.at[phase, col, move],
            recv_sem=sum_recv.at[phase, col, move],
            device_id={"tp": other(move, core)},
            device_id_type=MESH,
        )

    def piece_span(owner, piece):
        return pl.ds(aligned(owner * chunk + piece * piece_rows, 16), piece_rows)

    def twin_copy(phase, piece):
        rows = piece_span(tp, piece)
        return pltpu.make_async_remote_copy(
            src_ref=streams.at[phase, rows, :],
            dst_ref=streams.at[phase, rows, :],
            send_sem=twin_send.at[phase, piece],
            recv_sem=twin_recv.at[phase, piece],
            device_id={"tp": twin},
            device_id_type=MESH,
        )

    def put_copy(phase, piece, move):
        rows = piece_span(tp, piece)
        return pltpu.make_async_remote_copy(
            src_ref=streams.at[phase, rows, :],
            dst_ref=streams.at[phase, rows, :],
            send_sem=put_send.at[phase, piece, move],
            recv_sem=put_recv.at[phase, piece, move],
            device_id={"tp": other(move, core)},
            device_id_type=MESH,
        )

    def pass_copy(phase, piece, move):
        rows = piece_span(origin(move, core), piece)
        return pltpu.make_async_remote_copy(
            src_ref=streams.at[phase, rows, :],
            dst_ref=streams.at[phase, rows, :],
            send_sem=pass_send.at[phase, piece, move],
            recv_sem=pass_recv.at[phase, piece, move],
            device_id={"tp": twin},
            device_id_type=MESH,
        )

    def gain(row):
        return all_gains[row][...].astype(F32).reshape(1, width)

    def norm_rows(load, row):
        def body(low):
            values = load(pl.ds(low, 32)).astype(F32)
            scale = lax.rsqrt(jnp.mean(values * values, axis=-1, keepdims=True) + 1e-06)
            normed[pl.ds(low, 32), :] = (values * scale * gain(row)).astype(BF16)

        over_rows(count, 32, body)

    def start_sums(phase, col):
        for move in range(1, chips):
            pair_copy(phase, col, move).wait_recv()
            span = column_span(col)
            mine = parts[phase, chunk_rows(other(move, core)), span].astype(F32)
            both = mine + paired[phase, move, :, span].astype(F32)
            outgoing[phase, move, :, span] = both.astype(BF16)
            sum_copy(phase, col, move).start()

    def add_branch(phase, load, row, factor):
        for col in range(columns):
            pair_copy(phase, col, 0).wait_recv()
            for move in range(1, chips):
                sum_copy(phase, col, move).wait_recv()
        for piece in range(piece_n):

            def body(low, piece=piece):
                here = pl.ds(aligned(piece * piece_rows + low, 16), 16)
                rows = pl.ds(aligned(tp * chunk + piece * piece_rows + low, 16), 16)
                total = parts[phase, rows, :].astype(F32) + paired[phase, 0, here, :].astype(F32)
                for move in range(1, chips):
                    total = total + landed[phase, move, here, :].astype(F32)
                scale = lax.rsqrt(jnp.mean(total * total, axis=-1, keepdims=True) + 1e-06)
                branch = total * scale * gain(row)
                streams[phase, rows, :] = (load(rows).astype(F32) + factor * branch).astype(BF16)

            over_rows(piece_rows, 16, body)
            for move in range(1, chips):
                put_copy(phase, piece, move).start()
            twin_copy(phase, piece).start()

    def wait_put(phase):
        for piece in range(piece_n):
            for move in range(1, chips):
                put_copy(phase, piece, move).wait_recv()
                pass_copy(phase, piece, move).start()
        for piece in range(piece_n):
            twin_copy(phase, piece).wait_recv()
            for move in range(1, chips):
                pass_copy(phase, piece, move).wait_recv()

    def finish_phase(phase):
        for col in range(columns):
            for move in range(chips):
                pair_copy(phase, col, move).wait_send()
            for move in range(1, chips):
                sum_copy(phase, col, move).wait_send()
        for piece in range(piece_n):
            twin_copy(phase, piece).wait_send()
            for move in range(1, chips):
                put_copy(phase, piece, move).wait_send()
                pass_copy(phase, piece, move).wait_send()

    def hidden_units():
        def body(low, size):
            cols = pl.ds(low, size)
            gate = jnp.dot(normed[...], gate_full[:, cols], preferred_element_type=F32)
            upper = jnp.dot(normed[...], up_full[:, cols], preferred_element_type=F32)
            hidden[:, cols] = (gate / (1.0 + jnp.exp(-gate)) * upper).astype(BF16)

        over_tiles(hidden.shape[1], body)

    def project(phase, left, right):
        blocks = fs_n // columns

        def step(col, carry):
            terms = [
                jnp.dot(left[...], right[col * blocks + b], preferred_element_type=F32)
                for b in range(blocks)
            ]
            terms = terms[0] if blocks == 1 else jnp.concatenate(terms, axis=1)
            parts[phase, :, column_span(col)] = terms.astype(BF16)
            for move in range(chips - 1, -1, -1):
                pair_copy(phase, col, move).start()

            @pl.when(col > 0)
            def _():
                start_sums(phase, col - 1)

            return carry

        lax.fori_loop(0, columns, step, 0)
        start_sums(phase, columns - 1)

    def mix():
        rows = lax.broadcasted_iota(jnp.int32, (BLOCK, BLOCK), 0)
        cols = lax.broadcasted_iota(jnp.int32, (BLOCK, BLOCK), 1)
        all_spatial_gain = spatial_gain[...].astype(F32).reshape(1, mixed.shape[1])
        for g in range(mixed.shape[1] // GROUP_WIDTH):
            span = slice(g * GROUP_WIDTH, (g + 1) * GROUP_WIDTH)
            v = gelu(jnp.dot(normed[...], v_full[:, span], preferred_element_type=F32))
            u = gelu(jnp.dot(normed[...], u_full[:, span], preferred_element_type=F32))
            v = v - jnp.mean(v, axis=-1, keepdims=True)
            v = v * lax.rsqrt(jnp.mean(v * v, axis=-1, keepdims=True) + 1e-05)
            v = (v * all_spatial_gain[:, span]).astype(BF16)
            weight = spatial_weight[g].astype(F32)
            weight = jnp.where(rows >= cols, weight, 0.0).astype(BF16)
            bias = spatial_bias[...][g : g + 1, :].astype(F32)
            bias = jnp.sum(jnp.where(rows == cols, bias, 0.0), axis=1, keepdims=True)
            for n in range(count // BLOCK):
                part = slice(n * BLOCK, (n + 1) * BLOCK)
                spatial = jnp.dot(weight, v[part], preferred_element_type=F32)
                spatial = spatial + bias
                mixed[part, span] = (u[part] * spatial).astype(BF16)

    load_tokens = lambda rows: tokens[rows, :]
    load_first = lambda rows: streams[0, rows, :]
    load_second = lambda rows: streams[1, rows, :]

    send_own(0)
    send_own(1)
    for w in range(6):
        own_copy(w).start()
    norm_rows(load_tokens, 0)

    for unit in range(5):
        relay(unit)
        send_own(unit + 2)
    wait_weight(0)
    wait_weight(1)
    hidden_units()
    relay(5)
    send_own(7)
    relay(6)
    send_own(8)
    send_own(9)
    wait_weight(2)
    project(0, hidden, down_full)
    relay(7)
    add_branch(0, load_tokens, 1, 0.5)
    relay(8)
    wait_put(0)
    norm_rows(load_first, 2)
    relay(9)
    wait_weight(3)
    wait_weight(4)
    mix()
    wait_weight(5)
    project(1, mixed, out_full)
    add_branch(1, load_first, 3, 1.0)
    wait_put(1)
    norm_rows(load_second, 4)
    hidden_units()
    project(2, hidden, down_full)
    add_branch(2, load_second, 5, 0.5)
    finish_sends()
    wait_put(2)
    last = pltpu.make_async_copy(streams.at[2], result, last_sem)
    last.start()
    for phase in range(3):
        finish_phase(phase)
    last.wait()


def shards(
    sizes,
    tokens,
    ffn_pre_gain,
    gate_weight,
    up_weight,
    down_weight,
    ffn_post_gain,
    mix_pre_gain,
    mix_u_weight,
    mix_v_weight,
    spatial_gain,
    spatial_weight,
    spatial_bias,
    mix_out_weight,
    mix_post_gain,
    late_pre_gain,
    late_post_gain,
):
    grp_n, fs_n, tp_n = sizes
    count, width = tokens.shape
    hidden_width = gate_weight.shape[1]
    channels = mix_u_weight.shape[1]
    columns = math.gcd(fs_n, 4)
    chips = tp_n // 2
    chunk = count // tp_n
    pieces = max(1, chunk // PIECE)
    vmem = pl.BlockSpec(memory_space=pltpu.VMEM)
    hbm = pl.BlockSpec(memory_space=pl.ANY)
    units = sum(SPLITS)
    dma = pltpu.SemaphoreType.DMA
    return pl.pallas_call(
        functools.partial(kernel, sizes),
        out_shape=jax.ShapeDtypeStruct((count, width), BF16),
        in_specs=[vmem] * 7 + [hbm, hbm, hbm, hbm, hbm, hbm, vmem, vmem, vmem],
        out_specs=hbm,
        scratch_shapes=[
            pltpu.VMEM((width, hidden_width), BF16),
            pltpu.VMEM((width, hidden_width), BF16),
            pltpu.VMEM((fs_n,) + down_weight.shape, BF16),
            pltpu.VMEM((width, channels), BF16),
            pltpu.VMEM((width, channels), BF16),
            pltpu.VMEM((fs_n,) + mix_out_weight.shape, BF16),
            pltpu.VMEM((count, width), BF16),
            pltpu.VMEM((count, hidden_width), BF16),
            pltpu.VMEM((count, channels), BF16),
            pltpu.VMEM((3, count, width), BF16),
            pltpu.VMEM((3, chips, chunk, width), BF16),
            pltpu.VMEM((3, chips, chunk, width), BF16),
            pltpu.VMEM((3, chips, chunk, width), BF16),
            pltpu.VMEM((3, count, width), BF16),
            dma((6,)),
            dma((units, fs_n)),
            dma((units, fs_n)),
            dma((units, fs_n)),
            dma((units, fs_n)),
            dma((units, 2, grp_n - 1, fs_n)),
            dma((units, 2, grp_n - 1, fs_n)),
            dma((3, columns, chips)),
            dma((3, columns, chips)),
            dma((3, columns, chips)),
            dma((3, columns, chips)),
            dma((3, pieces)),
            dma((3, pieces)),
            dma((3, pieces, chips)),
            dma((3, pieces, chips)),
            dma((3, pieces, chips)),
            dma((3, pieces, chips)),
            dma(()),
        ],
        compiler_params=pltpu.CompilerParams(
            collective_id=0, has_side_effects=True, vmem_limit_bytes=60 * 2**20
        ),
    )(
        tokens,
        ffn_pre_gain,
        ffn_post_gain,
        mix_pre_gain,
        mix_post_gain,
        late_pre_gain,
        late_post_gain,
        gate_weight,
        up_weight,
        down_weight,
        mix_u_weight,
        mix_v_weight,
        mix_out_weight,
        spatial_gain,
        spatial_weight,
        spatial_bias,
    )


PIECES = (2, 2, 2, 1, 1, 1)
AHEAD = 4
LAG = 2
ROW_SPLIT = (2, 5)
END_GROUPS = 1


def halves(size):
    small = size // 256 * 128
    return small, size - 2 * small


def end_share(size):
    return size // (4 * GROUP_WIDTH) * END_GROUPS * GROUP_WIDTH


def weight_units(shapes, grp_n):
    units = []
    for group in ((0, 1), (2,), (3,), (4,), (5,)):
        made = []
        for w in group:
            rows, cols = shapes[w]
            split = w in ROW_SPLIT
            size = rows if split else cols
            small, extra = halves(size)
            ends = end_share(size)
            if w < 3:
                cuts = [("side", (0, small + extra), 0, small, PIECES[w])]
                if extra:
                    cuts.append(("middle", (small, small), small, extra, 1))
            else:
                cuts = [
                    ("middle", (ends, ends), 0, size - ends, PIECES[w]),
                    ("ends", (0, 0), 0, ends, PIECES[w]),
                ]
            mine = []
            for route, source, target, span, pieces in cuts:
                share = (span if split else rows) // grp_n
                piece = share // pieces
                for n in range(pieces):
                    mine.append((w, route, source, target, span, share, n * piece, piece))
            made.append(mine)
        for n in range(max(len(mine) for mine in made)):
            units += [mine[n] for mine in made if n < len(mine)]
    return units


def shared_kernel(
    sizes,
    units,
    tokens,
    gain0,
    gain1,
    gain2,
    gain3,
    gain4,
    gain5,
    gate_w,
    up_w,
    down_w,
    u_w,
    v_w,
    out_w,
    spatial_gain,
    spatial_weight,
    spatial_bias,
    result,
    gate_full,
    up_full,
    down_full,
    u_full,
    v_full,
    out_full,
    normed,
    hidden,
    mixed,
    streams,
    parts,
    paired,
    outgoing,
    landed,
    crossing,
    crossed,
    own_sem,
    fresh_send,
    relay_send,
    relay_recv,
    side_send,
    side_recv,
    pair_send,
    pair_recv,
    sum_send,
    sum_recv,
    cross_send,
    cross_recv,
    put_send,
    put_recv,
    last_sem,
):
    grp_n, fs_n, tp_n = sizes
    grp, fs, tp = lax.axis_index("grp"), lax.axis_index("fs"), lax.axis_index("tp")
    shards = (gate_w, up_w, down_w, u_w, v_w, out_w)
    fulls = (gate_full, up_full, down_full, u_full, v_full, out_full)
    count, width = tokens.shape
    chips = tp_n // 2
    chip, core = tp // 2, lax.rem(tp, 2)
    twin = tp + 1 - 2 * core
    across = (1 - chip) * 2 + core
    spot = core * chips + chip
    far_spot = core * chips + 1 - chip
    columns = pair_recv.shape[2]
    column = width // columns
    piece_n = put_send.shape[1]
    piece_rows = count // piece_n
    chunk = piece_rows // tp_n
    all_gains = (gain0, gain1, gain2, gain3, gain4, gain5)
    middle = fs_n // 2

    last = [unit for unit in range(len(units)) if units[unit][0] < 2][-1]
    downs = [unit for unit in range(len(units)) if units[unit][0] == 2]
    first = [unit for unit in range(len(units)) if units[unit][0] == 3]
    second = [unit for unit in range(len(units)) if units[unit][0] == 4]
    third = [unit for unit in range(len(units)) if units[unit][0] == 5]

    inner = jnp.logical_and(fs > 0, fs < fs_n - 1)
    outer = jnp.logical_not(inner)

    class Near:
        half = jnp.where(inner, 1, 0)
        partner = fs + 1 - 2 * lax.rem(fs, 2)

    class Far:
        half = fs // middle
        partner = lax.rem(fs + middle, fs_n)

    ffn, mixer = Far, Near
    phases = (ffn, mixer, ffn)

    barrier = pltpu.get_barrier_semaphore()
    for move in range(1, fs_n):
        pl.semaphore_signal(
            barrier, inc=1, device_id={"fs": lax.rem(fs + move, fs_n)}, device_id_type=MESH
        )
    for move in range(1, grp_n):
        pl.semaphore_signal(
            barrier, inc=1, device_id={"grp": lax.rem(grp + move, grp_n)}, device_id_type=MESH
        )
    for move in range(1, tp_n):
        pl.semaphore_signal(
            barrier, inc=1, device_id={"tp": lax.rem(tp + move, tp_n)}, device_id_type=MESH
        )
    pl.semaphore_wait(barrier, fs_n - 1 + grp_n - 1 + tp_n - 1)

    def view(unit, block):
        w, _, _, target, span, share, low, rows = units[unit]
        start = grp * share + low
        if w in ROW_SPLIT:
            return fulls[w].at[block, pl.ds(aligned(target + start, 16), rows), :]
        start = aligned(block * shards[w].shape[0] + start, 16)
        return fulls[w].at[pl.ds(start, rows), pl.ds(target, span)]

    def shard_view(unit, half):
        w, _, source, _, span, share, low, rows = units[unit]
        start = grp * share + low
        base = source[0] + half * (source[1] - source[0])
        if w in ROW_SPLIT:
            return shards[w].at[pl.ds(aligned(base + start, 16), rows), :]
        return shards[w].at[pl.ds(aligned(start, 16), rows), pl.ds(aligned(base, 128), span)]

    def has(unit):
        return {"side": True, "middle": inner, "ends": outer}[units[unit][1]]

    def own_copies(w):
        size = shards[w].shape[0 if w in ROW_SPLIT else 1]
        small, extra = halves(size)
        ends = end_share(size)

        def part(base, low, span, sem):
            if w in ROW_SPLIT:
                source = shards[w].at[pl.ds(aligned(base, 128), span), :]
                target = fulls[w].at[fs, pl.ds(low, span), :]
            else:
                rows = shards[w].shape[0]
                source = shards[w].at[:, pl.ds(aligned(base, 128), span)]
                target = fulls[w].at[pl.ds(aligned(fs * rows, 16), rows), pl.ds(low, span)]
            return pltpu.make_async_copy(source, target, own_sem.at[w, sem])

        if w >= 3:
            return [(inner, part(ends, 0, size - ends, 0)), (outer, part(0, 0, ends, 1))]
        made = [(True, part(ffn.half * (small + extra), 0, small, 0))]
        if extra:
            made.append((inner, part(small, small, extra, 1)))
        return made

    def guarded(ok, act):
        if ok is True:
            act()
        else:
            pl.when(ok)(act)

    def fresh_copies(unit):
        route = units[unit][1]
        half = ffn.half
        block = view(unit, fs)

        def made(slot, half, target):
            return pltpu.make_async_remote_copy(
                src_ref=shard_view(unit, half),
                dst_ref=block,
                send_sem=fresh_send.at[unit, slot],
                recv_sem=relay_recv.at[unit, fs],
                device_id={"fs": target},
                device_id_type=MESH,
            )

        if route == "middle":
            return (
                (fs != middle - 1, lambda: made(0, 0, middle - 1)),
                (fs != middle, lambda: made(1, 0, middle)),
            )
        if route == "ends":
            return (
                (fs > 0, lambda: made(0, 0, 0)),
                (fs < fs_n - 1, lambda: made(1, 0, fs_n - 1)),
            )
        near = fs + 1 - 2 * lax.rem(fs, 2)
        return (
            (True, lambda: made(0, half, near)),
            (True, lambda: made(1, 1 - half, jnp.where(fs < middle, middle, middle - 1))),
        )

    def send_own(unit):
        if unit < first[0]:
            for ok, copy in fresh_copies(unit):
                guarded(ok, lambda copy=copy: copy().start())

    def send_some(some, route):
        for unit in some:
            if units[unit][1] == route:
                for ok, copy in fresh_copies(unit):
                    guarded(ok, lambda copy=copy: copy().start())

    def relay_copy(unit, block, leftward):
        target = view(unit, block)
        return pltpu.make_async_remote_copy(
            src_ref=target,
            dst_ref=target,
            send_sem=relay_send.at[unit, block],
            recv_sem=relay_recv.at[unit, block],
            device_id={"fs": fs - 1 if leftward else fs + 1},
            device_id_type=MESH,
        )

    def goes_on(unit, leftward, act):
        if units[unit][1] == "side":
            pl.when(lax.rem(fs, middle) == (1 if leftward else 0))(act)

    def side_copy(unit, block, move):
        target = view(unit, block)
        return pltpu.make_async_remote_copy(
            src_ref=target,
            dst_ref=target,
            send_sem=side_send.at[unit, move - 1],
            recv_sem=side_recv.at[unit, move - 1],
            device_id={"grp": lax.rem(grp + move, grp_n)},
            device_id_type=MESH,
        )

    def side_total(unit, move):
        w, _, _, target, span, share, low, rows = units[unit]
        others = fs_n - 1
        if w in ROW_SPLIT:
            total = fulls[w].at[pl.ds(0, others), pl.ds(0, rows), :]
        else:
            total = fulls[w].at[pl.ds(0, others * rows), pl.ds(target, span)]
        return pltpu.make_async_remote_copy(
            src_ref=total,
            dst_ref=total,
            send_sem=side_send.at[unit, move - 1],
            recv_sem=side_recv.at[unit, move - 1],
            device_id={"grp": lax.rem(grp + move, grp_n)},
            device_id_type=MESH,
        )

    def over_blocks(unit, act):
        def whole():
            def step(d, carry):
                @pl.when(fs + d < fs_n)
                def _():
                    act(fs + d, True)

                @pl.when(fs >= d)
                def _():
                    act(fs - d, False)

                return carry

            lax.fori_loop(1, fs_n, step, 0)

        guarded(has(unit), whole)

    def relay(unit):
        def act(block, leftward):
            relay_copy(unit, block, leftward).wait_recv()

            goes_on(unit, leftward, lambda: relay_copy(unit, block, leftward).start())

            for move in range(1, grp_n):
                side_copy(unit, block, move).start()

        over_blocks(unit, act)
        send_own(unit + AHEAD)

    def wait_weight(w):
        for ok, copy in own_copies(w):
            guarded(ok, copy.wait)
        for unit in range(len(units)):
            if units[unit][0] == w:

                def act(unit=unit):
                    for move in range(1, grp_n):
                        side_total(unit, move).wait_recv()

                guarded(has(unit), act)

    def finish_sends(some):
        for unit in some:
            for ok, copy in fresh_copies(unit):
                guarded(ok, lambda copy=copy: copy().wait_send())

            def act(block, leftward, unit=unit):
                goes_on(unit, leftward, lambda: relay_copy(unit, block, leftward).wait_send())

            def sides(unit=unit):
                for move in range(1, grp_n):
                    side_total(unit, move).wait_send()

            over_blocks(unit, act)
            guarded(has(unit), sides)

    def column_span(col):
        return pl.ds(aligned(col * column, 128), column)

    def pair_step(phase, piece, col):
        span = column_span(col)
        return pltpu.make_async_remote_copy(
            src_ref=parts.at[phase, piece, :, 1 - core, :, span],
            dst_ref=paired.at[phase, piece, :, :, span],
            send_sem=pair_send.at[phase, piece],
            recv_sem=pair_recv.at[phase, piece, col],
            device_id={"tp": twin},
            device_id_type=MESH,
        )

    def side_of(phase, turn):
        half = phases[phase].half
        return 1 - half if turn == 0 else half

    def sum_step(phase, piece, turn, col):
        span = column_span(col)
        return pltpu.make_async_remote_copy(
            src_ref=outgoing.at[phase, piece, turn, :, span],
            dst_ref=landed.at[phase, piece, turn, :, span],
            send_sem=sum_send.at[phase, piece],
            recv_sem=sum_recv.at[phase, piece, turn, col],
            device_id={"tp": across},
            device_id_type=MESH,
        )

    def cross_step(phase, piece, col):
        span = column_span(col)
        return pltpu.make_async_remote_copy(
            src_ref=crossing.at[phase, piece, :, span],
            dst_ref=crossed.at[phase, piece, :, span],
            send_sem=cross_send.at[phase, piece],
            recv_sem=cross_recv.at[phase, piece, col],
            device_id={"fs": phases[phase].partner},
            device_id_type=MESH,
        )

    def all_sent(source, target, sem, device):
        pltpu.make_async_remote_copy(
            src_ref=source,
            dst_ref=target,
            send_sem=sem,
            recv_sem=pair_recv.at[0, 0, 0],
            device_id=device,
            device_id_type=MESH,
        ).wait_send()

    def group_rows(phase, side, piece, inside, size):
        start = piece * 2 * piece_rows + side * piece_rows + inside
        if phase == 3:
            start = piece * piece_rows + inside
        return pl.ds(aligned(start, 16), size)

    def put_slot(phase, which):
        before = (0, 4, 11, 18)[phase]
        kinds = ((1, 3, 4, 6), (0, 1, 2, 3, 4, 5, 6), (0, 1, 2, 3, 4, 5, 6), (0, 2, 5))[phase]
        return before + kinds.index(3 if which == 7 else which)

    def put_copy(phase, which, piece):
        half = phases[phase].half if phase < 3 else 0
        side = 1 - half if which in (3, 4, 6) else half
        place = far_spot if which in (5, 6, 7) else spot
        rows = normed.at[phase, group_rows(phase, side, piece, place * chunk, chunk), :]
        if which in (0, 3):
            target = {"tp": across}
        elif which in (1, 7):
            target = {"fs": phases[phase].partner}
        else:
            target = {"tp": twin}
        return pltpu.make_async_remote_copy(
            src_ref=rows,
            dst_ref=rows,
            send_sem=put_send.at[put_slot(phase, which), piece],
            recv_sem=put_recv.at[put_slot(phase, which), piece],
            device_id=target,
            device_id_type=MESH,
        )

    own_puts = ((1,), (0, 1, 2), (0, 1, 2), (0, 2))
    every_put = (0, 1, 2, 3, 4, 5, 6, 7)
    all_puts = ((1, 3, 4, 6), every_put, every_put, (0, 2, 5))

    def start_puts(phase, piece):
        for which in (1, 0, 2):
            if which in own_puts[phase]:
                put_copy(phase, which, piece).start()

    def routed(phase, which):
        split = phase > 0 and phase < 3 and phases[phase] is Near
        cut = piece_n // 2 if split else piece_n
        return range(cut) if which == 3 else range(cut, piece_n)

    def pieces_of(phase, which):
        if which in (3, 7):
            return routed(phase, which)
        return range(piece_n)

    def pass_near(phase, piece):
        put_copy(phase, 1, piece).wait_recv()
        if piece in routed(phase, 3):
            put_copy(phase, 3, piece).start()
        put_copy(phase, 4, piece).start()

    def pass_side(phase, piece):
        put_copy(phase, 0, piece).wait_recv()
        if phase < 3 and piece in routed(phase, 7):
            put_copy(phase, 7, piece).start()
        put_copy(phase, 5, piece).start()

    def pass_last(phase, piece):
        put_copy(phase, 3 if piece in routed(phase, 3) else 7, piece).wait_recv()
        put_copy(phase, 6, piece).start()

    def wait_puts(phase, piece, some):
        for which in some:
            put_copy(phase, which, piece).wait_recv()

    def finish_phase(phase):
        for piece in range(piece_n):
            target = paired.at[phase, piece]
            source = parts.at[phase, piece, :, 1 - core]
            all_sent(source, target, pair_send.at[phase, piece], {"tp": twin})
            source, target = outgoing.at[phase, piece], landed.at[phase, piece]
            all_sent(source, target, sum_send.at[phase, piece], {"tp": across})
            source, target = crossing.at[phase, piece], crossed.at[phase, piece]
            device = {"fs": phases[phase].partner}
            all_sent(source, target, cross_send.at[phase, piece], device)

    def finish_puts(phase):
        for which in all_puts[phase]:
            for piece in pieces_of(phase, which):
                put_copy(phase, which, piece).wait_send()

    def gain(row):
        return all_gains[row][...].astype(F32).reshape(1, width)

    def scaled(values, row):
        scale = lax.rsqrt(jnp.mean(values * values, axis=-1, keepdims=True) + 1e-06)
        return values * scale * gain(row)

    def norm_tokens(piece, start, size):
        def body(low):
            here = aligned(piece * piece_rows + start + low, 16)
            values = tokens[pl.ds(here, 16), :].astype(F32)
            target = group_rows(0, ffn.half, piece, start + low, 16)
            normed[0, target, :] = scaled(values, 0).astype(BF16)

        over_rows(size, 16, body)

    def pass_sum(phase, piece, turn, col):
        span = column_span(col)
        if turn == 0:
            pair_step(phase, piece, col).wait_recv()
        here = pl.ds(aligned((1 - chip) * chunk, 16), chunk)
        side = side_of(phase, turn)
        total = parts[phase, piece, side, core, here, span].astype(F32)
        total = total + paired[phase, piece, side, here, span].astype(F32)
        outgoing[phase, piece, turn, :, span] = total.astype(BF16)
        sum_step(phase, piece, turn, col).start()

    def cross_sums(phase, piece):
        side = 1 - phases[phase].half
        here = pl.ds(aligned(chip * chunk, 16), chunk)

        def step(col, carry):
            span = column_span(col)
            sum_step(phase, piece, 0, col).wait_recv()
            total = parts[phase, piece, side, core, here, span].astype(F32)
            total = total + paired[phase, piece, side, here, span].astype(F32)
            total = total + landed[phase, piece, 0, :, span].astype(F32)
            crossing[phase, piece, :, span] = total.astype(BF16)
            cross_step(phase, piece, col).start()
            return carry

        lax.fori_loop(0, columns, step, 0)

    def add_branch(phase, piece, load, row, factor):
        def wait(col, carry):
            sum_step(phase, piece, 1, col).wait_recv()
            cross_step(phase, piece, col).wait_recv()
            return carry

        lax.fori_loop(0, columns, wait, 0)
        side = phases[phase].half
        after = phases[phase + 1].half if phase < 2 else 0

        def body(low):
            rows = pl.ds(low, 16)
            here = pl.ds(aligned(chip * chunk + low, 16), 16)
            total = parts[phase, piece, side, core, here, :].astype(F32)
            total = total + paired[phase, piece, side, here, :].astype(F32)
            total = total + landed[phase, piece, 1, rows, :].astype(F32)
            total = total + crossed[phase, piece, rows, :].astype(F32)
            value = load(piece, low).astype(F32) + factor * scaled(total, row)
            value = value.astype(BF16)
            if phase < 2:
                streams[phase, pl.ds(aligned(piece * chunk + low, 16), 16), :] = value
                value = scaled(value.astype(F32), row + 1).astype(BF16)
            target = group_rows(phase + 1, after, piece, spot * chunk + low, 16)
            normed[phase + 1, target, :] = value

        over_rows(chunk, 16, body)
        start_puts(phase + 1, piece)

    def hidden_tile(phase, rows, cols):
        left = normed[phase, rows, :]
        gate = jnp.dot(left, gate_full[:, cols], preferred_element_type=F32)
        upper = jnp.dot(left, up_full[:, cols], preferred_element_type=F32)
        hidden[rows, cols] = (gate / (1.0 + jnp.exp(-gate)) * upper).astype(BF16)

    def piece_span(piece):
        return pl.ds(piece * 2 * piece_rows, 2 * piece_rows)

    def hidden_piece(phase, piece):
        rows = piece_span(piece)
        over_tiles(hidden.shape[1], lambda low, size: hidden_tile(phase, rows, pl.ds(low, size)))

    def project(phase, piece, left, right):
        rows = piece_span(piece)

        def step(col, carry):
            per = fs_n // columns
            terms = [
                jnp.dot(left[rows, :], right[col * per + b], preferred_element_type=F32)
                for b in range(per)
            ]
            terms = terms[0] if per == 1 else jnp.concatenate(terms, axis=1)
            terms = terms.astype(BF16).reshape(2, 2, chips * chunk, column)
            parts[phase, piece, :, :, :, column_span(col)] = terms
            pair_step(phase, piece, col).start()

            @pl.when(col >= LAG)
            def _():
                pass_sum(phase, piece, 0, col - LAG)

            return carry

        def late(turn):
            def step(col, carry):
                pass_sum(phase, piece, turn, col)
                return carry

            return step

        lax.fori_loop(0, columns, step, 0)
        lax.fori_loop(columns - LAG, columns, late(0), 0)
        lax.fori_loop(0, columns, late(1), 0)

    def mix(piece):
        at = lax.broadcasted_iota(jnp.int32, (BLOCK, BLOCK), 0)
        to = lax.broadcasted_iota(jnp.int32, (BLOCK, BLOCK), 1)
        here = mixed.shape[1]
        groups = here // GROUP_WIDTH
        shift = spatial_weight.shape[0] - groups
        all_gain = spatial_gain[...].astype(F32).reshape(1, spatial_gain.shape[0])
        all_gain = jnp.where(inner, all_gain[:, all_gain.shape[1] - here :], all_gain[:, :here])
        all_bias = spatial_bias[...].astype(F32)
        all_bias = jnp.where(inner, all_bias[shift:], all_bias[:groups])

        def block(n, carry):
            rows = pl.ds(aligned(piece * 2 * piece_rows + n * BLOCK, 16), BLOCK)
            left = normed[1, rows, :]
            every_v = gelu(jnp.dot(left, v_full[...], preferred_element_type=F32))
            every_u = gelu(jnp.dot(left, u_full[...], preferred_element_type=F32))
            for g in range(groups):
                span = slice(g * GROUP_WIDTH, (g + 1) * GROUP_WIDTH)
                v = every_v[:, span]
                v = v - jnp.mean(v, axis=-1, keepdims=True)
                v = v * lax.rsqrt(jnp.mean(v * v, axis=-1, keepdims=True) + 1e-05)
                v = (v * all_gain[:, span]).astype(BF16)
                weight = spatial_weight[g + shift * mixer.half].astype(F32)
                weight = jnp.where(at >= to, weight, 0.0).astype(BF16)
                bias = jnp.where(at == to, all_bias[g : g + 1, :], 0.0)
                bias = jnp.sum(bias, axis=1, keepdims=True)
                spatial = jnp.dot(weight, v, preferred_element_type=F32) + bias
                mixed[rows, span] = (every_u[:, span] * spatial).astype(BF16)
            return carry

        lax.fori_loop(0, 2 * piece_rows // BLOCK, block, 0)

    def load_tokens(piece, low):
        start = piece * piece_rows + spot * chunk + low
        return tokens[pl.ds(aligned(start, 16), 16), :]

    def load_stream(phase):
        return lambda piece, low: streams[phase, pl.ds(aligned(piece * chunk + low, 16), 16), :]

    def relays(some):
        for unit in some:
            relay(unit)

    for unit in range(AHEAD):
        send_own(unit)
    for w in range(6):
        for ok, copy in own_copies(w):
            guarded(ok, copy.start)
    for piece in range(piece_n):
        norm_tokens(piece, spot * chunk, chunk)
        start_puts(0, piece)

    def clear(pads, low):
        for full in pads:
            size = full.shape[-1] if len(full.shape) == 2 else full.shape[1]
            if low == size:
                continue
            if len(full.shape) == 2:
                full[:, pl.ds(low, size - low)] = jnp.zeros((full.shape[0], size - low), BF16)
            else:
                blank = jnp.zeros((fs_n, size - low, full.shape[2]), BF16)
                full[:, pl.ds(low, size - low), :] = blank

    @pl.when(outer)
    def _():
        small, extra = halves(gate_w.shape[1])
        if extra:
            clear((gate_full, up_full, down_full), small)
        clear((u_full, v_full, out_full), end_share(u_w.shape[1]))

    for piece in range(piece_n):
        for move in range(1, tp_n):
            norm_tokens(piece, lax.rem(spot + move, tp_n) * chunk, chunk)

    relays(range(0, 4))
    for piece in range(piece_n):
        pass_near(0, piece)
    send_some(first, "middle")
    relays(range(4, last + 1))
    for piece in range(piece_n):
        pass_last(0, piece)
    send_some(second, "middle")
    relay(downs[0])
    wait_weight(0)
    wait_weight(1)
    for piece in range(piece_n):
        wait_puts(0, piece, (4, 6))
        hidden_piece(0, piece)
        if piece == 0:
            relays(downs[1:2])
            send_some(third, "middle")
    relays(downs[2:])
    pl.when(inner)(lambda: relays(first))
    wait_weight(2)
    project(0, 0, hidden, down_full)
    project(0, 1, hidden, down_full)
    finish_sends(range(first[0]))
    send_some(first, "ends")
    pl.when(outer)(lambda: send_some(second + third, "ends"))
    pl.when(inner)(lambda: relays(second))
    cross_sums(0, 0)
    cross_sums(0, 1)
    pl.when(inner)(lambda: send_some(second, "ends"))
    pl.when(inner)(lambda: relays(third))
    pl.when(outer)(lambda: relays(first))
    add_branch(0, 0, load_tokens, 1, 0.5)
    pl.when(inner)(lambda: send_some(third, "ends"))
    add_branch(0, 1, load_tokens, 1, 0.5)
    pl.when(outer)(lambda: relays(second))
    pass_near(1, 0)
    pass_side(1, 0)
    wait_weight(3)
    wait_weight(4)
    pass_last(1, 0)
    pl.when(outer)(lambda: relays(third))
    pass_near(1, 1)
    pass_side(1, 1)
    wait_puts(1, 0, (2, 4, 5, 6))
    mix(0)
    wait_weight(5)
    project(1, 0, mixed, out_full)
    pass_last(1, 1)
    wait_puts(1, 1, (2, 4, 5, 6))
    cross_sums(1, 0)
    mix(1)
    project(1, 1, mixed, out_full)
    add_branch(1, 0, load_stream(0), 3, 1.0)
    cross_sums(1, 1)
    add_branch(1, 1, load_stream(0), 3, 1.0)
    pass_side(2, 0)
    pass_near(2, 0)
    pass_last(2, 0)
    pass_side(2, 1)
    wait_puts(2, 0, (2, 4, 5, 6))
    hidden_piece(2, 0)
    pass_near(2, 1)
    project(2, 0, hidden, down_full)
    cross_sums(2, 0)
    pass_last(2, 1)
    wait_puts(2, 1, (2, 4, 5, 6))
    hidden_piece(2, 1)
    project(2, 1, hidden, down_full)
    add_branch(2, 0, load_stream(1), 5, 0.5)
    cross_sums(2, 1)
    pass_side(3, 0)
    add_branch(2, 1, load_stream(1), 5, 0.5)
    pass_side(3, 1)
    finish_sends(range(first[0], len(units)))
    for phase in range(3):
        finish_phase(phase)
        finish_puts(phase)
    for piece in range(piece_n):
        wait_puts(3, piece, (2, 5))
    copy = pltpu.make_async_copy(normed.at[3, pl.ds(0, count), :], result, last_sem)
    copy.start()
    finish_puts(3)
    copy.wait()


def shared(
    sizes,
    tokens,
    ffn_pre_gain,
    gate_weight,
    up_weight,
    down_weight,
    ffn_post_gain,
    mix_pre_gain,
    mix_u_weight,
    mix_v_weight,
    spatial_gain,
    spatial_weight,
    spatial_bias,
    mix_out_weight,
    mix_post_gain,
    late_pre_gain,
    late_post_gain,
):
    grp_n, fs_n, tp_n = sizes
    count, width = tokens.shape
    small, extra = halves(gate_weight.shape[1])
    hidden_width = small + extra
    channels = mix_u_weight.shape[1] - end_share(mix_u_weight.shape[1])
    columns = math.gcd(fs_n, 4)
    pieces = count // BLOCK
    chunk = BLOCK // tp_n
    vmem = pl.BlockSpec(memory_space=pltpu.VMEM)
    hbm = pl.BlockSpec(memory_space=pl.ANY)
    weights = (gate_weight, up_weight, down_weight, mix_u_weight, mix_v_weight, mix_out_weight)
    units = weight_units([w.shape for w in weights], grp_n)
    unit_n = len(units)
    dma = pltpu.SemaphoreType.DMA
    return pl.pallas_call(
        functools.partial(shared_kernel, sizes, units),
        out_shape=jax.ShapeDtypeStruct((count, width), BF16),
        in_specs=[vmem] * 7 + [hbm, hbm, hbm, hbm, hbm, hbm, vmem, vmem, vmem],
        out_specs=hbm,
        scratch_shapes=[
            pltpu.VMEM((width, hidden_width), BF16),
            pltpu.VMEM((width, hidden_width), BF16),
            pltpu.VMEM((fs_n, hidden_width, down_weight.shape[1]), BF16),
            pltpu.VMEM((width, channels), BF16),
            pltpu.VMEM((width, channels), BF16),
            pltpu.VMEM((fs_n, channels, mix_out_weight.shape[1]), BF16),
            pltpu.VMEM((4, 2 * count, width), BF16),
            pltpu.VMEM((2 * count, hidden_width), BF16),
            pltpu.VMEM((2 * count, channels), BF16),
            pltpu.VMEM((2, count // tp_n, width), BF16),
            pltpu.VMEM((3, pieces, 2, 2, BLOCK // 2, width), BF16),
            pltpu.VMEM((3, pieces, 2, BLOCK // 2, width), BF16),
            pltpu.VMEM((3, pieces, 2, chunk, width), BF16),
            pltpu.VMEM((3, pieces, 2, chunk, width), BF16),
            pltpu.VMEM((3, pieces, chunk, width), BF16),
            pltpu.VMEM((3, pieces, chunk, width), BF16),
            dma((6, 2)),
            dma((unit_n, 2)),
            dma((unit_n, fs_n)),
            dma((unit_n, fs_n)),
            dma((unit_n, max(1, grp_n - 1))),
            dma((unit_n, max(1, grp_n - 1))),
            dma((3, pieces)),
            dma((3, pieces, columns)),
            dma((3, pieces)),
            dma((3, pieces, 2, columns)),
            dma((3, pieces)),
            dma((3, pieces, columns)),
            dma((21, pieces)),
            dma((21, pieces)),
            dma(()),
        ],
        compiler_params=pltpu.CompilerParams(
            collective_id=0, has_side_effects=True, vmem_limit_bytes=60 * 2**20
        ),
    )(
        tokens,
        ffn_pre_gain,
        ffn_post_gain,
        mix_pre_gain,
        mix_post_gain,
        late_pre_gain,
        late_post_gain,
        gate_weight,
        up_weight,
        down_weight,
        mix_u_weight,
        mix_v_weight,
        mix_out_weight,
        spatial_gain,
        spatial_weight,
        spatial_bias,
    )


def can_share(sizes, tokens, gate_weight, mix_u_weight):
    grp_n, fs_n, tp_n = sizes
    count = tokens.shape[0] // (grp_n * fs_n)
    rows = gate_weight.shape[0] // fs_n
    hidden_width = gate_weight.shape[1] // tp_n
    channels = mix_u_weight.shape[1] // tp_n
    return (
        tp_n == 4
        and fs_n == 4
        and count == 2 * BLOCK
        and rows % (32 * grp_n) == 0
        and hidden_width % 128 == 0
        and halves(hidden_width)[0] % (32 * grp_n) == 0
        and channels % (4 * GROUP_WIDTH) == 0
    )


def solution(mesh):
    in_specs = (
        P(("grp", "fs"), None),
        P(),
        P("fs", "tp"),
        P("fs", "tp"),
        P("tp", "fs"),
        P(),
        P(),
        P("fs", "tp"),
        P("fs", "tp"),
        P("tp"),
        P("tp", None, None),
        P("tp", None),
        P("tp", "fs"),
        P(),
        P(),
        P(),
    )
    out_specs = P(("grp", "fs"), None)
    sizes = (mesh.shape["grp"], mesh.shape["fs"], mesh.shape["tp"])

    def step(*arrays):
        plan = shared if can_share(sizes, arrays[0], arrays[2], arrays[7]) else shards
        body = functools.partial(plan, sizes)
        return jax.shard_map(
            body, mesh=mesh, in_specs=in_specs, out_specs=out_specs, check_vma=False
        )(*arrays)

    return step
```

```python
import functools
import math

import jax
import jax.numpy as jnp
from jax import lax
from jax.experimental import pallas as pl
from jax.experimental.pallas import tpu as pltpu
from jax.sharding import PartitionSpec as P

GROUP_WIDTH = 128
BLOCK = 128
TILE = 256
F32 = jnp.float32
BF16 = jnp.bfloat16
MESH = pl.DeviceIdType.MESH
SPLITS = (2, 2, 2, 1, 1, 2)
PIECE = 32


def aligned(value, unit):
    return value if isinstance(value, int) else pl.multiple_of(value, unit)


def over_tiles(width, body):
    count = width // TILE

    def step(i, carry):
        body(pl.multiple_of(i * TILE, TILE), TILE)
        return carry

    lax.fori_loop(0, count, step, 0)
    if width % TILE:
        body(count * TILE, width % TILE)


def over_rows(count, size, body):
    def step(i, carry):
        body(pl.multiple_of(i * size, size))
        return carry

    lax.fori_loop(0, count // size, step, 0)


def gelu(a):
    return 0.5 * a * (1.0 + lax.erf(a * (2.0**-0.5)))


def kernel(
    sizes,
    tokens,
    gain0,
    gain1,
    gain2,
    gain3,
    gain4,
    gain5,
    gate_w,
    up_w,
    down_w,
    u_w,
    v_w,
    out_w,
    spatial_gain,
    spatial_weight,
    spatial_bias,
    result,
    gate_full,
    up_full,
    down_full,
    u_full,
    v_full,
    out_full,
    normed,
    hidden,
    mixed,
    parts,
    paired,
    outgoing,
    landed,
    streams,
    own_sem,
    left_send,
    left_recv,
    right_send,
    right_recv,
    side_send,
    side_recv,
    pair_send,
    pair_recv,
    sum_send,
    sum_recv,
    twin_send,
    twin_recv,
    put_send,
    put_recv,
    pass_send,
    pass_recv,
    last_sem,
):
    grp_n, fs_n, tp_n = sizes
    grp, fs, tp = lax.axis_index("grp"), lax.axis_index("fs"), lax.axis_index("tp")
    shards = (gate_w, up_w, down_w, u_w, v_w, out_w)
    fulls = (gate_full, up_full, down_full, u_full, v_full, out_full)
    count, width = tokens.shape
    chunk = count // tp_n
    chips = tp_n // 2
    chip, core = tp // 2, lax.rem(tp, 2)
    twin = tp + 1 - 2 * core
    columns = pair_send.shape[1]
    column = width // columns
    piece_n = put_send.shape[1]
    piece_rows = chunk // piece_n
    all_gains = (gain0, gain1, gain2, gain3, gain4, gain5)

    barrier = pltpu.get_barrier_semaphore()
    for move in (1, fs_n - 1):
        pl.semaphore_signal(
            barrier, inc=1, device_id={"fs": lax.rem(fs + move, fs_n)}, device_id_type=MESH
        )
    for move in range(1, grp_n):
        pl.semaphore_signal(
            barrier, inc=1, device_id={"grp": lax.rem(grp + move, grp_n)}, device_id_type=MESH
        )
    for move in range(1, tp_n):
        pl.semaphore_signal(
            barrier, inc=1, device_id={"tp": lax.rem(tp + move, tp_n)}, device_id_type=MESH
        )
    pl.semaphore_wait(barrier, 2 + grp_n - 1 + tp_n - 1)

    units = []
    for w in range(6):
        piece = shards[w].shape[0] // grp_n // SPLITS[w]
        for s in range(SPLITS[w]):
            units.append((w, s * piece, piece))

    def unit_rows(unit):
        w, low, piece = units[unit]
        return aligned(grp * (shards[w].shape[0] // grp_n) + low, 16), piece

    def place(w, block, low, piece):
        if w in (2, 5):
            return fulls[w].at[block, pl.ds(low, piece), :]
        start = aligned(block * shards[w].shape[0] + low, 16)
        return fulls[w].at[pl.ds(start, piece), :]

    def own_copy(w):
        return pltpu.make_async_copy(
            shards[w], place(w, fs, 0, shards[w].shape[0]), own_sem.at[w]
        )

    def to_right(unit, hop, own=False):
        w = units[unit][0]
        low, piece = unit_rows(unit)
        target = place(w, fs - hop, low, piece)
        source = shards[w].at[pl.ds(low, piece), :] if own else target
        return pltpu.make_async_remote_copy(
            src_ref=source,
            dst_ref=target,
            send_sem=right_send.at[unit, hop],
            recv_sem=right_recv.at[unit, hop],
            device_id={"fs": fs + 1},
            device_id_type=MESH,
        )

    def to_left(unit, hop, own=False):
        w = units[unit][0]
        low, piece = unit_rows(unit)
        target = place(w, fs + hop, low, piece)
        source = shards[w].at[pl.ds(low, piece), :] if own else target
        return pltpu.make_async_remote_copy(
            src_ref=source,
            dst_ref=target,
            send_sem=left_send.at[unit, hop],
            recv_sem=left_recv.at[unit, hop],
            device_id={"fs": fs - 1},
            device_id_type=MESH,
        )

    def to_side(unit, side, hop, move):
        w = units[unit][0]
        low, piece = unit_rows(unit)
        block = fs - hop if side == 0 else fs + hop
        target = place(w, block, low, piece)
        return pltpu.make_async_remote_copy(
            src_ref=target,
            dst_ref=target,
            send_sem=side_send.at[unit, side, move - 1, hop],
            recv_sem=side_recv.at[unit, side, move - 1, hop],
            device_id={"grp": lax.rem(grp + move, grp_n)},
            device_id_type=MESH,
        )

    def send_own(unit):
        if unit >= len(units):
            return

        @pl.when(fs < fs_n - 1)
        def _():
            to_right(unit, 0, own=True).start()

        @pl.when(fs > 0)
        def _():
            to_left(unit, 0, own=True).start()

    def relay(unit):
        def step(hop, carry):
            @pl.when(fs >= hop)
            def _():
                to_right(unit, hop - 1).wait_recv()

                @pl.when(fs < fs_n - 1)
                def _():
                    to_right(unit, hop).start()

                for move in range(1, grp_n):
                    to_side(unit, 0, hop, move).start()

            @pl.when(fs + hop < fs_n)
            def _():
                to_left(unit, hop - 1).wait_recv()

                @pl.when(fs > 0)
                def _():
                    to_left(unit, hop).start()

                for move in range(1, grp_n):
                    to_side(unit, 1, hop, move).start()

            return carry

        lax.fori_loop(1, fs_n, step, 0)

    def wait_weight(w):
        own_copy(w).wait()
        for unit in range(len(units)):
            if units[unit][0] == w:

                def step(hop, carry, unit=unit):
                    for move in range(1, grp_n):

                        @pl.when(fs >= hop)
                        def _():
                            to_side(unit, 0, hop, move).wait_recv()

                        @pl.when(fs + hop < fs_n)
                        def _():
                            to_side(unit, 1, hop, move).wait_recv()

                    return carry

                lax.fori_loop(1, fs_n, step, 0)

    def finish_sends():
        for unit in range(len(units)):

            def step(hop, carry, unit=unit):
                @pl.when((fs >= hop) & (fs < fs_n - 1))
                def _():
                    to_right(unit, hop).wait_send()

                @pl.when((fs + hop < fs_n) & (fs > 0))
                def _():
                    to_left(unit, hop).wait_send()

                @pl.when(hop > 0)
                def _():
                    for move in range(1, grp_n):

                        @pl.when(fs >= hop)
                        def _():
                            to_side(unit, 0, hop, move).wait_send()

                        @pl.when(fs + hop < fs_n)
                        def _():
                            to_side(unit, 1, hop, move).wait_send()

                return carry

            lax.fori_loop(0, fs_n, step, 0)

    def other(move, which):
        return lax.rem(chip + move, chips) * 2 + which

    def origin(move, which):
        return lax.rem(chip + chips - move, chips) * 2 + which

    def chunk_rows(owner):
        return pl.ds(aligned(owner * chunk, 16), chunk)

    def column_span(col):
        return pl.ds(aligned(col * column, 128), column)

    def pair_copy(phase, col, move):
        span = column_span(col)
        return pltpu.make_async_remote_copy(
            src_ref=parts.at[phase, chunk_rows(other(move, 1 - core)), span],
            dst_ref=paired.at[phase, move, :, span],
            send_sem=pair_send.at[phase, col, move],
            recv_sem=pair_recv.at[phase, col, move],
            device_id={"tp": twin},
            device_id_type=MESH,
        )

    def sum_copy(phase, col, move):
        span = column_span(col)
        return pltpu.make_async_remote_copy(
            src_ref=outgoing.at[phase, move, :, span],
            dst_ref=landed.at[phase, move, :, span],
            send_sem=sum_send.at[phase, col, move],
            recv_sem=sum_recv.at[phase, col, move],
            device_id={"tp": other(move, core)},
            device_id_type=MESH,
        )

    def piece_span(owner, piece):
        return pl.ds(aligned(owner * chunk + piece * piece_rows, 16), piece_rows)

    def twin_copy(phase, piece):
        rows = piece_span(tp, piece)
        return pltpu.make_async_remote_copy(
            src_ref=streams.at[phase, rows, :],
            dst_ref=streams.at[phase, rows, :],
            send_sem=twin_send.at[phase, piece],
            recv_sem=twin_recv.at[phase, piece],
            device_id={"tp": twin},
            device_id_type=MESH,
        )

    def put_copy(phase, piece, move):
        rows = piece_span(tp, piece)
        return pltpu.make_async_remote_copy(
            src_ref=streams.at[phase, rows, :],
            dst_ref=streams.at[phase, rows, :],
            send_sem=put_send.at[phase, piece, move],
            recv_sem=put_recv.at[phase, piece, move],
            device_id={"tp": other(move, core)},
            device_id_type=MESH,
        )

    def pass_copy(phase, piece, move):
        rows = piece_span(origin(move, core), piece)
        return pltpu.make_async_remote_copy(
            src_ref=streams.at[phase, rows, :],
            dst_ref=streams.at[phase, rows, :],
            send_sem=pass_send.at[phase, piece, move],
            recv_sem=pass_recv.at[phase, piece, move],
            device_id={"tp": twin},
            device_id_type=MESH,
        )

    def gain(row):
        return all_gains[row][...].astype(F32).reshape(1, width)

    def norm_rows(load, row):
        def body(low):
            values = load(pl.ds(low, 32)).astype(F32)
            scale = lax.rsqrt(jnp.mean(values * values, axis=-1, keepdims=True) + 1e-06)
            normed[pl.ds(low, 32), :] = (values * scale * gain(row)).astype(BF16)

        over_rows(count, 32, body)

    def start_sums(phase, col):
        for move in range(1, chips):
            pair_copy(phase, col, move).wait_recv()
            span = column_span(col)
            mine = parts[phase, chunk_rows(other(move, core)), span].astype(F32)
            both = mine + paired[phase, move, :, span].astype(F32)
            outgoing[phase, move, :, span] = both.astype(BF16)
            sum_copy(phase, col, move).start()

    def add_branch(phase, load, row, factor):
        for col in range(columns):
            pair_copy(phase, col, 0).wait_recv()
            for move in range(1, chips):
                sum_copy(phase, col, move).wait_recv()
        for piece in range(piece_n):

            def body(low, piece=piece):
                here = pl.ds(aligned(piece * piece_rows + low, 16), 16)
                rows = pl.ds(aligned(tp * chunk + piece * piece_rows + low, 16), 16)
                total = parts[phase, rows, :].astype(F32) + paired[phase, 0, here, :].astype(F32)
                for move in range(1, chips):
                    total = total + landed[phase, move, here, :].astype(F32)
                scale = lax.rsqrt(jnp.mean(total * total, axis=-1, keepdims=True) + 1e-06)
                branch = total * scale * gain(row)
                streams[phase, rows, :] = (load(rows).astype(F32) + factor * branch).astype(BF16)

            over_rows(piece_rows, 16, body)
            for move in range(1, chips):
                put_copy(phase, piece, move).start()
            twin_copy(phase, piece).start()

    def wait_put(phase):
        for piece in range(piece_n):
            for move in range(1, chips):
                put_copy(phase, piece, move).wait_recv()
                pass_copy(phase, piece, move).start()
        for piece in range(piece_n):
            twin_copy(phase, piece).wait_recv()
            for move in range(1, chips):
                pass_copy(phase, piece, move).wait_recv()

    def finish_phase(phase):
        for col in range(columns):
            for move in range(chips):
                pair_copy(phase, col, move).wait_send()
            for move in range(1, chips):
                sum_copy(phase, col, move).wait_send()
        for piece in range(piece_n):
            twin_copy(phase, piece).wait_send()
            for move in range(1, chips):
                put_copy(phase, piece, move).wait_send()
                pass_copy(phase, piece, move).wait_send()

    def hidden_units():
        def body(low, size):
            cols = pl.ds(low, size)
            gate = jnp.dot(normed[...], gate_full[:, cols], preferred_element_type=F32)
            upper = jnp.dot(normed[...], up_full[:, cols], preferred_element_type=F32)
            hidden[:, cols] = (gate / (1.0 + jnp.exp(-gate)) * upper).astype(BF16)

        over_tiles(hidden.shape[1], body)

    def project(phase, left, right):
        blocks = fs_n // columns

        def step(col, carry):
            terms = [
                jnp.dot(left[...], right[col * blocks + b], preferred_element_type=F32)
                for b in range(blocks)
            ]
            terms = terms[0] if blocks == 1 else jnp.concatenate(terms, axis=1)
            parts[phase, :, column_span(col)] = terms.astype(BF16)
            for move in range(chips - 1, -1, -1):
                pair_copy(phase, col, move).start()

            @pl.when(col > 0)
            def _():
                start_sums(phase, col - 1)

            return carry

        lax.fori_loop(0, columns, step, 0)
        start_sums(phase, columns - 1)

    def mix():
        rows = lax.broadcasted_iota(jnp.int32, (BLOCK, BLOCK), 0)
        cols = lax.broadcasted_iota(jnp.int32, (BLOCK, BLOCK), 1)
        all_spatial_gain = spatial_gain[...].astype(F32).reshape(1, mixed.shape[1])
        for g in range(mixed.shape[1] // GROUP_WIDTH):
            span = slice(g * GROUP_WIDTH, (g + 1) * GROUP_WIDTH)
            v = gelu(jnp.dot(normed[...], v_full[:, span], preferred_element_type=F32))
            u = gelu(jnp.dot(normed[...], u_full[:, span], preferred_element_type=F32))
            v = v - jnp.mean(v, axis=-1, keepdims=True)
            v = v * lax.rsqrt(jnp.mean(v * v, axis=-1, keepdims=True) + 1e-05)
            v = (v * all_spatial_gain[:, span]).astype(BF16)
            weight = spatial_weight[g].astype(F32)
            weight = jnp.where(rows >= cols, weight, 0.0).astype(BF16)
            bias = spatial_bias[...][g : g + 1, :].astype(F32)
            bias = jnp.sum(jnp.where(rows == cols, bias, 0.0), axis=1, keepdims=True)
            for n in range(count // BLOCK):
                part = slice(n * BLOCK, (n + 1) * BLOCK)
                spatial = jnp.dot(weight, v[part], preferred_element_type=F32)
                spatial = spatial + bias
                mixed[part, span] = (u[part] * spatial).astype(BF16)

    load_tokens = lambda rows: tokens[rows, :]
    load_first = lambda rows: streams[0, rows, :]
    load_second = lambda rows: streams[1, rows, :]

    send_own(0)
    send_own(1)
    for w in range(6):
        own_copy(w).start()
    norm_rows(load_tokens, 0)

    for unit in range(5):
        relay(unit)
        send_own(unit + 2)
    wait_weight(0)
    wait_weight(1)
    hidden_units()
    relay(5)
    send_own(7)
    relay(6)
    send_own(8)
    send_own(9)
    wait_weight(2)
    project(0, hidden, down_full)
    relay(7)
    add_branch(0, load_tokens, 1, 0.5)
    relay(8)
    wait_put(0)
    norm_rows(load_first, 2)
    relay(9)
    wait_weight(3)
    wait_weight(4)
    mix()
    wait_weight(5)
    project(1, mixed, out_full)
    add_branch(1, load_first, 3, 1.0)
    wait_put(1)
    norm_rows(load_second, 4)
    hidden_units()
    project(2, hidden, down_full)
    add_branch(2, load_second, 5, 0.5)
    finish_sends()
    wait_put(2)
    last = pltpu.make_async_copy(streams.at[2], result, last_sem)
    last.start()
    for phase in range(3):
        finish_phase(phase)
    last.wait()


def shards(
    sizes,
    tokens,
    ffn_pre_gain,
    gate_weight,
    up_weight,
    down_weight,
    ffn_post_gain,
    mix_pre_gain,
    mix_u_weight,
    mix_v_weight,
    spatial_gain,
    spatial_weight,
    spatial_bias,
    mix_out_weight,
    mix_post_gain,
    late_pre_gain,
    late_post_gain,
):
    grp_n, fs_n, tp_n = sizes
    count, width = tokens.shape
    hidden_width = gate_weight.shape[1]
    channels = mix_u_weight.shape[1]
    columns = math.gcd(fs_n, 4)
    chips = tp_n // 2
    chunk = count // tp_n
    pieces = max(1, chunk // PIECE)
    vmem = pl.BlockSpec(memory_space=pltpu.VMEM)
    hbm = pl.BlockSpec(memory_space=pl.ANY)
    units = sum(SPLITS)
    dma = pltpu.SemaphoreType.DMA
    return pl.pallas_call(
        functools.partial(kernel, sizes),
        out_shape=jax.ShapeDtypeStruct((count, width), BF16),
        in_specs=[vmem] * 7 + [hbm, hbm, hbm, hbm, hbm, hbm, vmem, vmem, vmem],
        out_specs=hbm,
        scratch_shapes=[
            pltpu.VMEM((width, hidden_width), BF16),
            pltpu.VMEM((width, hidden_width), BF16),
            pltpu.VMEM((fs_n,) + down_weight.shape, BF16),
            pltpu.VMEM((width, channels), BF16),
            pltpu.VMEM((width, channels), BF16),
            pltpu.VMEM((fs_n,) + mix_out_weight.shape, BF16),
            pltpu.VMEM((count, width), BF16),
            pltpu.VMEM((count, hidden_width), BF16),
            pltpu.VMEM((count, channels), BF16),
            pltpu.VMEM((3, count, width), BF16),
            pltpu.VMEM((3, chips, chunk, width), BF16),
            pltpu.VMEM((3, chips, chunk, width), BF16),
            pltpu.VMEM((3, chips, chunk, width), BF16),
            pltpu.VMEM((3, count, width), BF16),
            dma((6,)),
            dma((units, fs_n)),
            dma((units, fs_n)),
            dma((units, fs_n)),
            dma((units, fs_n)),
            dma((units, 2, grp_n - 1, fs_n)),
            dma((units, 2, grp_n - 1, fs_n)),
            dma((3, columns, chips)),
            dma((3, columns, chips)),
            dma((3, columns, chips)),
            dma((3, columns, chips)),
            dma((3, pieces)),
            dma((3, pieces)),
            dma((3, pieces, chips)),
            dma((3, pieces, chips)),
            dma((3, pieces, chips)),
            dma((3, pieces, chips)),
            dma(()),
        ],
        compiler_params=pltpu.CompilerParams(
            collective_id=0, has_side_effects=True, vmem_limit_bytes=60 * 2**20
        ),
    )(
        tokens,
        ffn_pre_gain,
        ffn_post_gain,
        mix_pre_gain,
        mix_post_gain,
        late_pre_gain,
        late_post_gain,
        gate_weight,
        up_weight,
        down_weight,
        mix_u_weight,
        mix_v_weight,
        mix_out_weight,
        spatial_gain,
        spatial_weight,
        spatial_bias,
    )


PIECES = (2, 2, 2, 1, 1, 1)
AHEAD = 4
LAG = 2
ROW_SPLIT = (2, 5)
END_GROUPS = 1


def halves(size):
    small = size // 256 * 128
    return small, size - 2 * small


def end_share(size):
    return size // (4 * GROUP_WIDTH) * END_GROUPS * GROUP_WIDTH


def weight_units(shapes, grp_n):
    units = []
    for group in ((0, 1), (2,), (3,), (4,), (5,)):
        made = []
        for w in group:
            rows, cols = shapes[w]
            split = w in ROW_SPLIT
            size = rows if split else cols
            small, extra = halves(size)
            ends = end_share(size)
            if w < 3:
                cuts = [("side", (0, small + extra), 0, small, PIECES[w])]
                if extra:
                    cuts.append(("middle", (small, small), small, extra, 1))
            else:
                cuts = [
                    ("middle", (ends, ends), 0, size - ends, PIECES[w]),
                    ("ends", (0, 0), 0, ends, PIECES[w]),
                ]
            mine = []
            for route, source, target, span, pieces in cuts:
                share = (span if split else rows) // grp_n
                piece = share // pieces
                for n in range(pieces):
                    mine.append((w, route, source, target, span, share, n * piece, piece))
            made.append(mine)
        for n in range(max(len(mine) for mine in made)):
            units += [mine[n] for mine in made if n < len(mine)]
    return units


def shared_kernel(
    sizes,
    units,
    tokens,
    gain0,
    gain1,
    gain2,
    gain3,
    gain4,
    gain5,
    gate_w,
    up_w,
    down_w,
    u_w,
    v_w,
    out_w,
    spatial_gain,
    spatial_weight,
    spatial_bias,
    result,
    gate_full,
    up_full,
    down_full,
    u_full,
    v_full,
    out_full,
    normed,
    hidden,
    mixed,
    streams,
    parts,
    paired,
    outgoing,
    landed,
    crossing,
    crossed,
    own_sem,
    fresh_send,
    relay_send,
    relay_recv,
    side_send,
    side_recv,
    pair_send,
    pair_recv,
    sum_send,
    sum_recv,
    cross_send,
    cross_recv,
    put_send,
    put_recv,
    last_sem,
):
    grp_n, fs_n, tp_n = sizes
    grp, fs, tp = lax.axis_index("grp"), lax.axis_index("fs"), lax.axis_index("tp")
    shards = (gate_w, up_w, down_w, u_w, v_w, out_w)
    fulls = (gate_full, up_full, down_full, u_full, v_full, out_full)
    count, width = tokens.shape
    chips = tp_n // 2
    chip, core = tp // 2, lax.rem(tp, 2)
    twin = tp + 1 - 2 * core
    across = (1 - chip) * 2 + core
    spot = core * chips + chip
    far_spot = core * chips + 1 - chip
    columns = pair_recv.shape[2]
    column = width // columns
    piece_n = put_send.shape[1]
    piece_rows = count // piece_n
    chunk = piece_rows // tp_n
    all_gains = (gain0, gain1, gain2, gain3, gain4, gain5)
    middle = fs_n // 2

    last = [unit for unit in range(len(units)) if units[unit][0] < 2][-1]
    downs = [unit for unit in range(len(units)) if units[unit][0] == 2]
    first = [unit for unit in range(len(units)) if units[unit][0] == 3]
    second = [unit for unit in range(len(units)) if units[unit][0] == 4]
    third = [unit for unit in range(len(units)) if units[unit][0] == 5]

    inner = jnp.logical_and(fs > 0, fs < fs_n - 1)
    outer = jnp.logical_not(inner)

    class Near:
        half = jnp.where(inner, 1, 0)
        partner = fs + 1 - 2 * lax.rem(fs, 2)

    class Far:
        half = fs // middle
        partner = lax.rem(fs + middle, fs_n)

    ffn, mixer = Far, Near
    phases = (ffn, mixer, ffn)

    barrier = pltpu.get_barrier_semaphore()
    for move in range(1, fs_n):
        pl.semaphore_signal(
            barrier, inc=1, device_id={"fs": lax.rem(fs + move, fs_n)}, device_id_type=MESH
        )
    for move in range(1, grp_n):
        pl.semaphore_signal(
            barrier, inc=1, device_id={"grp": lax.rem(grp + move, grp_n)}, device_id_type=MESH
        )
    for move in range(1, tp_n):
        pl.semaphore_signal(
            barrier, inc=1, device_id={"tp": lax.rem(tp + move, tp_n)}, device_id_type=MESH
        )
    pl.semaphore_wait(barrier, fs_n - 1 + grp_n - 1 + tp_n - 1)

    def view(unit, block):
        w, _, _, target, span, share, low, rows = units[unit]
        start = grp * share + low
        if w in ROW_SPLIT:
            return fulls[w].at[block, pl.ds(aligned(target + start, 16), rows), :]
        start = aligned(block * shards[w].shape[0] + start, 16)
        return fulls[w].at[pl.ds(start, rows), pl.ds(target, span)]

    def shard_view(unit, half):
        w, _, source, _, span, share, low, rows = units[unit]
        start = grp * share + low
        base = source[0] + half * (source[1] - source[0])
        if w in ROW_SPLIT:
            return shards[w].at[pl.ds(aligned(base + start, 16), rows), :]
        return shards[w].at[pl.ds(aligned(start, 16), rows), pl.ds(aligned(base, 128), span)]

    def has(unit):
        return {"side": True, "middle": inner, "ends": outer}[units[unit][1]]

    def own_copies(w):
        size = shards[w].shape[0 if w in ROW_SPLIT else 1]
        small, extra = halves(size)
        ends = end_share(size)

        def part(base, low, span, sem):
            if w in ROW_SPLIT:
                source = shards[w].at[pl.ds(aligned(base, 128), span), :]
                target = fulls[w].at[fs, pl.ds(low, span), :]
            else:
                rows = shards[w].shape[0]
                source = shards[w].at[:, pl.ds(aligned(base, 128), span)]
                target = fulls[w].at[pl.ds(aligned(fs * rows, 16), rows), pl.ds(low, span)]
            return pltpu.make_async_copy(source, target, own_sem.at[w, sem])

        if w >= 3:
            return [(inner, part(ends, 0, size - ends, 0)), (outer, part(0, 0, ends, 1))]
        made = [(True, part(ffn.half * (small + extra), 0, small, 0))]
        if extra:
            made.append((inner, part(small, small, extra, 1)))
        return made

    def guarded(ok, act):
        if ok is True:
            act()
        else:
            pl.when(ok)(act)

    def fresh_copies(unit):
        route = units[unit][1]
        half = ffn.half
        block = view(unit, fs)

        def made(slot, half, target):
            return pltpu.make_async_remote_copy(
                src_ref=shard_view(unit, half),
                dst_ref=block,
                send_sem=fresh_send.at[unit, slot],
                recv_sem=relay_recv.at[unit, fs],
                device_id={"fs": target},
                device_id_type=MESH,
            )

        if route == "middle":
            return (
                (fs != middle - 1, lambda: made(0, 0, middle - 1)),
                (fs != middle, lambda: made(1, 0, middle)),
            )
        if route == "ends":
            return (
                (fs > 0, lambda: made(0, 0, 0)),
                (fs < fs_n - 1, lambda: made(1, 0, fs_n - 1)),
            )
        near = fs + 1 - 2 * lax.rem(fs, 2)
        return (
            (True, lambda: made(0, half, near)),
            (True, lambda: made(1, 1 - half, jnp.where(fs < middle, middle, middle - 1))),
        )

    def send_own(unit):
        if unit < first[0]:
            for ok, copy in fresh_copies(unit):
                guarded(ok, lambda copy=copy: copy().start())

    def send_some(some, route):
        for unit in some:
            if units[unit][1] == route:
                for ok, copy in fresh_copies(unit):
                    guarded(ok, lambda copy=copy: copy().start())

    def relay_copy(unit, block, leftward):
        target = view(unit, block)
        return pltpu.make_async_remote_copy(
            src_ref=target,
            dst_ref=target,
            send_sem=relay_send.at[unit, block],
            recv_sem=relay_recv.at[unit, block],
            device_id={"fs": fs - 1 if leftward else fs + 1},
            device_id_type=MESH,
        )

    def goes_on(unit, leftward, act):
        if units[unit][1] == "side":
            pl.when(lax.rem(fs, middle) == (1 if leftward else 0))(act)

    def side_copy(unit, block, move):
        target = view(unit, block)
        return pltpu.make_async_remote_copy(
            src_ref=target,
            dst_ref=target,
            send_sem=side_send.at[unit, move - 1],
            recv_sem=side_recv.at[unit, move - 1],
            device_id={"grp": lax.rem(grp + move, grp_n)},
            device_id_type=MESH,
        )

    def side_total(unit, move):
        w, _, _, target, span, share, low, rows = units[unit]
        others = fs_n - 1
        if w in ROW_SPLIT:
            total = fulls[w].at[pl.ds(0, others), pl.ds(0, rows), :]
        else:
            total = fulls[w].at[pl.ds(0, others * rows), pl.ds(target, span)]
        return pltpu.make_async_remote_copy(
            src_ref=total,
            dst_ref=total,
            send_sem=side_send.at[unit, move - 1],
            recv_sem=side_recv.at[unit, move - 1],
            device_id={"grp": lax.rem(grp + move, grp_n)},
            device_id_type=MESH,
        )

    def over_blocks(unit, act):
        def whole():
            def step(d, carry):
                @pl.when(fs + d < fs_n)
                def _():
                    act(fs + d, True)

                @pl.when(fs >= d)
                def _():
                    act(fs - d, False)

                return carry

            lax.fori_loop(1, fs_n, step, 0)

        guarded(has(unit), whole)

    def relay(unit):
        def act(block, leftward):
            relay_copy(unit, block, leftward).wait_recv()

            goes_on(unit, leftward, lambda: relay_copy(unit, block, leftward).start())

            for move in range(1, grp_n):
                side_copy(unit, block, move).start()

        over_blocks(unit, act)
        send_own(unit + AHEAD)

    def wait_weight(w):
        for ok, copy in own_copies(w):
            guarded(ok, copy.wait)
        for unit in range(len(units)):
            if units[unit][0] == w:

                def act(unit=unit):
                    for move in range(1, grp_n):
                        side_total(unit, move).wait_recv()

                guarded(has(unit), act)

    def finish_sends(some):
        for unit in some:
            for ok, copy in fresh_copies(unit):
                guarded(ok, lambda copy=copy: copy().wait_send())

            def act(block, leftward, unit=unit):
                goes_on(unit, leftward, lambda: relay_copy(unit, block, leftward).wait_send())

            def sides(unit=unit):
                for move in range(1, grp_n):
                    side_total(unit, move).wait_send()

            over_blocks(unit, act)
            guarded(has(unit), sides)

    def column_span(col):
        return pl.ds(aligned(col * column, 128), column)

    def pair_step(phase, piece, col):
        span = column_span(col)
        return pltpu.make_async_remote_copy(
            src_ref=parts.at[phase, piece, :, 1 - core, :, span],
            dst_ref=paired.at[phase, piece, :, :, span],
            send_sem=pair_send.at[phase, piece],
            recv_sem=pair_recv.at[phase, piece, col],
            device_id={"tp": twin},
            device_id_type=MESH,
        )

    def side_of(phase, turn):
        half = phases[phase].half
        return 1 - half if turn == 0 else half

    def sum_step(phase, piece, turn, col):
        span = column_span(col)
        return pltpu.make_async_remote_copy(
            src_ref=outgoing.at[phase, piece, turn, :, span],
            dst_ref=landed.at[phase, piece, turn, :, span],
            send_sem=sum_send.at[phase, piece],
            recv_sem=sum_recv.at[phase, piece, turn, col],
            device_id={"tp": across},
            device_id_type=MESH,
        )

    def cross_step(phase, piece, col):
        span = column_span(col)
        return pltpu.make_async_remote_copy(
            src_ref=crossing.at[phase, piece, :, span],
            dst_ref=crossed.at[phase, piece, :, span],
            send_sem=cross_send.at[phase, piece],
            recv_sem=cross_recv.at[phase, piece, col],
            device_id={"fs": phases[phase].partner},
            device_id_type=MESH,
        )

    def all_sent(source, target, sem, device):
        pltpu.make_async_remote_copy(
            src_ref=source,
            dst_ref=target,
            send_sem=sem,
            recv_sem=pair_recv.at[0, 0, 0],
            device_id=device,
            device_id_type=MESH,
        ).wait_send()

    def group_rows(phase, side, piece, inside, size):
        start = piece * 2 * piece_rows + side * piece_rows + inside
        if phase == 3:
            start = piece * piece_rows + inside
        return pl.ds(aligned(start, 16), size)

    def put_slot(phase, which):
        before = (0, 4, 11, 18)[phase]
        kinds = ((1, 3, 4, 6), (0, 1, 2, 3, 4, 5, 6), (0, 1, 2, 3, 4, 5, 6), (0, 2, 5))[phase]
        return before + kinds.index(3 if which == 7 else which)

    def put_copy(phase, which, piece):
        half = phases[phase].half if phase < 3 else 0
        side = 1 - half if which in (3, 4, 6) else half
        place = far_spot if which in (5, 6, 7) else spot
        rows = normed.at[phase, group_rows(phase, side, piece, place * chunk, chunk), :]
        if which in (0, 3):
            target = {"tp": across}
        elif which in (1, 7):
            target = {"fs": phases[phase].partner}
        else:
            target = {"tp": twin}
        return pltpu.make_async_remote_copy(
            src_ref=rows,
            dst_ref=rows,
            send_sem=put_send.at[put_slot(phase, which), piece],
            recv_sem=put_recv.at[put_slot(phase, which), piece],
            device_id=target,
            device_id_type=MESH,
        )

    own_puts = ((1,), (0, 1, 2), (0, 1, 2), (0, 2))
    every_put = (0, 1, 2, 3, 4, 5, 6, 7)
    all_puts = ((1, 3, 4, 6), every_put, every_put, (0, 2, 5))

    def start_puts(phase, piece):
        for which in (1, 0, 2):
            if which in own_puts[phase]:
                put_copy(phase, which, piece).start()

    def routed(phase, which):
        split = phase > 0 and phase < 3 and phases[phase] is Near
        cut = piece_n // 2 if split else piece_n
        return range(cut) if which == 3 else range(cut, piece_n)

    def pieces_of(phase, which):
        if which in (3, 7):
            return routed(phase, which)
        return range(piece_n)

    def pass_near(phase, piece):
        put_copy(phase, 1, piece).wait_recv()
        if piece in routed(phase, 3):
            put_copy(phase, 3, piece).start()
        put_copy(phase, 4, piece).start()

    def pass_side(phase, piece):
        put_copy(phase, 0, piece).wait_recv()
        if phase < 3 and piece in routed(phase, 7):
            put_copy(phase, 7, piece).start()
        put_copy(phase, 5, piece).start()

    def pass_last(phase, piece):
        put_copy(phase, 3 if piece in routed(phase, 3) else 7, piece).wait_recv()
        put_copy(phase, 6, piece).start()

    def wait_puts(phase, piece, some):
        for which in some:
            put_copy(phase, which, piece).wait_recv()

    def finish_phase(phase):
        for piece in range(piece_n):
            target = paired.at[phase, piece]
            source = parts.at[phase, piece, :, 1 - core]
            all_sent(source, target, pair_send.at[phase, piece], {"tp": twin})
            source, target = outgoing.at[phase, piece], landed.at[phase, piece]
            all_sent(source, target, sum_send.at[phase, piece], {"tp": across})
            source, target = crossing.at[phase, piece], crossed.at[phase, piece]
            device = {"fs": phases[phase].partner}
            all_sent(source, target, cross_send.at[phase, piece], device)

    def finish_puts(phase):
        for which in all_puts[phase]:
            for piece in pieces_of(phase, which):
                put_copy(phase, which, piece).wait_send()

    def gain(row):
        return all_gains[row][...].astype(F32).reshape(1, width)

    def scaled(values, row):
        scale = lax.rsqrt(jnp.mean(values * values, axis=-1, keepdims=True) + 1e-06)
        return values * scale * gain(row)

    def norm_tokens(piece, start, size):
        def body(low):
            here = aligned(piece * piece_rows + start + low, 16)
            values = tokens[pl.ds(here, 16), :].astype(F32)
            target = group_rows(0, ffn.half, piece, start + low, 16)
            normed[0, target, :] = scaled(values, 0).astype(BF16)

        over_rows(size, 16, body)

    def pass_sum(phase, piece, turn, col):
        span = column_span(col)
        if turn == 0:
            pair_step(phase, piece, col).wait_recv()
        here = pl.ds(aligned((1 - chip) * chunk, 16), chunk)
        side = side_of(phase, turn)
        total = parts[phase, piece, side, core, here, span].astype(F32)
        total = total + paired[phase, piece, side, here, span].astype(F32)
        outgoing[phase, piece, turn, :, span] = total.astype(BF16)
        sum_step(phase, piece, turn, col).start()

    def cross_sums(phase, piece):
        side = 1 - phases[phase].half
        here = pl.ds(aligned(chip * chunk, 16), chunk)

        def step(col, carry):
            span = column_span(col)
            sum_step(phase, piece, 0, col).wait_recv()
            total = parts[phase, piece, side, core, here, span].astype(F32)
            total = total + paired[phase, piece, side, here, span].astype(F32)
            total = total + landed[phase, piece, 0, :, span].astype(F32)
            crossing[phase, piece, :, span] = total.astype(BF16)
            cross_step(phase, piece, col).start()
            return carry

        lax.fori_loop(0, columns, step, 0)

    def add_branch(phase, piece, load, row, factor):
        def wait(col, carry):
            sum_step(phase, piece, 1, col).wait_recv()
            cross_step(phase, piece, col).wait_recv()
            return carry

        lax.fori_loop(0, columns, wait, 0)
        side = phases[phase].half
        after = phases[phase + 1].half if phase < 2 else 0

        def body(low):
            rows = pl.ds(low, 16)
            here = pl.ds(aligned(chip * chunk + low, 16), 16)
            total = parts[phase, piece, side, core, here, :].astype(F32)
            total = total + paired[phase, piece, side, here, :].astype(F32)
            total = total + landed[phase, piece, 1, rows, :].astype(F32)
            total = total + crossed[phase, piece, rows, :].astype(F32)
            value = load(piece, low).astype(F32) + factor * scaled(total, row)
            value = value.astype(BF16)
            if phase < 2:
                streams[phase, pl.ds(aligned(piece * chunk + low, 16), 16), :] = value
                value = scaled(value.astype(F32), row + 1).astype(BF16)
            target = group_rows(phase + 1, after, piece, spot * chunk + low, 16)
            normed[phase + 1, target, :] = value

        over_rows(chunk, 16, body)
        start_puts(phase + 1, piece)

    def hidden_tile(phase, rows, cols):
        left = normed[phase, rows, :]
        gate = jnp.dot(left, gate_full[:, cols], preferred_element_type=F32)
        upper = jnp.dot(left, up_full[:, cols], preferred_element_type=F32)
        hidden[rows, cols] = (gate / (1.0 + jnp.exp(-gate)) * upper).astype(BF16)

    def piece_span(piece):
        return pl.ds(piece * 2 * piece_rows, 2 * piece_rows)

    def hidden_piece(phase, piece):
        rows = piece_span(piece)
        over_tiles(hidden.shape[1], lambda low, size: hidden_tile(phase, rows, pl.ds(low, size)))

    def project(phase, piece, left, right):
        rows = piece_span(piece)

        def step(col, carry):
            per = fs_n // columns
            terms = [
                jnp.dot(left[rows, :], right[col * per + b], preferred_element_type=F32)
                for b in range(per)
            ]
            terms = terms[0] if per == 1 else jnp.concatenate(terms, axis=1)
            terms = terms.astype(BF16).reshape(2, 2, chips * chunk, column)
            parts[phase, piece, :, :, :, column_span(col)] = terms
            pair_step(phase, piece, col).start()

            @pl.when(col >= LAG)
            def _():
                pass_sum(phase, piece, 0, col - LAG)

            return carry

        def late(turn):
            def step(col, carry):
                pass_sum(phase, piece, turn, col)
                return carry

            return step

        lax.fori_loop(0, columns, step, 0)
        lax.fori_loop(columns - LAG, columns, late(0), 0)
        lax.fori_loop(0, columns, late(1), 0)

    def mix(piece):
        at = lax.broadcasted_iota(jnp.int32, (BLOCK, BLOCK), 0)
        to = lax.broadcasted_iota(jnp.int32, (BLOCK, BLOCK), 1)
        here = mixed.shape[1]
        groups = here // GROUP_WIDTH
        shift = spatial_weight.shape[0] - groups
        all_gain = spatial_gain[...].astype(F32).reshape(1, spatial_gain.shape[0])
        all_gain = jnp.where(inner, all_gain[:, all_gain.shape[1] - here :], all_gain[:, :here])
        all_bias = spatial_bias[...].astype(F32)
        all_bias = jnp.where(inner, all_bias[shift:], all_bias[:groups])

        def block(n, carry):
            rows = pl.ds(aligned(piece * 2 * piece_rows + n * BLOCK, 16), BLOCK)
            left = normed[1, rows, :]
            every_v = gelu(jnp.dot(left, v_full[...], preferred_element_type=F32))
            every_u = gelu(jnp.dot(left, u_full[...], preferred_element_type=F32))
            for g in range(groups):
                span = slice(g * GROUP_WIDTH, (g + 1) * GROUP_WIDTH)
                v = every_v[:, span]
                v = v - jnp.mean(v, axis=-1, keepdims=True)
                v = v * lax.rsqrt(jnp.mean(v * v, axis=-1, keepdims=True) + 1e-05)
                v = (v * all_gain[:, span]).astype(BF16)
                weight = spatial_weight[g + shift * mixer.half].astype(F32)
                weight = jnp.where(at >= to, weight, 0.0).astype(BF16)
                bias = jnp.where(at == to, all_bias[g : g + 1, :], 0.0)
                bias = jnp.sum(bias, axis=1, keepdims=True)
                spatial = jnp.dot(weight, v, preferred_element_type=F32) + bias
                mixed[rows, span] = (every_u[:, span] * spatial).astype(BF16)
            return carry

        lax.fori_loop(0, 2 * piece_rows // BLOCK, block, 0)

    def load_tokens(piece, low):
        start = piece * piece_rows + spot * chunk + low
        return tokens[pl.ds(aligned(start, 16), 16), :]

    def load_stream(phase):
        return lambda piece, low: streams[phase, pl.ds(aligned(piece * chunk + low, 16), 16), :]

    def relays(some):
        for unit in some:
            relay(unit)

    for unit in range(AHEAD):
        send_own(unit)
    for w in range(6):
        for ok, copy in own_copies(w):
            guarded(ok, copy.start)
    for piece in range(piece_n):
        norm_tokens(piece, spot * chunk, chunk)
        start_puts(0, piece)

    def clear(pads, low):
        for full in pads:
            size = full.shape[-1] if len(full.shape) == 2 else full.shape[1]
            if low == size:
                continue
            if len(full.shape) == 2:
                full[:, pl.ds(low, size - low)] = jnp.zeros((full.shape[0], size - low), BF16)
            else:
                blank = jnp.zeros((fs_n, size - low, full.shape[2]), BF16)
                full[:, pl.ds(low, size - low), :] = blank

    @pl.when(outer)
    def _():
        small, extra = halves(gate_w.shape[1])
        if extra:
            clear((gate_full, up_full, down_full), small)
        clear((u_full, v_full, out_full), end_share(u_w.shape[1]))

    for piece in range(piece_n):
        for move in range(1, tp_n):
            norm_tokens(piece, lax.rem(spot + move, tp_n) * chunk, chunk)

    relays(range(0, 4))
    for piece in range(piece_n):
        pass_near(0, piece)
    send_some(first, "middle")
    relays(range(4, last + 1))
    for piece in range(piece_n):
        pass_last(0, piece)
    send_some(second, "middle")
    relay(downs[0])
    wait_weight(0)
    wait_weight(1)
    for piece in range(piece_n):
        wait_puts(0, piece, (4, 6))
        hidden_piece(0, piece)
        if piece == 0:
            relays(downs[1:2])
            send_some(third, "middle")
    relays(downs[2:])
    pl.when(inner)(lambda: relays(first))
    wait_weight(2)
    project(0, 0, hidden, down_full)
    project(0, 1, hidden, down_full)
    finish_sends(range(first[0]))
    send_some(first, "ends")
    pl.when(outer)(lambda: send_some(second + third, "ends"))
    pl.when(inner)(lambda: relays(second))
    cross_sums(0, 0)
    cross_sums(0, 1)
    pl.when(inner)(lambda: send_some(second, "ends"))
    pl.when(inner)(lambda: relays(third))
    add_branch(0, 0, load_tokens, 1, 0.5)
    pl.when(inner)(lambda: send_some(third, "ends"))
    add_branch(0, 1, load_tokens, 1, 0.5)
    pl.when(outer)(lambda: relays(first + second))
    pass_near(1, 0)
    pass_side(1, 0)
    wait_weight(3)
    wait_weight(4)
    pass_last(1, 0)
    pl.when(outer)(lambda: relays(third))
    pass_near(1, 1)
    pass_side(1, 1)
    wait_puts(1, 0, (2, 4, 5, 6))
    mix(0)
    wait_weight(5)
    project(1, 0, mixed, out_full)
    pass_last(1, 1)
    wait_puts(1, 1, (2, 4, 5, 6))
    cross_sums(1, 0)
    mix(1)
    project(1, 1, mixed, out_full)
    add_branch(1, 0, load_stream(0), 3, 1.0)
    cross_sums(1, 1)
    add_branch(1, 1, load_stream(0), 3, 1.0)
    pass_side(2, 0)
    pass_near(2, 0)
    pass_last(2, 0)
    pass_side(2, 1)
    wait_puts(2, 0, (2, 4, 5, 6))
    hidden_piece(2, 0)
    pass_near(2, 1)
    project(2, 0, hidden, down_full)
    cross_sums(2, 0)
    pass_last(2, 1)
    wait_puts(2, 1, (2, 4, 5, 6))
    hidden_piece(2, 1)
    project(2, 1, hidden, down_full)
    add_branch(2, 0, load_stream(1), 5, 0.5)
    cross_sums(2, 1)
    pass_side(3, 0)
    add_branch(2, 1, load_stream(1), 5, 0.5)
    pass_side(3, 1)
    finish_sends(range(first[0], len(units)))
    for phase in range(3):
        finish_phase(phase)
        finish_puts(phase)
    for piece in range(piece_n):
        wait_puts(3, piece, (2, 5))
    copy = pltpu.make_async_copy(normed.at[3, pl.ds(0, count), :], result, last_sem)
    copy.start()
    finish_puts(3)
    copy.wait()


def shared(
    sizes,
    tokens,
    ffn_pre_gain,
    gate_weight,
    up_weight,
    down_weight,
    ffn_post_gain,
    mix_pre_gain,
    mix_u_weight,
    mix_v_weight,
    spatial_gain,
    spatial_weight,
    spatial_bias,
    mix_out_weight,
    mix_post_gain,
    late_pre_gain,
    late_post_gain,
):
    grp_n, fs_n, tp_n = sizes
    count, width = tokens.shape
    small, extra = halves(gate_weight.shape[1])
    hidden_width = small + extra
    channels = mix_u_weight.shape[1] - end_share(mix_u_weight.shape[1])
    columns = math.gcd(fs_n, 4)
    pieces = count // BLOCK
    chunk = BLOCK // tp_n
    vmem = pl.BlockSpec(memory_space=pltpu.VMEM)
    hbm = pl.BlockSpec(memory_space=pl.ANY)
    weights = (gate_weight, up_weight, down_weight, mix_u_weight, mix_v_weight, mix_out_weight)
    units = weight_units([w.shape for w in weights], grp_n)
    unit_n = len(units)
    dma = pltpu.SemaphoreType.DMA
    return pl.pallas_call(
        functools.partial(shared_kernel, sizes, units),
        out_shape=jax.ShapeDtypeStruct((count, width), BF16),
        in_specs=[vmem] * 7 + [hbm, hbm, hbm, hbm, hbm, hbm, vmem, vmem, vmem],
        out_specs=hbm,
        scratch_shapes=[
            pltpu.VMEM((width, hidden_width), BF16),
            pltpu.VMEM((width, hidden_width), BF16),
            pltpu.VMEM((fs_n, hidden_width, down_weight.shape[1]), BF16),
            pltpu.VMEM((width, channels), BF16),
            pltpu.VMEM((width, channels), BF16),
            pltpu.VMEM((fs_n, channels, mix_out_weight.shape[1]), BF16),
            pltpu.VMEM((4, 2 * count, width), BF16),
            pltpu.VMEM((2 * count, hidden_width), BF16),
            pltpu.VMEM((2 * count, channels), BF16),
            pltpu.VMEM((2, count // tp_n, width), BF16),
            pltpu.VMEM((3, pieces, 2, 2, BLOCK // 2, width), BF16),
            pltpu.VMEM((3, pieces, 2, BLOCK // 2, width), BF16),
            pltpu.VMEM((3, pieces, 2, chunk, width), BF16),
            pltpu.VMEM((3, pieces, 2, chunk, width), BF16),
            pltpu.VMEM((3, pieces, chunk, width), BF16),
            pltpu.VMEM((3, pieces, chunk, width), BF16),
            dma((6, 2)),
            dma((unit_n, 2)),
            dma((unit_n, fs_n)),
            dma((unit_n, fs_n)),
            dma((unit_n, max(1, grp_n - 1))),
            dma((unit_n, max(1, grp_n - 1))),
            dma((3, pieces)),
            dma((3, pieces, columns)),
            dma((3, pieces)),
            dma((3, pieces, 2, columns)),
            dma((3, pieces)),
            dma((3, pieces, columns)),
            dma((21, pieces)),
            dma((21, pieces)),
            dma(()),
        ],
        compiler_params=pltpu.CompilerParams(
            collective_id=0, has_side_effects=True, vmem_limit_bytes=60 * 2**20
        ),
    )(
        tokens,
        ffn_pre_gain,
        ffn_post_gain,
        mix_pre_gain,
        mix_post_gain,
        late_pre_gain,
        late_post_gain,
        gate_weight,
        up_weight,
        down_weight,
        mix_u_weight,
        mix_v_weight,
        mix_out_weight,
        spatial_gain,
        spatial_weight,
        spatial_bias,
    )


def can_share(sizes, tokens, gate_weight, mix_u_weight):
    grp_n, fs_n, tp_n = sizes
    count = tokens.shape[0] // (grp_n * fs_n)
    rows = gate_weight.shape[0] // fs_n
    hidden_width = gate_weight.shape[1] // tp_n
    channels = mix_u_weight.shape[1] // tp_n
    return (
        tp_n == 4
        and fs_n == 4
        and count == 2 * BLOCK
        and rows % (32 * grp_n) == 0
        and hidden_width % 128 == 0
        and halves(hidden_width)[0] % (32 * grp_n) == 0
        and channels % (4 * GROUP_WIDTH) == 0
    )


def solution(mesh):
    in_specs = (
        P(("grp", "fs"), None),
        P(),
        P("fs", "tp"),
        P("fs", "tp"),
        P("tp", "fs"),
        P(),
        P(),
        P("fs", "tp"),
        P("fs", "tp"),
        P("tp"),
        P("tp", None, None),
        P("tp", None),
        P("tp", "fs"),
        P(),
        P(),
        P(),
    )
    out_specs = P(("grp", "fs"), None)
    sizes = (mesh.shape["grp"], mesh.shape["fs"], mesh.shape["tp"])

    def step(*arrays):
        plan = shared if can_share(sizes, arrays[0], arrays[2], arrays[7]) else shards
        body = functools.partial(plan, sizes)
        return jax.shard_map(
            body, mesh=mesh, in_specs=in_specs, out_specs=out_specs, check_vma=False
        )(*arrays)

    return step
```
